32 devices in a mesh: kv: 4 (over y, x), tp: 8 (over z, core).
Axes of the slice: x: 2, y: 2, z: 4, core: 2. Of those that a mesh axis runs over, the one named last changes fastest.
Arguments:
- resid: bfloat16 [32, 4096], P('tp', 'kv'), may hold values from -35 to 35
- attn_gain: bfloat16 [4096], replicated, may hold values from 0.099609375 to 1.8984375
- w_query_nope: bfloat16 [4096, 8192], P('kv', 'tp'), may hold values from -0.09375 to 0.09375
- w_query_rope: bfloat16 [4096, 4096], P('kv', 'tp'), may hold values from -0.09375 to 0.09375
- w_latent: bfloat16 [4096, 512], P('kv'), may hold values from -0.09375 to 0.09375
- w_key_rope: bfloat16 [4096, 64], replicated, may hold values from -0.09375 to 0.09375
- latent_gain: bfloat16 [512], replicated, may hold values from 0.099609375 to 1.8984375
- key_up: bfloat16 [512, 64, 128], P(None, 'tp'), may hold values from -0.5 to 0.5
- value_up: bfloat16 [512, 64, 128], P(None, 'tp'), may hold values from -0.25 to 0.25
- w_out: bfloat16 [8192, 4096], P('tp', 'kv'), may hold values from -4 to 4
- post_gain: bfloat16 [4096], replicated, may hold values from 0.099609375 to 1.8984375
- mlp_gain: bfloat16 [4096], replicated, may hold values from 0.099609375 to 1.8984375
- w_gate: bfloat16 [4096, 11008], P('kv', 'tp'), may hold values from -3 to 3
- w_up: bfloat16 [4096, 11008], P('kv', 'tp'), may hold values from -3 to 3
- w_down: bfloat16 [11008, 4096], P('tp', 'kv'), may hold values from -0.0546875 to 0.0546875
- cache_latent: bfloat16 [32, 2048, 512], P('tp', 'kv'), may hold values from -6 to 6
- cache_rope_key: bfloat16 [32, 2048, 64], P('tp', 'kv'), may hold values from -740 to 740
Outputs:
- next_resid: bfloat16 [32, 4096], P('tp', 'kv')
- new_latent: bfloat16 [32, 512], P('tp')
- new_rope_key: bfloat16 [32, 64], P('tp')
The draws below stay inside these ranges and needn't reach their ends.
All inputs are finite; a program needn't handle non-finite values.
Results may differ from the reference program's by a relative error of at most 0.035.
Values may be sent and summed in bfloat16 or wider, within the bound.
No kernel may reach another device: no remote copies, remote signals or barrier semaphores. Data moves between devices by JAX's collectives and lax.ppermute only.
A program may use at most 64 MiB of HBM per device.

```python
import jax
import jax.numpy as jnp
from jax import lax

D = 4096
H = 64
NOPE = 128
ROPE = 64
VD = 128
LAT = 512
FF = 11008
POS_DEV = 512
BATCH = 32
CTX = 2048
N_KV = 4


def rising_profile(length, factor):
    place = (jnp.arange(length, dtype=jnp.float32) + 0.5) / length
    profile = jnp.exp(jnp.log(factor) * (place - 0.5))
    return profile / jnp.sqrt(jnp.mean(profile * profile))


def draw_resid(key, part):
    key_base, key_rows = jax.random.split(jax.random.fold_in(key, 101))
    column_pos = jnp.arange(D, dtype=jnp.float32) / D
    column_scale = 0.5 * jnp.exp(jnp.log(4.0) * column_pos)[None, :]
    base_draw = jnp.clip(jax.random.normal(key_base, (BATCH, D), jnp.float32), -6.0, 6.0)
    row_scale = jnp.exp(jax.random.uniform(key_rows, (BATCH, 1), jnp.float32, -0.5, 0.5))
    return (base_draw * column_scale * row_scale).astype(jnp.bfloat16)


def draw_w_out(key, part):
    factor = 6.0
    base_draw = jnp.clip(jax.random.normal(jax.random.fold_in(key, 103), (H * VD, D), jnp.float32), -6.0, 6.0)
    scaled = base_draw * rising_profile(H * VD, factor)[:, None] * rising_profile(D, factor)[None, :]
    return (scaled * (H * VD) ** (-0.5)).astype(jnp.bfloat16)


def rising_rows(key, factor):
    base_draw = jnp.clip(jax.random.normal(key, (D, FF), jnp.float32), -6.0, 6.0)
    return (base_draw * rising_profile(D, factor)[:, None] * D ** (-0.5)).astype(jnp.bfloat16)


def draw_w_gate(key, part):
    factor = 6.0
    return rising_rows(jax.random.fold_in(key, 107), factor)


def draw_w_up(key, part):
    factor = 6.0
    return rising_rows(jax.random.fold_in(key, 109), factor)


def draw_cache_rope_key(key, part):
    key_base = jax.random.fold_in(jax.random.fold_in(key, 113), 0)
    base_draw = jnp.clip(jax.random.normal(key_base, (BATCH, CTX, ROPE), jnp.float32), -6.0, 6.0)
    return base_draw.astype(jnp.bfloat16)


def block_levels(stream_key, shape, cuts, smallest, top_value):
    def one(dim, blocks):
        draws = jax.random.uniform(jax.random.fold_in(jax.random.fold_in(stream_key, 6), dim), (blocks,), jnp.float32, smallest / len(cuts), top_value / len(cuts))
        return jnp.repeat(jnp.exp(draws), shape[dim] // blocks).reshape((-1,) + (1,) * (len(shape) - dim - 1))

    loudness = one(*cuts[0])
    for cut in cuts[1:]:
        loudness = loudness * one(*cut)
    return loudness


def noise(key, shape, width, reach, pieces=(), kind=jnp.bfloat16):
    values = jax.random.normal(key, shape, jnp.float32) * width
    if len(pieces) > 0:
        values = block_levels(key, shape, pieces, -0.22, 0.18) * values
    return jnp.clip(values, min=-reach, max=reach).astype(kind)


def setup_inputs(seed: int = 0) -> dict:
    streams_of = jax.random.split(jax.random.key(seed), 18)
    resid = draw_resid(jax.random.fold_in(streams_of[17], 71), 0)
    attn_gain = jnp.clip(1.0 + 0.18 * jax.random.normal(streams_of[1], (D,), jnp.float32), 0.099609375, 1.8984375).astype(jnp.bfloat16)
    w_query_nope = noise(streams_of[2], (D, H * NOPE), D ** -0.5, 0.09375, ((0, 4), (1, 8)))
    w_query_rope = noise(streams_of[3], (D, H * ROPE), D ** -0.5, 0.09375, ((0, 4), (1, 8)))
    w_latent = noise(streams_of[4], (D, LAT), D ** -0.5, 0.09375, ((0, 4),))
    w_key_rope = noise(streams_of[5], (D, ROPE), D ** -0.5, 0.09375)
    latent_gain = jnp.clip(1.0 + 0.18 * jax.random.normal(streams_of[6], (LAT,), jnp.float32), 0.099609375, 1.8984375).astype(jnp.bfloat16)
    key_up = noise(streams_of[7], (LAT, H, NOPE), NOPE ** -0.5, 0.5, ((1, 8),))
    value_up = noise(streams_of[8], (LAT, H, VD), LAT ** -0.5, 0.25, ((1, 8),))
    w_out = draw_w_out(jax.random.fold_in(streams_of[17], 71), 0)
    post_gain = jnp.clip(1.0 + 0.18 * jax.random.normal(streams_of[10], (D,), jnp.float32), 0.099609375, 1.8984375).astype(jnp.bfloat16)
    mlp_gain = jnp.clip(1.0 + 0.18 * jax.random.normal(streams_of[11], (D,), jnp.float32), 0.099609375, 1.8984375).astype(jnp.bfloat16)
    w_gate = draw_w_gate(jax.random.fold_in(streams_of[17], 71), 0)
    w_up = draw_w_up(jax.random.fold_in(streams_of[17], 71), 0)
    w_down = noise(streams_of[14], (FF, D), FF ** -0.5, 0.0546875, ((0, 8), (1, 4)))
    cache_latent = noise(streams_of[15], (BATCH, CTX, LAT), 1.0, 6.0, ((0, 8), (1, 4)))
    cache_rope_key = draw_cache_rope_key(jax.random.fold_in(streams_of[17], 71), 0)
    return dict(resid=resid, attn_gain=attn_gain, w_query_nope=w_query_nope, w_query_rope=w_query_rope, w_latent=w_latent, w_key_rope=w_key_rope, latent_gain=latent_gain, key_up=key_up, value_up=value_up, w_out=w_out, post_gain=post_gain, mlp_gain=mlp_gain, w_gate=w_gate, w_up=w_up, w_down=w_down, cache_latent=cache_latent, cache_rope_key=cache_rope_key)


EPS = 1e-06
THETA = 10000.0

def rotate(vector, position):
    half_width = vector.shape[-1] // 2
    frequency = THETA ** (-jnp.arange(half_width, dtype=jnp.float32) / half_width)
    angles = jnp.asarray(position, jnp.float32) * frequency
    cos_table, sin_table = (jnp.cos(angles), jnp.sin(angles))
    lower_half, upper_half = (vector[..., :half_width], vector[..., half_width:])
    return jnp.concatenate([lower_half * cos_table - upper_half * sin_table, lower_half * sin_table + upper_half * cos_table], axis=-1)

def reference(resid, attn_gain, w_query_nope, w_query_rope, w_latent, w_key_rope, latent_gain, key_up, value_up, w_out, post_gain, mlp_gain, w_gate, w_up, w_down, cache_latent, cache_rope_key):
    batch_rows = resid.shape[0]
    head_count = key_up.shape[1]
    context = cache_latent.shape[1]
    latent_width = cache_latent.shape[2]
    score_scale = (key_up.shape[2] + cache_rope_key.shape[2]) ** (-0.5)
    resid_float = resid.astype(jnp.float32)
    normed_a = (resid_float * attn_gain.astype(jnp.float32)).astype(jnp.bfloat16)
    scale_in = lax.rsqrt(lax.optimization_barrier(jnp.mean(resid_float * resid_float, axis=1, keepdims=True)) + EPS)
    q_nope = (jnp.dot(normed_a, w_query_nope, preferred_element_type=jnp.float32) * scale_in).astype(jnp.bfloat16)
    q_rope_raw = jnp.dot(normed_a, w_query_rope, preferred_element_type=jnp.float32) * scale_in
    q_rope = rotate(q_rope_raw.reshape(batch_rows, head_count, -1), context).astype(jnp.bfloat16)
    latent_raw = jnp.dot(normed_a, w_latent, preferred_element_type=jnp.float32)
    new_latent = (latent_raw * lax.rsqrt(lax.optimization_barrier(jnp.mean(latent_raw * latent_raw, axis=1, keepdims=True)) + EPS) * latent_gain.astype(jnp.float32)).astype(jnp.bfloat16)
    key_raw = jnp.dot(normed_a, w_key_rope, preferred_element_type=jnp.float32) * scale_in
    new_rope_key = rotate(key_raw, context).astype(jnp.bfloat16)
    q_lat = jnp.einsum('bhd,chd->bhc', q_nope.reshape(batch_rows, head_count, -1).astype(jnp.float32), key_up.astype(jnp.float32)).astype(jnp.bfloat16)

    def attend(item):
        query_lat, query_rope, keys, rope_keys, own_latent, own_rope = item
        scores = (jnp.dot(query_lat, keys.T, preferred_element_type=jnp.float32) + jnp.dot(query_rope, rope_keys.T, preferred_element_type=jnp.float32)) * score_scale
        own_score = (jnp.dot(query_lat, own_latent, preferred_element_type=jnp.float32) + jnp.dot(query_rope, own_rope, preferred_element_type=jnp.float32)) * score_scale
        peak = jnp.maximum(lax.optimization_barrier(jnp.max(scores, axis=1)), own_score)
        probs = jnp.exp(scores - peak[:, None])
        own_prob = jnp.exp(own_score - peak)
        totals = lax.optimization_barrier(jnp.sum(probs, axis=1)) + own_prob
        weights = probs.astype(jnp.bfloat16).reshape(head_count, N_KV, POS_DEV)
        blocks = keys.reshape(N_KV, POS_DEV, latent_width)
        partial_value = jnp.einsum('hjp,jpc->hjc', weights.astype(jnp.float32), blocks.astype(jnp.float32))
        partial_value = partial_value.astype(jnp.bfloat16).astype(jnp.float32)
        summed = lax.optimization_barrier(jnp.sum(partial_value, axis=1)) + own_prob[:, None] * own_latent.astype(jnp.float32)[None, :]
        return (summed / totals[:, None]).astype(jnp.bfloat16)
    o_lat = lax.map(attend, (q_lat, q_rope, cache_latent, cache_rope_key, new_latent, new_rope_key))
    o_heads = jnp.einsum('bhc,che->bhe', o_lat.astype(jnp.float32), value_up.astype(jnp.float32))
    o_heads = o_heads.astype(jnp.bfloat16).reshape(batch_rows, -1)
    attended = jnp.dot(o_heads, w_out, preferred_element_type=jnp.float32)
    post_part = attended * lax.rsqrt(lax.optimization_barrier(jnp.mean(attended * attended, axis=1, keepdims=True)) + EPS) * post_gain.astype(jnp.float32)
    resid_mid = (resid_float + post_part).astype(jnp.bfloat16)
    mid_float = resid_mid.astype(jnp.float32)
    normed_m = (mid_float * mlp_gain.astype(jnp.float32)).astype(jnp.bfloat16)
    scale_mid = lax.rsqrt(lax.optimization_barrier(jnp.mean(mid_float * mid_float, axis=1, keepdims=True)) + EPS)
    gate = jnp.dot(normed_m, w_gate, preferred_element_type=jnp.float32) * scale_mid
    up_part = jnp.dot(normed_m, w_up, preferred_element_type=jnp.float32) * scale_mid
    hidden = (jax.nn.silu(gate) * up_part).astype(jnp.bfloat16)
    next_resid = (mid_float + jnp.dot(hidden, w_down, preferred_element_type=jnp.float32)).astype(jnp.bfloat16)
    return (next_resid, new_latent, new_rope_key)
```

```python
import functools

import jax
import jax.numpy as jnp
import numpy as np
from jax import lax
from jax.experimental import pallas as pl
from jax.experimental.pallas import tpu as pltpu
from jax.sharding import PartitionSpec as P

EPS = 1e-06
THETA = 10000.0
BF = jnp.bfloat16
F32 = jnp.float32


def rotate(vector, position):
    half_width = vector.shape[-1] // 2
    frequency = THETA ** (-jnp.arange(half_width, dtype=F32) / half_width)
    angles = jnp.asarray(position, F32) * frequency
    cos_table, sin_table = (jnp.cos(angles), jnp.sin(angles))
    lower_half, upper_half = (vector[..., :half_width], vector[..., half_width:])
    return jnp.concatenate(
        [
            lower_half * cos_table - upper_half * sin_table,
            lower_half * sin_table + upper_half * cos_table,
        ],
        axis=-1,
    )


def dot(a, b):
    return jnp.dot(a, b, preferred_element_type=F32)


def pieces(value, count):
    out, rest = [], value
    for _ in range(count):
        term = lax.reduce_precision(rest, 8, 7)
        out.append(term.astype(BF))
        rest = rest - term
    return out


def spread(block, axis, groups=None):
    count = len(groups[0]) if groups else lax.axis_size(axis)
    copies = jnp.broadcast_to(block[None], (count,) + block.shape)
    return lax.all_to_all(copies, axis, 0, 0, tiled=True, axis_index_groups=groups)


def plain_body(
    resid,
    attn_gain,
    w_query_nope,
    w_query_rope,
    w_latent,
    w_key_rope,
    latent_gain,
    key_up,
    value_up,
    w_out,
    post_gain,
    mlp_gain,
    w_gate,
    w_up,
    w_down,
    cache_latent,
    cache_rope_key,
):
    nk = lax.axis_size("kv")
    nt = lax.axis_size("tp")
    kv_index = lax.axis_index("kv")
    tp_index = lax.axis_index("tp")
    own, width = resid.shape
    rows = own * nt
    model_width = width * nk
    latent, heads, nope = key_up.shape
    value_width = value_up.shape[2]
    rope = cache_rope_key.shape[2]
    pos_dev = cache_latent.shape[1]
    context = pos_dev * nk
    score_scale = (nope + rope) ** (-0.5)
    col_start = kv_index * width
    split_rows = own % nk == 0

    def block_of(vector):
        return lax.dynamic_slice_in_dim(vector, col_start, width, 0).astype(F32)[None, :]

    gathered = spread(resid, "tp").swapaxes(0, 1).reshape(rows, width)
    gathered_float = gathered.astype(F32)
    gain_a = block_of(attn_gain)
    normed_a = (gathered_float * gain_a).astype(BF)
    own_normed = (resid.astype(F32) * gain_a).astype(BF)
    key_rows = lax.dynamic_slice_in_dim(w_key_rope, col_start, width, 0)
    squares = jnp.sum(gathered_float * gathered_float, axis=1, keepdims=True)
    own_squares = jnp.sum(resid.astype(F32) ** 2, axis=1, keepdims=True)
    q_part = jnp.concatenate(
        [
            dot(normed_a, w_query_nope).astype(BF),
            dot(normed_a, w_query_rope).astype(BF),
            *pieces(squares, 2),
            jnp.zeros((rows, 126), BF),
        ],
        axis=1,
    )
    own_part = jnp.concatenate(
        [
            dot(own_normed, w_latent).astype(BF),
            dot(own_normed, key_rows).astype(BF),
            *pieces(own_squares, 2),
        ],
        axis=1,
    )
    nope_dev, rope_dev = heads * nope, heads * rope
    q_width, own_width = q_part.shape[1], own_part.shape[1]
    sent_width = max(q_width, own_width)
    q_part = jnp.pad(q_part, ((0, 0), (0, sent_width - q_width)))
    own_part = jnp.pad(own_part, ((0, 0), (0, sent_width - own_width)))
    summed = jnp.sum(
        spread(jnp.concatenate([q_part, own_part], axis=0), "kv").astype(F32), axis=0
    )
    q_sum, own_sum = summed[:rows], summed[rows:, :own_width]
    square_sum = jnp.sum(q_sum[:, nope_dev + rope_dev :], axis=1, keepdims=True)
    scale_in = lax.rsqrt(square_sum / model_width + EPS)
    q_nope = (q_sum[:, :nope_dev] * scale_in).astype(BF).reshape(rows, heads, nope)
    q_rope = rotate(
        (q_sum[:, nope_dev : nope_dev + rope_dev] * scale_in).reshape(rows, heads, rope), context
    ).astype(BF)
    latent_sum = own_sum[:, :latent]
    own_scale = lax.rsqrt(
        jnp.sum(own_sum[:, latent + rope :], axis=1, keepdims=True) / model_width + EPS
    )
    new_latent = (
        latent_sum
        * lax.rsqrt(jnp.mean(latent_sum * latent_sum, axis=1, keepdims=True) + EPS)
        * latent_gain.astype(F32)[None, :]
    ).astype(BF)
    new_rope_key = rotate(own_sum[:, latent : latent + rope] * own_scale, context).astype(BF)
    q_lat = jnp.einsum("bhd,chd->bhc", q_nope, key_up, preferred_element_type=F32).astype(BF)

    query = jnp.concatenate([q_lat, q_rope], axis=-1).reshape(own, nt, heads, latent + rope)
    query = lax.all_to_all(query.swapaxes(0, 1), "tp", 0, 0, tiled=True)
    query = query.transpose(1, 0, 2, 3).reshape(own, nt * heads, latent + rope)
    all_heads = nt * heads
    seq_lat, seq_rope = query[..., :latent], query[..., latent:]
    scores = (
        jnp.einsum("bhc,bpc->bhp", seq_lat, cache_latent, preferred_element_type=F32)
        + jnp.einsum("bhr,bpr->bhp", seq_rope, cache_rope_key, preferred_element_type=F32)
    ) * score_scale
    own_score = (
        jnp.einsum("bhc,bc->bh", seq_lat, new_latent, preferred_element_type=F32)
        + jnp.einsum("bhr,br->bh", seq_rope, new_rope_key, preferred_element_type=F32)
    ) * score_scale
    peak = jnp.maximum(jnp.max(scores, axis=2), own_score)
    probs = jnp.exp(scores - peak[:, :, None])
    own_prob = jnp.where(kv_index == 0, jnp.exp(own_score - peak), 0.0)
    totals = jnp.sum(probs, axis=2) + own_prob
    partial_value = (
        jnp.einsum("bhp,bpc->bhc", probs.astype(BF), cache_latent, preferred_element_type=F32)
        + own_prob[:, :, None] * new_latent.astype(F32)[:, None, :]
    )
    packed = jnp.concatenate(
        [partial_value.astype(BF)]
        + [p[:, :, None] for p in pieces(peak, 3) + pieces(totals, 3)]
        + [jnp.zeros((own, all_heads, 122), BF)],
        axis=2,
    )

    def combine(blocks):
        stats = blocks[..., latent:].astype(F32)
        peaks = jnp.sum(stats[..., :3], axis=-1, keepdims=True)
        sums = jnp.sum(stats[..., 3:6], axis=-1, keepdims=True)
        factor = jnp.exp(peaks - jnp.max(peaks, axis=0, keepdims=True))
        value = jnp.sum(blocks[..., :latent].astype(F32) * factor, axis=0)
        return (value / jnp.sum(sums * factor, axis=0)).astype(BF)

    if split_rows:
        per = own // nk
        sent = packed.reshape(nk, per, nt, heads, latent + 128).swapaxes(1, 2)
        sent = sent.reshape(nk * nt, per, heads, latent + 128)
        got = lax.all_to_all(sent, ("kv", "tp"), 0, 0, tiled=True)
        got = got.reshape(nk, nt, per, heads, latent + 128)
        o_lat = combine(got).swapaxes(0, 1).reshape(per * nt, heads, latent)
    else:
        flat = own * all_heads // nk
        got = lax.all_to_all(packed.reshape(nk, flat, latent + 128), "kv", 0, 0, tiled=True)
        o_own = spread(combine(got), "kv").reshape(own, nt, heads, latent)
        o_lat = lax.all_to_all(o_own.swapaxes(0, 1), "tp", 0, 0, tiled=True)
        o_lat = o_lat.swapaxes(0, 1).reshape(rows, heads, latent)
    o_heads = jnp.einsum("bhc,che->bhe", o_lat, value_up, preferred_element_type=F32).astype(BF)
    o_flat = o_heads.reshape(-1, heads * value_width)
    if split_rows:
        o_flat = spread(o_flat, "kv").reshape(rows, heads * value_width)

    core = lax.rem(tp_index, 2)
    swap = [(i, i ^ 1) for i in range(nt)]
    column = [list(range(c, nt, 2)) for c in range(2)]
    half = width // 2
    out_part = dot(o_flat, w_out).reshape(rows, 2, half)
    keep = jnp.where(core == 0, out_part[:, 0], out_part[:, 1])
    give = jnp.where(core == 0, out_part[:, 1], out_part[:, 0]).astype(BF)
    pair_sum = (keep + lax.ppermute(give, "tp", swap).astype(F32)).astype(BF)
    att_half = jnp.sum(spread(pair_sum, "tp", column).astype(F32), axis=0).astype(BF)
    att_other = lax.ppermute(att_half, "tp", swap)
    attended = jnp.where(
        core == 0,
        jnp.concatenate([att_half, att_other], axis=1),
        jnp.concatenate([att_other, att_half], axis=1),
    ).astype(F32)

    gain_m = block_of(mlp_gain)
    post = attended * block_of(post_gain)
    stacked = jnp.concatenate(
        [(gathered_float * gain_m).astype(BF), (post * gain_m).astype(BF)], axis=0
    )
    ff_dev = w_gate.shape[1]
    stats = [
        jnp.sum(a * b, axis=1, keepdims=True)
        for a, b in (
            (attended, attended),
            (gathered_float, gathered_float),
            (gathered_float, post),
            (post, post),
        )
    ]
    stat_block = jnp.concatenate(
        [jnp.concatenate(pieces(jnp.concatenate(stats[2 * i : 2 * i + 2], axis=0), 2), axis=1)
         for i in range(2)],
        axis=1,
    )
    ff_part = jnp.concatenate(
        [
            dot(stacked, w_gate).astype(BF),
            dot(stacked, w_up).astype(BF),
            stat_block,
        ],
        axis=1,
    )
    ff_sum = jnp.sum(spread(ff_part, "kv").astype(F32), axis=0)
    first = jnp.sum(ff_sum[:, 2 * ff_dev : 2 * ff_dev + 2], axis=1, keepdims=True)
    second = jnp.sum(ff_sum[:, 2 * ff_dev + 2 :], axis=1, keepdims=True)
    att_square, resid_square, cross, post_square = (
        first[:rows],
        first[rows:],
        second[:rows],
        second[rows:],
    )
    s = lax.rsqrt(att_square / model_width + EPS)
    mid_square = resid_square + 2.0 * s * cross + s * s * post_square
    scale_mid = lax.rsqrt(jnp.maximum(mid_square, 0.0) / model_width + EPS)
    mixed = (ff_sum[:rows] + s * ff_sum[rows:]) * scale_mid
    hidden = (jax.nn.silu(mixed[:, :ff_dev]) * mixed[:, ff_dev : 2 * ff_dev]).astype(BF)
    down = dot(hidden, w_down).astype(BF).reshape(own, nt, width).swapaxes(0, 1)
    lowered = jnp.sum(lax.all_to_all(down, "tp", 0, 0, tiled=True).astype(F32), axis=0)

    own_post = lax.dynamic_slice_in_dim(post.reshape(own, nt, width), tp_index, 1, 1)[:, 0]
    own_s = lax.dynamic_slice_in_dim(s.reshape(own, nt, 1), tp_index, 1, 1)[:, 0]
    resid_mid = (resid.astype(F32) + own_s * own_post).astype(BF).astype(F32)
    next_resid = (resid_mid + lowered).astype(BF)
    return (next_resid, new_latent, new_rope_key)


VMEM = pl.BlockSpec(memory_space=pltpu.VMEM)
NT = (((1,), (1,)), ((), ()))


def call(kernel, outs, *args, flops=0):
    many = isinstance(outs, (list, tuple))
    sizes = list(args) + (list(outs) if many else [outs])
    moved = sum(int(np.prod(a.shape)) * a.dtype.itemsize for a in sizes)
    return pl.pallas_call(
        kernel,
        out_shape=outs,
        in_specs=[VMEM] * len(args),
        out_specs=[VMEM] * len(outs) if many else VMEM,
        compiler_params=pltpu.CompilerParams(vmem_limit_bytes=16 << 20),
        cost_estimate=pl.CostEstimate(
            flops=max(flops, moved), bytes_accessed=moved, transcendentals=0
        ),
    )(*args)


def like(shape, dtype=BF):
    return jax.ShapeDtypeStruct(shape, dtype)


def lane_of(shape):
    return lax.broadcasted_iota(jnp.int32, shape, len(shape) - 1)


def terms(value, count):
    out, rest = [], value
    for _ in range(count):
        term = rest.astype(BF).astype(F32)
        out.append(term)
        rest = rest - term
    return out


def placed(columns, shape):
    lane = lane_of(shape)
    block = jnp.zeros(shape, F32)
    for at, column in columns:
        block = jnp.where(lane == at, column, block)
    return block


def picked(block, first, count):
    lane = lane_of(block.shape)
    inside = (lane >= first) & (lane < first + count)
    return jnp.sum(jnp.where(inside, block, 0.0), axis=-1, keepdims=True)


def turned(vector, table, half):
    width = vector.shape[1]
    low = lax.rem(lane_of(vector.shape), 2 * half) < half
    other = jnp.where(
        low, pltpu.roll(vector, width - half, 1), pltpu.roll(vector, half, 1)
    )
    return vector * table[0:1, :width] + other * table[1:2, :width]


def start_kernel(resid_ref, ga_ref, gp_ref, gm_ref, msg_ref, gains_ref):
    width = resid_ref.shape[1]
    tiles = width // 128
    at = pl.multiple_of(lax.axis_index("kv") * tiles, tiles)
    for i in range(msg_ref.shape[0]):
        msg_ref[i] = resid_ref[...]
    rows = []
    for ref in (ga_ref, gp_ref, gm_ref):
        block = ref[pl.ds(at, tiles), :].astype(F32)
        rows.append(jnp.concatenate([block[i : i + 1] for i in range(tiles)], axis=1))
    rows.append(jnp.zeros((8 - len(rows), width), F32))
    gains_ref[...] = jnp.concatenate(rows, axis=0)


def query_kernel(
    got_ref, resid_ref, gains_ref, wn_ref, wr_ref, wl_ref, wk_ref, msg_ref, rows_ref
):
    nt, own, width = got_ref.shape
    latent = wl_ref.shape[1]
    rope = wk_ref.shape[0]
    nope_dev, rope_dev = wn_ref.shape[1], wr_ref.shape[1]
    got = got_ref[...].astype(F32)
    x = jnp.concatenate([got[:, r, :] for r in range(own)], axis=0)
    rows_ref[...] = x.astype(BF)
    gain = gains_ref[0:1, :]
    normed = (x * gain).astype(BF)
    qn = jnp.dot(normed, wn_ref[...], preferred_element_type=F32)
    qr = jnp.dot(normed, wr_ref[...], preferred_element_type=F32)
    square = jnp.sum(x * x, axis=1, keepdims=True)
    mine = jnp.concatenate([resid_ref[...].astype(F32), jnp.zeros((nt - own, width), F32)], axis=0)
    own_square = jnp.sum(mine * mine, axis=1, keepdims=True)
    own_normed = (mine * gain).astype(BF)
    lat = jnp.dot(own_normed, wl_ref[...], preferred_element_type=F32)
    at = pl.multiple_of(lax.axis_index("kv") * width, width)
    key = lax.dot_general(own_normed, wk_ref[:, pl.ds(at, width)], NT, preferred_element_type=F32)
    half = latent // 2
    lat = lat[:, :half] + pltpu.roll(lat[:, half:], own, 0)
    key = jnp.concatenate([key, jnp.zeros((nt, 128 - rope), F32)], axis=1)
    own_terms = terms(own_square, 2)
    for r in range(msg_ref.shape[0]):
        part = slice(r * nt, (r + 1) * nt)
        msg_ref[r, :, :nope_dev] = qn[part].astype(BF)
        msg_ref[r, :, nope_dev : nope_dev + rope_dev] = qr[part].astype(BF)
        base = nope_dev + rope_dev
        msg_ref[r, :, base : base + half] = lat.astype(BF)
        columns = [(rope + i, c) for i, c in enumerate(own_terms + terms(square[part], 2))]
        stat = placed(columns, key.shape)
        msg_ref[r, :, base + half :] = jnp.where(lane_of(key.shape) < rope, key, stat).astype(BF)


def latent_kernel(
    model_width, heads, got_ref, ku_ref, gain_ref, table_ref, msg_ref, lat_ref, key_ref
):
    nk, nt, _ = got_ref.shape
    latent, nope_dev = ku_ref.shape
    own, rope = key_ref.shape
    rope_dev = heads * rope
    total = got_ref[0].astype(F32)
    for j in range(1, nk):
        total = total + got_ref[j].astype(F32)
    base, half = nope_dev + rope_dev, latent // 2
    stat = total[:, base + half :]
    scale = lax.rsqrt(picked(stat, rope + 2, 2) / model_width + EPS)
    own_scale = lax.rsqrt(picked(stat, rope, 2) / model_width + EPS)
    lat = total[:, base : base + half]
    lat = jnp.concatenate([lat, pltpu.roll(lat, own, 0)], axis=1)
    lat = lat * lax.rsqrt(jnp.mean(lat * lat, axis=1, keepdims=True) + EPS)
    lat_ref[...] = (lat * gain_ref[...].astype(F32))[:own].astype(BF)
    table = table_ref[...]
    key_ref[...] = turned(stat * own_scale, table, rope // 2)[:own, :rope].astype(BF)
    qn = (total[:, :nope_dev] * scale).astype(BF).astype(F32)
    qr = turned(total[:, nope_dev:base] * scale, table, rope // 2).astype(BF).astype(F32)

    def diagonal(q, size):
        shape = (nt, heads, heads * size)
        head = lax.broadcasted_iota(jnp.int32, shape, 1)
        lane = lax.broadcasted_iota(jnp.int32, shape, 2)
        keep = (lane >= head * size) & (lane < (head + 1) * size)
        spread_q = jnp.broadcast_to(q[:, None, :], shape)
        return jnp.where(keep, spread_q, 0.0).reshape(nt * heads, heads * size).astype(BF)

    q_lat = lax.dot_general(
        diagonal(qn, nope_dev // heads), ku_ref[...], NT, preferred_element_type=F32
    ).astype(BF)
    shape = (rope_dev, 128)
    row = lax.rem(lax.broadcasted_iota(jnp.int32, shape, 0), rope)
    unit = jnp.where(row == lane_of(shape), 1.0, 0.0).astype(BF)
    q_rope = jnp.dot(diagonal(qr, rope), unit, preferred_element_type=F32).astype(BF)
    for j in range(nk):
        msg_ref[j, :, :latent] = q_lat
        msg_ref[j, :, latent:] = q_rope


def attend_kernel(score_scale, q_ref, cache_ref, rope_ref, lat_ref, key_ref, msg_ref):
    own, all_heads, _ = q_ref.shape
    latent = cache_ref.shape[2]
    rope = rope_ref.shape[1]
    holds_own = lax.axis_index("kv") == 0
    lat, key = lat_ref[...].astype(F32), key_ref[...].astype(F32)
    for r in range(own):
        q_lat = q_ref[r, :, :latent]
        q_rope = q_ref[r, :, latent : latent + rope]
        keys = cache_ref[r]
        scores = (
            lax.dot_general(q_lat, keys, NT, preferred_element_type=F32)
            + jnp.dot(q_rope, rope_ref[r], preferred_element_type=F32)
        ) * score_scale
        own_score = (
            jnp.sum(q_lat.astype(F32) * lat[r : r + 1], axis=1, keepdims=True)
            + jnp.sum(q_rope.astype(F32) * key[r : r + 1], axis=1, keepdims=True)
        ) * score_scale
        peak = jnp.maximum(jnp.max(scores, axis=1, keepdims=True), own_score)
        probs = jnp.exp(scores - peak)
        own_prob = jnp.where(holds_own, jnp.exp(own_score - peak), 0.0)
        total = jnp.sum(probs, axis=1, keepdims=True) + own_prob
        value = jnp.dot(probs.astype(BF), keys, preferred_element_type=F32)
        msg_ref[r, :, :latent] = (value + own_prob * lat[r : r + 1]).astype(BF)
        columns = list(enumerate(terms(peak, 3) + terms(total, 3)))
        msg_ref[r, :, latent:] = placed(columns, (all_heads, 128)).astype(BF)


def value_kernel(heads, got_ref, vu_ref, msg_ref):
    nk, pairs, _ = got_ref.shape
    latent, value_dev = vu_ref.shape
    nt = pairs // heads
    stats = [got_ref[j, :, latent:].astype(F32) for j in range(nk)]
    peaks = [picked(s, 0, 3) for s in stats]
    peak = functools.reduce(jnp.maximum, peaks)
    factors = [jnp.exp(p - peak) for p in peaks]
    total = sum(picked(s, 3, 3) * f for s, f in zip(stats, factors))
    value = sum(got_ref[j, :, :latent].astype(F32) * f for j, f in enumerate(factors))
    o_lat = (value / total).astype(BF)
    full = jnp.dot(o_lat, vu_ref[...], preferred_element_type=F32)
    size = value_dev // heads
    shape = (nt, heads, value_dev)
    head = lax.broadcasted_iota(jnp.int32, shape, 1)
    lane = lax.broadcasted_iota(jnp.int32, shape, 2)
    keep = (lane >= head * size) & (lane < (head + 1) * size)
    o_heads = jnp.sum(jnp.where(keep, full.reshape(shape), 0.0), axis=1).astype(BF)
    for j in range(nk):
        msg_ref[j] = o_heads


def out_kernel(o_ref, w_ref, keep_ref, give_ref):
    half = keep_ref.shape[1]
    first = lax.rem(lax.axis_index("tp"), 2) == 0
    out = jnp.dot(o_ref[...], w_ref[...], preferred_element_type=F32)
    keep_ref[...] = jnp.where(first, out[:, :half], out[:, half:])
    give_ref[...] = jnp.where(first, out[:, half:], out[:, :half]).astype(BF)


def pair_kernel(keep_ref, got_ref, msg_ref):
    both = (keep_ref[...] + got_ref[...].astype(F32)).astype(BF)
    for i in range(msg_ref.shape[0]):
        msg_ref[i] = both


def column_kernel(got_ref, out_ref):
    total = got_ref[0].astype(F32)
    for i in range(1, got_ref.shape[0]):
        total = total + got_ref[i].astype(F32)
    out_ref[...] = total.astype(BF)


def gate_kernel(half_ref, other_ref, rows_ref, gains_ref, wg_ref, wu_ref, msg_ref, post_ref):
    nk, both, _ = msg_ref.shape
    rows = both // 2
    ff_dev = wg_ref.shape[0]
    chunk = (msg_ref.shape[2] - 128) // 2
    first = lax.rem(lax.axis_index("tp"), 2) == 0
    mine, other = half_ref[...].astype(F32), other_ref[...].astype(F32)
    att = jnp.concatenate(
        [jnp.where(first, mine, other), jnp.where(first, other, mine)], axis=1
    )
    x = rows_ref[...].astype(F32)
    post = att * gains_ref[1:2, :]
    post_ref[...] = post
    gain = gains_ref[2:3, :]
    stacked = jnp.concatenate([x * gain, post * gain], axis=0).astype(BF)

    def added(a, b):
        return jnp.sum(a * b, axis=1, keepdims=True)

    top = terms(added(att, att), 2) + terms(added(x, post), 2)
    low = terms(added(x, x), 2) + terms(added(post, post), 2)
    stat = placed(
        [(i, jnp.concatenate([a, b], axis=0)) for i, (a, b) in enumerate(zip(top, low))],
        (both, 128),
    ).astype(BF)
    for k, w_ref in enumerate((wg_ref, wu_ref)):
        part = lax.dot_general(stacked, w_ref[...], NT, preferred_element_type=F32)
        for j in range(nk):
            lo, hi = j * chunk, min((j + 1) * chunk, ff_dev)
            size = max(hi - lo, 0)
            if size < chunk:
                msg_ref[j, :, k * chunk : (k + 1) * chunk] = jnp.zeros((both, chunk), BF)
            if size > 0:
                msg_ref[j, :, k * chunk : k * chunk + size] = part[:, lo:hi].astype(BF)
    for j in range(nk):
        msg_ref[j, :, 2 * chunk :] = stat


def hidden_kernel(model_width, got_ref, msg_ref, s_ref):
    nk, both, _ = got_ref.shape
    rows, chunk = both // 2, msg_ref.shape[2]
    total = got_ref[0].astype(F32)
    for j in range(1, nk):
        total = total + got_ref[j].astype(F32)
    stat = total[:, 2 * chunk :]
    one, two = picked(stat, 0, 2), picked(stat, 2, 2)
    att_square, x_square, cross, post_square = one[:rows], one[rows:], two[:rows], two[rows:]
    s = lax.rsqrt(att_square / model_width + EPS)
    mid = jnp.maximum(x_square + 2.0 * s * cross + s * s * post_square, 0.0)
    scale = lax.rsqrt(mid / model_width + EPS)
    s_ref[...] = jnp.broadcast_to(s, s_ref.shape)
    mixed = (total[:rows, : 2 * chunk] + s * total[rows:, : 2 * chunk]) * scale
    gate, up = mixed[:, :chunk], mixed[:, chunk:]
    hidden = (gate / (1.0 + jnp.exp(-gate)) * up).astype(BF)
    for j in range(nk):
        msg_ref[j] = hidden


def down_kernel(got_ref, w_ref, msg_ref):
    nk, rows, chunk = got_ref.shape
    ff_dev = w_ref.shape[0]
    nt, own, _ = msg_ref.shape
    total = None
    for j in range(nk):
        lo, hi = j * chunk, min((j + 1) * chunk, ff_dev)
        if hi > lo:
            part = jnp.dot(
                got_ref[j, :, : hi - lo], w_ref[lo:hi, :], preferred_element_type=F32
            )
            total = part if total is None else total + part
    total = total.reshape(own, nt, total.shape[1])
    for t in range(nt):
        msg_ref[t] = total[:, t, :].astype(BF)


def last_kernel(got_ref, resid_ref, post_ref, s_ref, out_ref):
    nt, own, width = got_ref.shape
    total = got_ref[0].astype(F32)
    for t in range(1, nt):
        total = total + got_ref[t].astype(F32)
    added = (post_ref[...] * s_ref[:, 0:1]).reshape(own, nt, width)
    here = lax.broadcasted_iota(jnp.int32, added.shape, 1) == lax.axis_index("tp")
    mine = jnp.sum(jnp.where(here, added, 0.0), axis=1)
    mid = (resid_ref[...].astype(F32) + mine).astype(BF).astype(F32)
    out_ref[...] = (mid + total).astype(BF)


def exchange(message, axis, groups=None):
    return lax.all_to_all(message, axis, 0, 0, tiled=True, axis_index_groups=groups)


def kernel_body(
    resid,
    attn_gain,
    w_query_nope,
    w_query_rope,
    w_latent,
    w_key_rope,
    latent_gain,
    key_up,
    value_up,
    w_out,
    post_gain,
    mlp_gain,
    w_gate,
    w_up,
    w_down,
    cache_latent,
    cache_rope_key,
):
    nk = lax.axis_size("kv")
    nt = lax.axis_size("tp")
    own, width = resid.shape
    rows = own * nt
    model_width = width * nk
    latent, heads, nope = key_up.shape
    rope = cache_rope_key.shape[2]
    nope_dev, rope_dev = heads * nope, heads * rope
    ff_dev = w_gate.shape[1]
    context = cache_latent.shape[1] * nk
    half_rope = rope // 2
    angles = context * THETA ** (-np.arange(half_rope) / half_rope)
    cos, sin = np.cos(angles), np.sin(angles)
    table = np.zeros((8, rope_dev), np.float32)
    table[0] = np.tile(np.concatenate([cos, cos]), heads)
    table[1] = np.tile(np.concatenate([-sin, sin]), heads)

    tiles = [g.reshape(-1, 128) for g in (attn_gain, post_gain, mlp_gain)]
    msg, gains = call(
        start_kernel, [like((nt, own, width)), like((8, width), F32)], resid, *tiles
    )
    got = exchange(msg, "tp")
    msg, x_rows = call(
        query_kernel,
        [like((nk, nt, nope_dev + rope_dev + latent // 2 + 128)), like((rows, width))],
        got,
        resid,
        gains,
        w_query_nope,
        w_query_rope,
        w_latent,
        w_key_rope.T,
        flops=2 * rows * width * (nope_dev + rope_dev + latent),
    )
    got = exchange(msg, "kv")
    msg, new_latent, new_rope_key = call(
        functools.partial(latent_kernel, model_width, heads),
        [like((nk, rows * heads // own, latent + 128)), like((own, latent)), like((own, rope))],
        got,
        key_up.reshape(latent, nope_dev),
        latent_gain.reshape(1, latent),
        jnp.asarray(table),
        flops=2 * nt * heads * nope_dev * latent,
    )
    got = exchange(msg.reshape(nk * nt, heads, latent + 128), ("kv", "tp"))
    msg = call(
        functools.partial(attend_kernel, (nope + rope) ** (-0.5)),
        like((own, nt * heads, latent + 128)),
        got.reshape(own, nt * heads, latent + 128),
        cache_latent,
        cache_rope_key.swapaxes(1, 2),
        new_latent,
        new_rope_key,
        flops=4 * own * nt * heads * latent * cache_latent.shape[1],
    )
    got = exchange(msg.reshape(nk * nt, heads, latent + 128), ("kv", "tp"))
    value_dev = heads * value_up.shape[2]
    msg = call(
        functools.partial(value_kernel, heads),
        like((nk, nt, value_dev)),
        got.reshape(nk, nt * heads, latent + 128),
        value_up.reshape(latent, value_dev),
        flops=2 * nt * heads * latent * value_dev,
    )
    got = exchange(msg, "kv")
    half = width // 2
    keep, give = call(
        out_kernel,
        [like((rows, half), F32), like((rows, half))],
        got.reshape(rows, value_dev),
        w_out,
        flops=2 * rows * value_dev * width,
    )
    swap = [(i, i ^ 1) for i in range(nt)]
    column = [list(range(c, nt, 2)) for c in range(2)]
    got = lax.ppermute(give, "tp", swap)
    msg = call(pair_kernel, like((nt // 2, rows, half)), keep, got)
    got = exchange(msg, "tp", column)
    att_half = call(column_kernel, like((rows, half)), got)
    att_other = lax.ppermute(att_half, "tp", swap)
    chunk = -(-ff_dev // (nk * 128)) * 128
    msg, post = call(
        gate_kernel,
        [like((nk, 2 * rows, 2 * chunk + 128)), like((rows, width), F32)],
        att_half,
        att_other,
        x_rows,
        gains,
        w_gate.T,
        w_up.T,
        flops=8 * rows * width * ff_dev,
    )
    got = exchange(msg, "kv")
    msg, s = call(
        functools.partial(hidden_kernel, model_width),
        [like((nk, rows, chunk)), like((rows, 128), F32)],
        got,
    )
    got = exchange(msg, "kv")
    msg = call(
        down_kernel,
        like((nt, own, width)),
        got,
        w_down,
        flops=2 * rows * ff_dev * width,
    )
    got = exchange(msg, "tp")
    next_resid = call(last_kernel, like((own, width)), got, resid, post, s)
    return (next_resid, new_latent, new_rope_key)


def body(*args):
    resid, key_up, cache = args[0], args[7], args[15]
    nk, nt = lax.axis_size("kv"), lax.axis_size("tp")
    own, width = resid.shape
    latent, heads, nope = key_up.shape
    fits = (
        own == nk
        and nt == 8
        and heads == 8
        and 2 * own == nt
        and width % 1024 == 0
        and latent % 256 == 0
        and nope % 128 == 0
        and cache.shape[1] % 128 == 0
        and args[16].shape[2] == 64
    )
    return kernel_body(*args) if fits else plain_body(*args)


def solution(mesh):
    return jax.shard_map(
        body,
        mesh=mesh,
        in_specs=(
            P("tp", "kv"),
            P(),
            P("kv", "tp"),
            P("kv", "tp"),
            P("kv", None),
            P(),
            P(),
            P(None, "tp", None),
            P(None, "tp", None),
            P("tp", "kv"),
            P(),
            P(),
            P("kv", "tp"),
            P("kv", "tp"),
            P("tp", "kv"),
            P("tp", "kv", None),
            P("tp", "kv", None),
        ),
        out_specs=(P("tp", "kv"), P("tp", None), P("tp", None)),
        check_vma=False,
    )
```

```python
import functools

import jax
import jax.numpy as jnp
import numpy as np
from jax import lax
from jax.experimental import pallas as pl
from jax.experimental.pallas import tpu as pltpu
from jax.sharding import PartitionSpec as P

EPS = 1e-06
THETA = 10000.0
BF = jnp.bfloat16
F32 = jnp.float32


def rotate(vector, position):
    half_width = vector.shape[-1] // 2
    frequency = THETA ** (-jnp.arange(half_width, dtype=F32) / half_width)
    angles = jnp.asarray(position, F32) * frequency
    cos_table, sin_table = (jnp.cos(angles), jnp.sin(angles))
    lower_half, upper_half = (vector[..., :half_width], vector[..., half_width:])
    return jnp.concatenate(
        [
            lower_half * cos_table - upper_half * sin_table,
            lower_half * sin_table + upper_half * cos_table,
        ],
        axis=-1,
    )


def dot(a, b):
    return jnp.dot(a, b, preferred_element_type=F32)


def pieces(value, count):
    out, rest = [], value
    for _ in range(count):
        term = lax.reduce_precision(rest, 8, 7)
        out.append(term.astype(BF))
        rest = rest - term
    return out


def spread(block, axis, groups=None):
    count = len(groups[0]) if groups else lax.axis_size(axis)
    copies = jnp.broadcast_to(block[None], (count,) + block.shape)
    return lax.all_to_all(copies, axis, 0, 0, tiled=True, axis_index_groups=groups)


def plain_body(
    resid,
    attn_gain,
    w_query_nope,
    w_query_rope,
    w_latent,
    w_key_rope,
    latent_gain,
    key_up,
    value_up,
    w_out,
    post_gain,
    mlp_gain,
    w_gate,
    w_up,
    w_down,
    cache_latent,
    cache_rope_key,
):
    nk = lax.axis_size("kv")
    nt = lax.axis_size("tp")
    kv_index = lax.axis_index("kv")
    tp_index = lax.axis_index("tp")
    own, width = resid.shape
    rows = own * nt
    model_width = width * nk
    latent, heads, nope = key_up.shape
    value_width = value_up.shape[2]
    rope = cache_rope_key.shape[2]
    pos_dev = cache_latent.shape[1]
    context = pos_dev * nk
    score_scale = (nope + rope) ** (-0.5)
    col_start = kv_index * width
    split_rows = own % nk == 0

    def block_of(vector):
        return lax.dynamic_slice_in_dim(vector, col_start, width, 0).astype(F32)[None, :]

    gathered = spread(resid, "tp").swapaxes(0, 1).reshape(rows, width)
    gathered_float = gathered.astype(F32)
    gain_a = block_of(attn_gain)
    normed_a = (gathered_float * gain_a).astype(BF)
    own_normed = (resid.astype(F32) * gain_a).astype(BF)
    key_rows = lax.dynamic_slice_in_dim(w_key_rope, col_start, width, 0)
    squares = jnp.sum(gathered_float * gathered_float, axis=1, keepdims=True)
    own_squares = jnp.sum(resid.astype(F32) ** 2, axis=1, keepdims=True)
    q_part = jnp.concatenate(
        [
            dot(normed_a, w_query_nope).astype(BF),
            dot(normed_a, w_query_rope).astype(BF),
            *pieces(squares, 2),
            jnp.zeros((rows, 126), BF),
        ],
        axis=1,
    )
    own_part = jnp.concatenate(
        [
            dot(own_normed, w_latent).astype(BF),
            dot(own_normed, key_rows).astype(BF),
            *pieces(own_squares, 2),
        ],
        axis=1,
    )
    nope_dev, rope_dev = heads * nope, heads * rope
    q_width, own_width = q_part.shape[1], own_part.shape[1]
    sent_width = max(q_width, own_width)
    q_part = jnp.pad(q_part, ((0, 0), (0, sent_width - q_width)))
    own_part = jnp.pad(own_part, ((0, 0), (0, sent_width - own_width)))
    summed = jnp.sum(
        spread(jnp.concatenate([q_part, own_part], axis=0), "kv").astype(F32), axis=0
    )
    q_sum, own_sum = summed[:rows], summed[rows:, :own_width]
    square_sum = jnp.sum(q_sum[:, nope_dev + rope_dev :], axis=1, keepdims=True)
    scale_in = lax.rsqrt(square_sum / model_width + EPS)
    q_nope = (q_sum[:, :nope_dev] * scale_in).astype(BF).reshape(rows, heads, nope)
    q_rope = rotate(
        (q_sum[:, nope_dev : nope_dev + rope_dev] * scale_in).reshape(rows, heads, rope), context
    ).astype(BF)
    latent_sum = own_sum[:, :latent]
    own_scale = lax.rsqrt(
        jnp.sum(own_sum[:, latent + rope :], axis=1, keepdims=True) / model_width + EPS
    )
    new_latent = (
        latent_sum
        * lax.rsqrt(jnp.mean(latent_sum * latent_sum, axis=1, keepdims=True) + EPS)
        * latent_gain.astype(F32)[None, :]
    ).astype(BF)
    new_rope_key = rotate(own_sum[:, latent : latent + rope] * own_scale, context).astype(BF)
    q_lat = jnp.einsum("bhd,chd->bhc", q_nope, key_up, preferred_element_type=F32).astype(BF)

    query = jnp.concatenate([q_lat, q_rope], axis=-1).reshape(own, nt, heads, latent + rope)
    query = lax.all_to_all(query.swapaxes(0, 1), "tp", 0, 0, tiled=True)
    query = query.transpose(1, 0, 2, 3).reshape(own, nt * heads, latent + rope)
    all_heads = nt * heads
    seq_lat, seq_rope = query[..., :latent], query[..., latent:]
    scores = (
        jnp.einsum("bhc,bpc->bhp", seq_lat, cache_latent, preferred_element_type=F32)
        + jnp.einsum("bhr,bpr->bhp", seq_rope, cache_rope_key, preferred_element_type=F32)
    ) * score_scale
    own_score = (
        jnp.einsum("bhc,bc->bh", seq_lat, new_latent, preferred_element_type=F32)
        + jnp.einsum("bhr,br->bh", seq_rope, new_rope_key, preferred_element_type=F32)
    ) * score_scale
    peak = jnp.maximum(jnp.max(scores, axis=2), own_score)
    probs = jnp.exp(scores - peak[:, :, None])
    own_prob = jnp.where(kv_index == 0, jnp.exp(own_score - peak), 0.0)
    totals = jnp.sum(probs, axis=2) + own_prob
    partial_value = (
        jnp.einsum("bhp,bpc->bhc", probs.astype(BF), cache_latent, preferred_element_type=F32)
        + own_prob[:, :, None] * new_latent.astype(F32)[:, None, :]
    )
    packed = jnp.concatenate(
        [partial_value.astype(BF)]
        + [p[:, :, None] for p in pieces(peak, 3) + pieces(totals, 3)]
        + [jnp.zeros((own, all_heads, 122), BF)],
        axis=2,
    )

    def combine(blocks):
        stats = blocks[..., latent:].astype(F32)
        peaks = jnp.sum(stats[..., :3], axis=-1, keepdims=True)
        sums = jnp.sum(stats[..., 3:6], axis=-1, keepdims=True)
        factor = jnp.exp(peaks - jnp.max(peaks, axis=0, keepdims=True))
        value = jnp.sum(blocks[..., :latent].astype(F32) * factor, axis=0)
        return (value / jnp.sum(sums * factor, axis=0)).astype(BF)

    if split_rows:
        per = own // nk
        sent = packed.reshape(nk, per, nt, heads, latent + 128).swapaxes(1, 2)
        sent = sent.reshape(nk * nt, per, heads, latent + 128)
        got = lax.all_to_all(sent, ("kv", "tp"), 0, 0, tiled=True)
        got = got.reshape(nk, nt, per, heads, latent + 128)
        o_lat = combine(got).swapaxes(0, 1).reshape(per * nt, heads, latent)
    else:
        flat = own * all_heads // nk
        got = lax.all_to_all(packed.reshape(nk, flat, latent + 128), "kv", 0, 0, tiled=True)
        o_own = spread(combine(got), "kv").reshape(own, nt, heads, latent)
        o_lat = lax.all_to_all(o_own.swapaxes(0, 1), "tp", 0, 0, tiled=True)
        o_lat = o_lat.swapaxes(0, 1).reshape(rows, heads, latent)
    o_heads = jnp.einsum("bhc,che->bhe", o_lat, value_up, preferred_element_type=F32).astype(BF)
    o_flat = o_heads.reshape(-1, heads * value_width)
    if split_rows:
        o_flat = spread(o_flat, "kv").reshape(rows, heads * value_width)

    core = lax.rem(tp_index, 2)
    swap = [(i, i ^ 1) for i in range(nt)]
    column = [list(range(c, nt, 2)) for c in range(2)]
    half = width // 2
    out_part = dot(o_flat, w_out).reshape(rows, 2, half)
    keep = jnp.where(core == 0, out_part[:, 0], out_part[:, 1])
    give = jnp.where(core == 0, out_part[:, 1], out_part[:, 0]).astype(BF)
    pair_sum = (keep + lax.ppermute(give, "tp", swap).astype(F32)).astype(BF)
    att_half = jnp.sum(spread(pair_sum, "tp", column).astype(F32), axis=0).astype(BF)
    att_other = lax.ppermute(att_half, "tp", swap)
    attended = jnp.where(
        core == 0,
        jnp.concatenate([att_half, att_other], axis=1),
        jnp.concatenate([att_other, att_half], axis=1),
    ).astype(F32)

    gain_m = block_of(mlp_gain)
    post = attended * block_of(post_gain)
    stacked = jnp.concatenate(
        [(gathered_float * gain_m).astype(BF), (post * gain_m).astype(BF)], axis=0
    )
    ff_dev = w_gate.shape[1]
    stats = [
        jnp.sum(a * b, axis=1, keepdims=True)
        for a, b in (
            (attended, attended),
            (gathered_float, gathered_float),
            (gathered_float, post),
            (post, post),
        )
    ]
    stat_block = jnp.concatenate(
        [jnp.concatenate(pieces(jnp.concatenate(stats[2 * i : 2 * i + 2], axis=0), 2), axis=1)
         for i in range(2)],
        axis=1,
    )
    ff_part = jnp.concatenate(
        [
            dot(stacked, w_gate).astype(BF),
            dot(stacked, w_up).astype(BF),
            stat_block,
        ],
        axis=1,
    )
    ff_sum = jnp.sum(spread(ff_part, "kv").astype(F32), axis=0)
    first = jnp.sum(ff_sum[:, 2 * ff_dev : 2 * ff_dev + 2], axis=1, keepdims=True)
    second = jnp.sum(ff_sum[:, 2 * ff_dev + 2 :], axis=1, keepdims=True)
    att_square, resid_square, cross, post_square = (
        first[:rows],
        first[rows:],
        second[:rows],
        second[rows:],
    )
    s = lax.rsqrt(att_square / model_width + EPS)
    mid_square = resid_square + 2.0 * s * cross + s * s * post_square
    scale_mid = lax.rsqrt(jnp.maximum(mid_square, 0.0) / model_width + EPS)
    mixed = (ff_sum[:rows] + s * ff_sum[rows:]) * scale_mid
    hidden = (jax.nn.silu(mixed[:, :ff_dev]) * mixed[:, ff_dev : 2 * ff_dev]).astype(BF)
    down = dot(hidden, w_down).astype(BF).reshape(own, nt, width).swapaxes(0, 1)
    lowered = jnp.sum(lax.all_to_all(down, "tp", 0, 0, tiled=True).astype(F32), axis=0)

    own_post = lax.dynamic_slice_in_dim(post.reshape(own, nt, width), tp_index, 1, 1)[:, 0]
    own_s = lax.dynamic_slice_in_dim(s.reshape(own, nt, 1), tp_index, 1, 1)[:, 0]
    resid_mid = (resid.astype(F32) + own_s * own_post).astype(BF).astype(F32)
    next_resid = (resid_mid + lowered).astype(BF)
    return (next_resid, new_latent, new_rope_key)


VMEM = pl.BlockSpec(memory_space=pltpu.VMEM)
WAIT = 4_000_000_000
NT = (((1,), (1,)), ((), ()))


def call(kernel, outs, *args, flops=0, scratch=()):
    many = isinstance(outs, (list, tuple))
    sizes = list(args) + (list(outs) if many else [outs])
    moved = sum(int(np.prod(a.shape)) * a.dtype.itemsize for a in sizes)
    return pl.pallas_call(
        kernel,
        out_shape=outs,
        in_specs=[VMEM] * len(args),
        out_specs=[VMEM] * len(outs) if many else VMEM,
        scratch_shapes=list(scratch),
        compiler_params=pltpu.CompilerParams(vmem_limit_bytes=16 << 20),
        cost_estimate=pl.CostEstimate(
            flops=max(flops, moved), bytes_accessed=moved, transcendentals=0
        ),
    )(*args)


def like(shape, dtype=BF):
    return jax.ShapeDtypeStruct(shape, dtype)


def lane_of(shape):
    return lax.broadcasted_iota(jnp.int32, shape, len(shape) - 1)


def terms(value, count):
    out, rest = [], value
    for _ in range(count):
        term = rest.astype(BF).astype(F32)
        out.append(term)
        rest = rest - term
    return out


def placed(columns, shape):
    lane = lane_of(shape)
    block = jnp.zeros(shape, F32)
    for at, column in columns:
        block = jnp.where(lane == at, column, block)
    return block


def picked(block, first, count):
    lane = lane_of(block.shape)
    inside = (lane >= first) & (lane < first + count)
    return jnp.sum(jnp.where(inside, block, 0.0), axis=-1, keepdims=True)


def turned(vector, table, half):
    width = vector.shape[1]
    low = lax.rem(lane_of(vector.shape), 2 * half) < half
    other = jnp.where(
        low, pltpu.roll(vector, width - half, 1), pltpu.roll(vector, half, 1)
    )
    return vector * table[0:1, :width] + other * table[1:2, :width]


def other(axis, k, step=1):
    return jnp.bitwise_xor(lax.div(lax.axis_index(axis), step), k)


def start_kernel(resid_ref, got_ref, out_ref):
    first = lax.rem(lax.axis_index("tp"), 2) == 0
    mine, theirs = resid_ref[...].astype(F32), got_ref[...].astype(F32)
    out_ref[...] = jnp.concatenate(
        [jnp.where(first, mine, theirs), jnp.where(first, theirs, mine)], axis=0
    ).astype(BF)


def query_kernel(
    b0, b1, b2, b3, resid_ref, ga_ref, gp_ref, gm_ref, wn_ref, wr_ref, wl_ref, wk_ref,
    m0, m1, m2, m3, rows_ref, gains_ref, held_ref, sent_ref,
):
    own, width = resid_ref.shape
    chips = held_ref.shape[0]
    nt = 2 * chips
    latent = wl_ref.shape[1]
    rope = wk_ref.shape[0]
    nope_dev, rope_dev = wn_ref.shape[1], wr_ref.shape[1]
    for k, ref in enumerate((b0, b1, b2, b3)):
        held_ref[other("tp", k, 2)] = ref[...].astype(F32)
    x = jnp.concatenate(
        [
            held_ref[z, c * own + r : c * own + r + 1, :]
            for r in range(own)
            for z in range(chips)
            for c in range(2)
        ],
        axis=0,
    )
    rows_ref[...] = x.astype(BF)
    tiles = width // 128
    at = pl.multiple_of(lax.axis_index("kv") * tiles, tiles)
    gains = []
    for ref in (ga_ref, gp_ref, gm_ref):
        block = ref[pl.ds(at, tiles), :].astype(F32)
        gains.append(jnp.concatenate([block[i : i + 1] for i in range(tiles)], axis=1))
    gain = gains[0]
    gains_ref[...] = jnp.concatenate(gains + [jnp.zeros((8 - len(gains), width), F32)], axis=0)
    normed = (x * gain).astype(BF)
    qn = jnp.dot(normed, wn_ref[...], preferred_element_type=F32)
    qr = jnp.dot(normed, wr_ref[...], preferred_element_type=F32)
    square = jnp.sum(x * x, axis=1, keepdims=True)
    mine = jnp.concatenate([resid_ref[...].astype(F32), jnp.zeros((nt - own, width), F32)], axis=0)
    own_square = jnp.sum(mine * mine, axis=1, keepdims=True)
    own_normed = (mine * gain).astype(BF)
    lat = jnp.dot(own_normed, wl_ref[...], preferred_element_type=F32)
    at = pl.multiple_of(lax.axis_index("kv") * width, width)
    key = lax.dot_general(own_normed, wk_ref[:, pl.ds(at, width)], NT, preferred_element_type=F32)
    half = latent // 2
    lat = lat[:, :half] + pltpu.roll(lat[:, half:], own, 0)
    key = jnp.concatenate([key, jnp.zeros((nt, 128 - rope), F32)], axis=1)
    own_terms = terms(own_square, 2)
    for r in range(sent_ref.shape[0]):
        part = slice(r * nt, (r + 1) * nt)
        sent_ref[r, :, :nope_dev] = qn[part].astype(BF)
        sent_ref[r, :, nope_dev : nope_dev + rope_dev] = qr[part].astype(BF)
        base = nope_dev + rope_dev
        sent_ref[r, :, base : base + half] = lat.astype(BF)
        columns = [(rope + i, c) for i, c in enumerate(own_terms + terms(square[part], 2))]
        stat = placed(columns, key.shape)
        sent_ref[r, :, base + half :] = jnp.where(lane_of(key.shape) < rope, key, stat).astype(BF)
    for k, ref in enumerate((m0, m1, m2, m3)):
        ref[...] = sent_ref[other("kv", k)]


def four(refs):
    a, b, c, d = (ref[...].astype(F32) for ref in refs)
    return (a + b) + (c + d)


def latent_kernel(
    model_width, b0, b1, b2, b3, ku_ref, gain_ref, table_ref, msg_ref, lat_ref, key_ref, own_ref
):
    nk, nt = msg_ref.shape[0], b0.shape[0]
    latent, heads, nope = ku_ref.shape
    nope_dev = heads * nope
    own, rope = key_ref.shape
    rope_dev = heads * rope
    total = four((b0, b1, b2, b3))
    base, half = nope_dev + rope_dev, latent // 2
    stat = total[:, base + half :]
    scale = lax.rsqrt(picked(stat, rope + 2, 2) / model_width + EPS)
    own_scale = lax.rsqrt(picked(stat, rope, 2) / model_width + EPS)
    lat = total[:, base : base + half]
    lat = jnp.concatenate([lat, pltpu.roll(lat, own, 0)], axis=1)
    lat = lat * lax.rsqrt(jnp.mean(lat * lat, axis=1, keepdims=True) + EPS)
    lat = (lat * gain_ref[...].astype(F32)).astype(BF)
    table = table_ref[...]
    key = turned(stat * own_scale, table, rope // 2).astype(BF)
    lat_ref[...] = lat[:own]
    key_ref[...] = key[:own, :rope]
    own_ref[:, :latent] = lat.astype(F32)
    own_ref[:, latent:] = key.astype(F32)
    qn = (total[:, :nope_dev] * scale).astype(BF).astype(F32)
    qr = turned(total[:, nope_dev:base] * scale, table, rope // 2).astype(BF).astype(F32)

    def diagonal(q, size):
        shape = (nt, heads, heads * size)
        head = lax.broadcasted_iota(jnp.int32, shape, 1)
        lane = lax.broadcasted_iota(jnp.int32, shape, 2)
        keep = (lane >= head * size) & (lane < (head + 1) * size)
        spread_q = jnp.broadcast_to(q[:, None, :], shape)
        return jnp.where(keep, spread_q, 0.0).reshape(nt * heads, heads * size).astype(BF)

    q_lat = lax.dot_general(
        diagonal(qn, nope), ku_ref[...].reshape(latent, nope_dev), NT, preferred_element_type=F32
    ).astype(BF)
    shape = (rope_dev, 128)
    row = lax.rem(lax.broadcasted_iota(jnp.int32, shape, 0), rope)
    unit = jnp.where(row == lane_of(shape), 1.0, 0.0).astype(BF)
    q_rope = jnp.dot(diagonal(qr, rope), unit, preferred_element_type=F32).astype(BF)
    for j in range(nk):
        msg_ref[j, :, :latent] = q_lat
        msg_ref[j, :, latent:] = q_rope


def attend_kernel(score_scale, q_ref, cache_ref, rope_ref, own_ref, msg_ref):
    own, all_heads, _ = q_ref.shape
    latent = cache_ref.shape[2]
    rope = rope_ref.shape[1]
    holds_own = lax.axis_index("kv") == 0
    lat, key = own_ref[:, :latent], own_ref[:, latent : latent + rope]
    for r in range(own):
        q_lat = q_ref[r, :, :latent]
        q_rope = q_ref[r, :, latent : latent + rope]
        keys = cache_ref[r]
        scores = (
            lax.dot_general(q_lat, keys, NT, preferred_element_type=F32)
            + jnp.dot(q_rope, rope_ref[r], preferred_element_type=F32)
        ) * score_scale
        own_score = (
            jnp.sum(q_lat.astype(F32) * lat[r : r + 1], axis=1, keepdims=True)
            + jnp.sum(q_rope.astype(F32) * key[r : r + 1], axis=1, keepdims=True)
        ) * score_scale
        peak = jnp.maximum(jnp.max(scores, axis=1, keepdims=True), own_score)
        probs = jnp.exp(scores - peak)
        own_prob = jnp.where(holds_own, jnp.exp(own_score - peak), 0.0)
        total = jnp.sum(probs, axis=1, keepdims=True) + own_prob
        value = jnp.dot(probs.astype(BF), keys, preferred_element_type=F32)
        msg_ref[r, :, :latent] = (value + own_prob * lat[r : r + 1]).astype(BF)
        columns = list(enumerate(terms(peak, 3) + terms(total, 3)))
        msg_ref[r, :, latent:] = placed(columns, (all_heads, 128)).astype(BF)


def value_kernel(got_ref, vu_ref, out_ref):
    nk, pairs, _ = got_ref.shape
    latent, heads, size = vu_ref.shape
    value_dev = heads * size
    nt = pairs // heads
    stats = [got_ref[j, :, latent:].astype(F32) for j in range(nk)]
    peaks = [picked(s, 0, 3) for s in stats]
    peak = functools.reduce(jnp.maximum, peaks)
    factors = [jnp.exp(p - peak) for p in peaks]
    total = sum(picked(s, 3, 3) * f for s, f in zip(stats, factors))
    value = sum(got_ref[j, :, :latent].astype(F32) * f for j, f in enumerate(factors))
    o_lat = (value / total).astype(BF)
    full = jnp.dot(o_lat, vu_ref[...].reshape(latent, value_dev), preferred_element_type=F32)
    shape = (nt, heads, value_dev)
    head = lax.broadcasted_iota(jnp.int32, shape, 1)
    lane = lax.broadcasted_iota(jnp.int32, shape, 2)
    keep = (lane >= head * size) & (lane < (head + 1) * size)
    out_ref[...] = jnp.sum(jnp.where(keep, full.reshape(shape), 0.0), axis=1).astype(BF)


def out_kernel(b0, b1, b2, b3, w_ref, keep_ref, give_ref, held_ref):
    half = keep_ref.shape[1]
    for k, ref in enumerate((b0, b1, b2, b3)):
        held_ref[other("kv", k)] = ref[...].astype(F32)
    first = lax.rem(lax.axis_index("tp"), 2) == 0
    o_heads = held_ref[...].reshape(keep_ref.shape[0], w_ref.shape[0]).astype(BF)
    out = jnp.dot(o_heads, w_ref[...], preferred_element_type=F32)
    keep_ref[...] = jnp.where(first, out[:, :half], out[:, half:])
    give_ref[...] = jnp.where(first, out[:, half:], out[:, :half]).astype(BF)


def pair_kernel(keep_ref, got_ref, out_ref):
    out_ref[...] = (keep_ref[...] + got_ref[...].astype(F32)).astype(BF)


def column_kernel(b0, b1, b2, b3, out_ref):
    out_ref[...] = four((b0, b1, b2, b3)).astype(BF)


def gate_kernel(
    half_ref, other_ref, rows_ref, gains_ref, wg_ref, wu_ref, m0, m1, m2, m3, post_ref, msg_ref
):
    nk, both, _ = msg_ref.shape
    rows = both // 2
    ff_dev = wg_ref.shape[0]
    chunk = (msg_ref.shape[2] - 128) // 2
    first = lax.rem(lax.axis_index("tp"), 2) == 0
    mine, theirs = half_ref[...].astype(F32), other_ref[...].astype(F32)
    att = jnp.concatenate(
        [jnp.where(first, mine, theirs), jnp.where(first, theirs, mine)], axis=1
    )
    x = rows_ref[...].astype(F32)
    post = att * gains_ref[1:2, :]
    post_ref[...] = post
    gain = gains_ref[2:3, :]
    stacked = jnp.concatenate([x * gain, post * gain], axis=0).astype(BF)

    def added(a, b):
        return jnp.sum(a * b, axis=1, keepdims=True)

    top = terms(added(att, att), 2) + terms(added(x, post), 2)
    low = terms(added(x, x), 2) + terms(added(post, post), 2)
    stat = placed(
        [(i, jnp.concatenate([a, b], axis=0)) for i, (a, b) in enumerate(zip(top, low))],
        (both, 128),
    ).astype(BF)
    for k, w_ref in enumerate((wg_ref, wu_ref)):
        part = lax.dot_general(stacked, w_ref[...], NT, preferred_element_type=F32)
        for j in range(nk):
            lo, hi = j * chunk, min((j + 1) * chunk, ff_dev)
            size = max(hi - lo, 0)
            if size < chunk:
                msg_ref[j, :, k * chunk : (k + 1) * chunk] = jnp.zeros((both, chunk), BF)
            if size > 0:
                msg_ref[j, :, k * chunk : k * chunk + size] = part[:, lo:hi].astype(BF)
    for j in range(nk):
        msg_ref[j, :, 2 * chunk :] = stat
    for k, ref in enumerate((m0, m1, m2, m3)):
        ref[...] = msg_ref[other("kv", k)]


def hidden_kernel(model_width, b0, b1, b2, b3, out_ref, s_ref):
    rows, chunk = out_ref.shape
    total = four((b0, b1, b2, b3))
    stat = total[:, 2 * chunk :]
    one, two = picked(stat, 0, 2), picked(stat, 2, 2)
    att_square, x_square, cross, post_square = one[:rows], one[rows:], two[:rows], two[rows:]
    s = lax.rsqrt(att_square / model_width + EPS)
    mid = jnp.maximum(x_square + 2.0 * s * cross + s * s * post_square, 0.0)
    scale = lax.rsqrt(mid / model_width + EPS)
    s_ref[...] = jnp.broadcast_to(s, s_ref.shape)
    mixed = (total[:rows, : 2 * chunk] + s * total[rows:, : 2 * chunk]) * scale
    gate, up = mixed[:, :chunk], mixed[:, chunk:]
    out_ref[...] = (gate / (1.0 + jnp.exp(-gate)) * up).astype(BF)


def down_kernel(b0, b1, b2, b3, w_ref, msg_ref, held_ref):
    nk, rows, chunk = held_ref.shape
    for k, ref in enumerate((b0, b1, b2, b3)):
        held_ref[other("kv", k)] = ref[...]
    ff_dev = w_ref.shape[0]
    nt, own, _ = msg_ref.shape
    total = None
    for j in range(nk):
        lo, hi = j * chunk, min((j + 1) * chunk, ff_dev)
        if hi > lo:
            part = jnp.dot(
                held_ref[j, :, : hi - lo], w_ref[lo:hi, :], preferred_element_type=F32
            )
            total = part if total is None else total + part
    total = total.reshape(own, nt, total.shape[1])
    for t in range(nt):
        msg_ref[t] = total[:, t, :].astype(BF)


def last_kernel(got_ref, resid_ref, post_ref, s_ref, out_ref):
    nt, own, width = got_ref.shape
    total = got_ref[0].astype(F32)
    for t in range(1, nt):
        total = total + got_ref[t].astype(F32)
    added = (post_ref[...] * s_ref[:, 0:1]).reshape(own, nt, width)
    here = lax.broadcasted_iota(jnp.int32, added.shape, 1) == lax.axis_index("tp")
    mine = jnp.sum(jnp.where(here, added, 0.0), axis=1)
    mid = (resid_ref[...].astype(F32) + mine).astype(BF).astype(F32)
    out_ref[...] = (mid + total).astype(BF)


def exchange(message, axis):
    return lax.all_to_all(message, axis, 0, 0, tiled=True)


def deal(blocks, axis, step=1):
    size = lax.axis_size(axis)
    return [blocks[0]] + [
        lax.ppermute(blocks[k], axis, [(i, i ^ (k * step)) for i in range(size)])
        for k in range(1, len(blocks))
    ]


def kernel_body(
    resid,
    attn_gain,
    w_query_nope,
    w_query_rope,
    w_latent,
    w_key_rope,
    latent_gain,
    key_up,
    value_up,
    w_out,
    post_gain,
    mlp_gain,
    w_gate,
    w_up,
    w_down,
    cache_latent,
    cache_rope_key,
):
    nk = lax.axis_size("kv")
    nt = lax.axis_size("tp")
    own, width = resid.shape
    rows = own * nt
    model_width = width * nk
    latent, heads, nope = key_up.shape
    rope = cache_rope_key.shape[2]
    nope_dev, rope_dev = heads * nope, heads * rope
    ff_dev = w_gate.shape[1]
    context = cache_latent.shape[1] * nk
    half_rope = rope // 2
    angles = context * THETA ** (-np.arange(half_rope) / half_rope)
    cos, sin = np.cos(angles), np.sin(angles)
    table = np.zeros((8, rope_dev), np.float32)
    table[0] = np.tile(np.concatenate([cos, cos]), heads)
    table[1] = np.tile(np.concatenate([-sin, sin]), heads)

    swap = [(i, i ^ 1) for i in range(nt)]
    both = call(start_kernel, like((nt, width)), resid, lax.ppermute(resid, "tp", swap), flops=WAIT)
    chips = nt // 2
    sent_width = nope_dev + rope_dev + latent // 2 + 128
    *msg, x_rows, gains = call(
        query_kernel,
        [like((nt, sent_width))] * nk + [like((rows, width)), like((8, width), F32)],
        *deal([both] * chips, "tp", 2),
        resid,
        *[g.reshape(-1, 128) for g in (attn_gain, post_gain, mlp_gain)],
        w_query_nope,
        w_query_rope,
        w_latent,
        w_key_rope.T,
        scratch=[pltpu.VMEM((chips, 2 * own, width), F32), pltpu.VMEM((nk, nt, sent_width), BF)],
        flops=WAIT,
    )
    pairs = nt * heads
    msg, new_latent, new_rope_key, own_block = call(
        functools.partial(latent_kernel, model_width),
        [
            like((nk, pairs, latent + 128)),
            like((own, latent)),
            like((own, rope)),
            like((nt, latent + 128), F32),
        ],
        *deal(msg, "kv"),
        key_up,
        latent_gain.reshape(1, latent),
        jnp.asarray(table),
        flops=WAIT,
    )
    got = exchange(msg.reshape(nk * nt, heads, latent + 128), ("kv", "tp"))
    msg = call(
        functools.partial(attend_kernel, (nope + rope) ** (-0.5)),
        like((own, pairs, latent + 128)),
        got.reshape(own, pairs, latent + 128),
        cache_latent,
        cache_rope_key.swapaxes(1, 2),
        own_block,
        flops=WAIT,
    )
    got = exchange(msg.reshape(nk * nt, heads, latent + 128), ("kv", "tp"))
    value_dev = heads * value_up.shape[2]
    o_heads = call(
        value_kernel,
        like((nt, value_dev)),
        got.reshape(nk, pairs, latent + 128),
        value_up,
        flops=WAIT,
    )
    half = width // 2
    keep, give = call(
        out_kernel,
        [like((rows, half), F32), like((rows, half))],
        *deal([o_heads] * nk, "kv"),
        w_out,
        scratch=[pltpu.VMEM((nk, nt, value_dev), F32)],
        flops=WAIT,
    )
    pair = call(
        pair_kernel, like((rows, half)), keep, lax.ppermute(give, "tp", swap), flops=WAIT
    )
    att_half = call(
        column_kernel, like((rows, half)), *deal([pair] * chips, "tp", 2), flops=WAIT
    )
    att_other = lax.ppermute(att_half, "tp", swap)
    chunk = -(-ff_dev // (nk * 128)) * 128
    sent_width = 2 * chunk + 128
    *msg, post = call(
        gate_kernel,
        [like((2 * rows, sent_width))] * nk + [like((rows, width), F32)],
        att_half,
        att_other,
        x_rows,
        gains,
        w_gate.T,
        w_up.T,
        scratch=[pltpu.VMEM((nk, 2 * rows, sent_width), BF)],
        flops=WAIT,
    )
    hidden, s = call(
        functools.partial(hidden_kernel, model_width),
        [like((rows, chunk)), like((rows, 128), F32)],
        *deal(msg, "kv"),
        flops=WAIT,
    )
    msg = call(
        down_kernel,
        like((nt, own, width)),
        *deal([hidden] * nk, "kv"),
        w_down,
        scratch=[pltpu.VMEM((nk, rows, chunk), BF)],
        flops=WAIT,
    )
    got = exchange(msg, "tp")
    next_resid = call(last_kernel, like((own, width)), got, resid, post, s)
    return (next_resid, new_latent, new_rope_key)


def body(*args):
    resid, key_up, cache = args[0], args[7], args[15]
    nk, nt = lax.axis_size("kv"), lax.axis_size("tp")
    own, width = resid.shape
    latent, heads, nope = key_up.shape
    fits = (
        own == nk == 4
        and nt == 8
        and heads == 8
        and 2 * own == nt
        and width % 1024 == 0
        and latent % 256 == 0
        and nope % 128 == 0
        and cache.shape[1] % 128 == 0
        and args[16].shape[2] == 64
    )
    return kernel_body(*args) if fits else plain_body(*args)


def solution(mesh):
    return jax.shard_map(
        body,
        mesh=mesh,
        in_specs=(
            P("tp", "kv"),
            P(),
            P("kv", "tp"),
            P("kv", "tp"),
            P("kv", None),
            P(),
            P(),
            P(None, "tp", None),
            P(None, "tp", None),
            P("tp", "kv"),
            P(),
            P(),
            P("kv", "tp"),
            P("kv", "tp"),
            P("tp", "kv"),
            P("tp", "kv", None),
            P("tp", "kv", None),
        ),
        out_specs=(P("tp", "kv"), P("tp", None), P("tp", None)),
        check_vma=False,
    )
```

```python
import functools

import jax
import jax.numpy as jnp
import numpy as np
from jax import lax
from jax.experimental import pallas as pl
from jax.experimental.pallas import tpu as pltpu
from jax.sharding import PartitionSpec as P


EPS = 1e-06
THETA = 10000.0
BF = jnp.bfloat16
F32 = jnp.float32


def rotate(vector, position):
    half_width = vector.shape[-1] // 2
    frequency = THETA ** (-jnp.arange(half_width, dtype=F32) / half_width)
    angles = jnp.asarray(position, F32) * frequency
    cos_table, sin_table = (jnp.cos(angles), jnp.sin(angles))
    lower_half, upper_half = (vector[..., :half_width], vector[..., half_width:])
    return jnp.concatenate(
        [
            lower_half * cos_table - upper_half * sin_table,
            lower_half * sin_table + upper_half * cos_table,
        ],
        axis=-1,
    )


def dot(a, b):
    return jnp.dot(a, b, preferred_element_type=F32)


def pieces(value, count):
    out, rest = [], value
    for _ in range(count):
        term = lax.reduce_precision(rest, 8, 7)
        out.append(term.astype(BF))
        rest = rest - term
    return out


def spread(block, axis, groups=None):
    count = len(groups[0]) if groups else lax.axis_size(axis)
    copies = jnp.broadcast_to(block[None], (count,) + block.shape)
    return lax.all_to_all(copies, axis, 0, 0, tiled=True, axis_index_groups=groups)


def plain_body(
    resid,
    attn_gain,
    w_query_nope,
    w_query_rope,
    w_latent,
    w_key_rope,
    latent_gain,
    key_up,
    value_up,
    w_out,
    post_gain,
    mlp_gain,
    w_gate,
    w_up,
    w_down,
    cache_latent,
    cache_rope_key,
):
    nk = lax.axis_size("kv")
    nt = lax.axis_size("tp")
    kv_index = lax.axis_index("kv")
    tp_index = lax.axis_index("tp")
    own, width = resid.shape
    rows = own * nt
    model_width = width * nk
    latent, heads, nope = key_up.shape
    value_width = value_up.shape[2]
    rope = cache_rope_key.shape[2]
    pos_dev = cache_latent.shape[1]
    context = pos_dev * nk
    score_scale = (nope + rope) ** (-0.5)
    col_start = kv_index * width
    split_rows = own % nk == 0

    def block_of(vector):
        return lax.dynamic_slice_in_dim(vector, col_start, width, 0).astype(F32)[None, :]

    gathered = spread(resid, "tp").swapaxes(0, 1).reshape(rows, width)
    gathered_float = gathered.astype(F32)
    gain_a = block_of(attn_gain)
    normed_a = (gathered_float * gain_a).astype(BF)
    own_normed = (resid.astype(F32) * gain_a).astype(BF)
    key_rows = lax.dynamic_slice_in_dim(w_key_rope, col_start, width, 0)
    squares = jnp.sum(gathered_float * gathered_float, axis=1, keepdims=True)
    own_squares = jnp.sum(resid.astype(F32) ** 2, axis=1, keepdims=True)
    q_part = jnp.concatenate(
        [
            dot(normed_a, w_query_nope).astype(BF),
            dot(normed_a, w_query_rope).astype(BF),
            *pieces(squares, 2),
            jnp.zeros((rows, 126), BF),
        ],
        axis=1,
    )
    own_part = jnp.concatenate(
        [
            dot(own_normed, w_latent).astype(BF),
            dot(own_normed, key_rows).astype(BF),
            *pieces(own_squares, 2),
        ],
        axis=1,
    )
    nope_dev, rope_dev = heads * nope, heads * rope
    q_width, own_width = q_part.shape[1], own_part.shape[1]
    sent_width = max(q_width, own_width)
    q_part = jnp.pad(q_part, ((0, 0), (0, sent_width - q_width)))
    own_part = jnp.pad(own_part, ((0, 0), (0, sent_width - own_width)))
    summed = jnp.sum(
        spread(jnp.concatenate([q_part, own_part], axis=0), "kv").astype(F32), axis=0
    )
    q_sum, own_sum = summed[:rows], summed[rows:, :own_width]
    square_sum = jnp.sum(q_sum[:, nope_dev + rope_dev :], axis=1, keepdims=True)
    scale_in = lax.rsqrt(square_sum / model_width + EPS)
    q_nope = (q_sum[:, :nope_dev] * scale_in).astype(BF).reshape(rows, heads, nope)
    q_rope = rotate(
        (q_sum[:, nope_dev : nope_dev + rope_dev] * scale_in).reshape(rows, heads, rope), context
    ).astype(BF)
    latent_sum = own_sum[:, :latent]
    own_scale = lax.rsqrt(
        jnp.sum(own_sum[:, latent + rope :], axis=1, keepdims=True) / model_width + EPS
    )
    new_latent = (
        latent_sum
        * lax.rsqrt(jnp.mean(latent_sum * latent_sum, axis=1, keepdims=True) + EPS)
        * latent_gain.astype(F32)[None, :]
    ).astype(BF)
    new_rope_key = rotate(own_sum[:, latent : latent + rope] * own_scale, context).astype(BF)
    q_lat = jnp.einsum("bhd,chd->bhc", q_nope, key_up, preferred_element_type=F32).astype(BF)

    query = jnp.concatenate([q_lat, q_rope], axis=-1).reshape(own, nt, heads, latent + rope)
    query = lax.all_to_all(query.swapaxes(0, 1), "tp", 0, 0, tiled=True)
    query = query.transpose(1, 0, 2, 3).reshape(own, nt * heads, latent + rope)
    all_heads = nt * heads
    seq_lat, seq_rope = query[..., :latent], query[..., latent:]
    scores = (
        jnp.einsum("bhc,bpc->bhp", seq_lat, cache_latent, preferred_element_type=F32)
        + jnp.einsum("bhr,bpr->bhp", seq_rope, cache_rope_key, preferred_element_type=F32)
    ) * score_scale
    own_score = (
        jnp.einsum("bhc,bc->bh", seq_lat, new_latent, preferred_element_type=F32)
        + jnp.einsum("bhr,br->bh", seq_rope, new_rope_key, preferred_element_type=F32)
    ) * score_scale
    peak = jnp.maximum(jnp.max(scores, axis=2), own_score)
    probs = jnp.exp(scores - peak[:, :, None])
    own_prob = jnp.where(kv_index == 0, jnp.exp(own_score - peak), 0.0)
    totals = jnp.sum(probs, axis=2) + own_prob
    partial_value = (
        jnp.einsum("bhp,bpc->bhc", probs.astype(BF), cache_latent, preferred_element_type=F32)
        + own_prob[:, :, None] * new_latent.astype(F32)[:, None, :]
    )
    packed = jnp.concatenate(
        [partial_value.astype(BF)]
        + [p[:, :, None] for p in pieces(peak, 3) + pieces(totals, 3)]
        + [jnp.zeros((own, all_heads, 122), BF)],
        axis=2,
    )

    def combine(blocks):
        stats = blocks[..., latent:].astype(F32)
        peaks = jnp.sum(stats[..., :3], axis=-1, keepdims=True)
        sums = jnp.sum(stats[..., 3:6], axis=-1, keepdims=True)
        factor = jnp.exp(peaks - jnp.max(peaks, axis=0, keepdims=True))
        value = jnp.sum(blocks[..., :latent].astype(F32) * factor, axis=0)
        return (value / jnp.sum(sums * factor, axis=0)).astype(BF)

    if split_rows:
        per = own // nk
        sent = packed.reshape(nk, per, nt, heads, latent + 128).swapaxes(1, 2)
        sent = sent.reshape(nk * nt, per, heads, latent + 128)
        got = lax.all_to_all(sent, ("kv", "tp"), 0, 0, tiled=True)
        got = got.reshape(nk, nt, per, heads, latent + 128)
        o_lat = combine(got).swapaxes(0, 1).reshape(per * nt, heads, latent)
    else:
        flat = own * all_heads // nk
        got = lax.all_to_all(packed.reshape(nk, flat, latent + 128), "kv", 0, 0, tiled=True)
        o_own = spread(combine(got), "kv").reshape(own, nt, heads, latent)
        o_lat = lax.all_to_all(o_own.swapaxes(0, 1), "tp", 0, 0, tiled=True)
        o_lat = o_lat.swapaxes(0, 1).reshape(rows, heads, latent)
    o_heads = jnp.einsum("bhc,che->bhe", o_lat, value_up, preferred_element_type=F32).astype(BF)
    o_flat = o_heads.reshape(-1, heads * value_width)
    if split_rows:
        o_flat = spread(o_flat, "kv").reshape(rows, heads * value_width)

    core = lax.rem(tp_index, 2)
    swap = [(i, i ^ 1) for i in range(nt)]
    column = [list(range(c, nt, 2)) for c in range(2)]
    half = width // 2
    out_part = dot(o_flat, w_out).reshape(rows, 2, half)
    keep = jnp.where(core == 0, out_part[:, 0], out_part[:, 1])
    give = jnp.where(core == 0, out_part[:, 1], out_part[:, 0]).astype(BF)
    pair_sum = (keep + lax.ppermute(give, "tp", swap).astype(F32)).astype(BF)
    att_half = jnp.sum(spread(pair_sum, "tp", column).astype(F32), axis=0).astype(BF)
    att_other = lax.ppermute(att_half, "tp", swap)
    attended = jnp.where(
        core == 0,
        jnp.concatenate([att_half, att_other], axis=1),
        jnp.concatenate([att_other, att_half], axis=1),
    ).astype(F32)

    gain_m = block_of(mlp_gain)
    post = attended * block_of(post_gain)
    stacked = jnp.concatenate(
        [(gathered_float * gain_m).astype(BF), (post * gain_m).astype(BF)], axis=0
    )
    ff_dev = w_gate.shape[1]
    stats = [
        jnp.sum(a * b, axis=1, keepdims=True)
        for a, b in (
            (attended, attended),
            (gathered_float, gathered_float),
            (gathered_float, post),
            (post, post),
        )
    ]
    stat_block = jnp.concatenate(
        [jnp.concatenate(pieces(jnp.concatenate(stats[2 * i : 2 * i + 2], axis=0), 2), axis=1)
         for i in range(2)],
        axis=1,
    )
    ff_part = jnp.concatenate(
        [
            dot(stacked, w_gate).astype(BF),
            dot(stacked, w_up).astype(BF),
            stat_block,
        ],
        axis=1,
    )
    ff_sum = jnp.sum(spread(ff_part, "kv").astype(F32), axis=0)
    first = jnp.sum(ff_sum[:, 2 * ff_dev : 2 * ff_dev + 2], axis=1, keepdims=True)
    second = jnp.sum(ff_sum[:, 2 * ff_dev + 2 :], axis=1, keepdims=True)
    att_square, resid_square, cross, post_square = (
        first[:rows],
        first[rows:],
        second[:rows],
        second[rows:],
    )
    s = lax.rsqrt(att_square / model_width + EPS)
    mid_square = resid_square + 2.0 * s * cross + s * s * post_square
    scale_mid = lax.rsqrt(jnp.maximum(mid_square, 0.0) / model_width + EPS)
    mixed = (ff_sum[:rows] + s * ff_sum[rows:]) * scale_mid
    hidden = (jax.nn.silu(mixed[:, :ff_dev]) * mixed[:, ff_dev : 2 * ff_dev]).astype(BF)
    down = dot(hidden, w_down).astype(BF).reshape(own, nt, width).swapaxes(0, 1)
    lowered = jnp.sum(lax.all_to_all(down, "tp", 0, 0, tiled=True).astype(F32), axis=0)

    own_post = lax.dynamic_slice_in_dim(post.reshape(own, nt, width), tp_index, 1, 1)[:, 0]
    own_s = lax.dynamic_slice_in_dim(s.reshape(own, nt, 1), tp_index, 1, 1)[:, 0]
    resid_mid = (resid.astype(F32) + own_s * own_post).astype(BF).astype(F32)
    next_resid = (resid_mid + lowered).astype(BF)
    return (next_resid, new_latent, new_rope_key)


VMEM = pl.BlockSpec(memory_space=pltpu.VMEM)
WAIT = 4_000_000_000
NT = (((1,), (1,)), ((), ()))


def call(kernel, outs, *args, flops=0, scratch=()):
    many = isinstance(outs, (list, tuple))
    sizes = list(args) + (list(outs) if many else [outs])
    moved = sum(int(np.prod(a.shape)) * a.dtype.itemsize for a in sizes)
    return pl.pallas_call(
        kernel,
        out_shape=outs,
        in_specs=[VMEM] * len(args),
        out_specs=[VMEM] * len(outs) if many else VMEM,
        scratch_shapes=list(scratch),
        compiler_params=pltpu.CompilerParams(vmem_limit_bytes=16 << 20),
        cost_estimate=pl.CostEstimate(
            flops=max(flops, moved), bytes_accessed=moved, transcendentals=0
        ),
    )(*args)


def like(shape, dtype=BF):
    return jax.ShapeDtypeStruct(shape, dtype)


def lane_of(shape):
    return lax.broadcasted_iota(jnp.int32, shape, len(shape) - 1)


def terms(value, count):
    out, rest = [], value
    for _ in range(count):
        term = rest.astype(BF).astype(F32)
        out.append(term)
        rest = rest - term
    return out


def placed(columns, shape):
    lane = lane_of(shape)
    block = jnp.zeros(shape, F32)
    for at, column in columns:
        block = jnp.where(lane == at, column, block)
    return block


def picked(block, first, count):
    lane = lane_of(block.shape)
    inside = (lane >= first) & (lane < first + count)
    return jnp.sum(jnp.where(inside, block, 0.0), axis=-1, keepdims=True)


def turned(vector, table, half):
    width = vector.shape[1]
    low = lax.rem(lane_of(vector.shape), 2 * half) < half
    other = jnp.where(
        low, pltpu.roll(vector, width - half, 1), pltpu.roll(vector, half, 1)
    )
    return vector * table[0:1, :width] + other * table[1:2, :width]


def other(axis, k, step=1):
    return jnp.bitwise_xor(lax.div(lax.axis_index(axis), step), k)


def unit_kernel(out_ref):
    row = lax.rem(lax.broadcasted_iota(jnp.int32, out_ref.shape, 0), out_ref.shape[1] // 2)
    out_ref[...] = jnp.where(row == lane_of(out_ref.shape), 1.0, 0.0).astype(BF)


def flat_kernel(in_ref, out_ref):
    out_ref[...] = in_ref[...].reshape(out_ref.shape)


def start_kernel(b0, b1, b2, b3, unit_ref, out_ref, held_ref):
    chips, own, _ = held_ref.shape
    for k, ref in enumerate((b0, b1, b2, b3)):
        held_ref[other("tp", k, 2)] = ref[...].astype(F32)
    out_ref[...] = jnp.concatenate(
        [held_ref[z, r : r + 1, :] for r in range(own) for z in range(chips)], axis=0
    ).astype(BF)


def query_kernel(
    half_ref, other_ref, resid_ref, ga_ref, gp_ref, gm_ref, wn_ref, wr_ref, wl_ref, wk_ref,
    m3, m2, m1, m0, rows_ref, gains_ref, sent_ref,
):
    own, width = resid_ref.shape
    nt = rows_ref.shape[0] // own
    latent = wl_ref.shape[1]
    rope = wk_ref.shape[0]
    nope_dev, rope_dev = wn_ref.shape[1], wr_ref.shape[1]
    first = lax.rem(lax.axis_index("tp"), 2) == 0
    mine, theirs = half_ref[...].astype(F32), other_ref[...].astype(F32)
    cores = (jnp.where(first, mine, theirs), jnp.where(first, theirs, mine))
    x = jnp.concatenate(
        [core[i : i + 1] for i in range(mine.shape[0]) for core in cores], axis=0
    )
    rows_ref[...] = x.astype(BF)
    tiles = width // 128
    at = pl.multiple_of(lax.axis_index("kv") * tiles, tiles)
    gains = []
    for ref in (ga_ref, gp_ref, gm_ref):
        block = ref[pl.ds(at, tiles), :].astype(F32)
        gains.append(jnp.concatenate([block[i : i + 1] for i in range(tiles)], axis=1))
    gain = gains[0]
    gains_ref[...] = jnp.concatenate(gains + [jnp.zeros((8 - len(gains), width), F32)], axis=0)
    normed = (x * gain).astype(BF)
    qn = jnp.dot(normed, wn_ref[...], preferred_element_type=F32)
    qr = jnp.dot(normed, wr_ref[...], preferred_element_type=F32)
    square = jnp.sum(x * x, axis=1, keepdims=True)
    mine = jnp.concatenate([resid_ref[...].astype(F32), jnp.zeros((nt - own, width), F32)], axis=0)
    own_square = jnp.sum(mine * mine, axis=1, keepdims=True)
    own_normed = (mine * gain).astype(BF)
    lat = jnp.dot(own_normed, wl_ref[...], preferred_element_type=F32)
    at = pl.multiple_of(lax.axis_index("kv") * width, width)
    key = lax.dot_general(own_normed, wk_ref[:, pl.ds(at, width)], NT, preferred_element_type=F32)
    half = latent // 2
    lat = lat[:, :half] + pltpu.roll(lat[:, half:], own, 0)
    key = jnp.concatenate([key, jnp.zeros((nt, 128 - rope), F32)], axis=1)
    own_terms = terms(own_square, 2)
    for r in range(sent_ref.shape[0]):
        part = slice(r * nt, (r + 1) * nt)
        sent_ref[r, :, :nope_dev] = qn[part].astype(BF)
        sent_ref[r, :, nope_dev : nope_dev + rope_dev] = qr[part].astype(BF)
        base = nope_dev + rope_dev
        sent_ref[r, :, base : base + half] = lat.astype(BF)
        columns = [(rope + i, c) for i, c in enumerate(own_terms + terms(square[part], 2))]
        stat = placed(columns, key.shape)
        sent_ref[r, :, base + half :] = jnp.where(lane_of(key.shape) < rope, key, stat).astype(BF)
    for k, ref in enumerate((m0, m1, m2, m3)):
        ref[...] = sent_ref[other("kv", k)]


def four(refs):
    a, b, c, d = (ref[...].astype(F32) for ref in refs)
    return (a + b) + (c + d)


def latent_kernel(
    model_width, b0, b1, b2, b3, ku_ref, gain_ref, table_ref, unit_ref,
    msg_ref, lat_ref, key_ref, own_ref,
):
    nk, pairs, _ = msg_ref.shape
    nt = b0.shape[0]
    heads = pairs // nt
    latent, nope_dev = ku_ref.shape
    nope = nope_dev // heads
    own, rope = key_ref.shape
    rope_dev = heads * rope
    total = four((b0, b1, b2, b3))
    base, half = nope_dev + rope_dev, latent // 2
    stat = total[:, base + half :]
    scale = lax.rsqrt(picked(stat, rope + 2, 2) / model_width + EPS)
    own_scale = lax.rsqrt(picked(stat, rope, 2) / model_width + EPS)
    lat = total[:, base : base + half]
    lat = jnp.concatenate([lat, pltpu.roll(lat, own, 0)], axis=1)
    lat = lat * lax.rsqrt(jnp.mean(lat * lat, axis=1, keepdims=True) + EPS)
    lat = (lat * gain_ref[...].astype(F32)).astype(BF)
    table = table_ref[...]
    key = turned(stat * own_scale, table, rope // 2).astype(BF)
    lat_ref[...] = lat[:own]
    key_ref[...] = key[:own, :rope]
    own_ref[:, :latent] = lat.astype(F32)
    own_ref[:, latent:] = key.astype(F32)
    qn = (total[:, :nope_dev] * scale).astype(BF).astype(F32)
    qr = turned(total[:, nope_dev:base] * scale, table, rope // 2).astype(BF).astype(F32)

    def diagonal(q, size):
        shape = (nt, heads, heads * size)
        head = lax.broadcasted_iota(jnp.int32, shape, 1)
        lane = lax.broadcasted_iota(jnp.int32, shape, 2)
        keep = (lane >= head * size) & (lane < (head + 1) * size)
        spread_q = jnp.broadcast_to(q[:, None, :], shape)
        return jnp.where(keep, spread_q, 0.0).reshape(nt * heads, heads * size).astype(BF)

    q_lat = lax.dot_general(
        diagonal(qn, nope), ku_ref[...], NT, preferred_element_type=F32
    ).astype(BF)
    q_rope = jnp.dot(diagonal(qr, rope), unit_ref[...], preferred_element_type=F32).astype(BF)
    for j in range(nk):
        msg_ref[j, :, :latent] = q_lat
        msg_ref[j, :, latent:] = q_rope


def attend_kernel(score_scale, q_ref, cache_ref, rope_ref, own_ref, msg_ref):
    own, all_heads, _ = q_ref.shape
    latent = cache_ref.shape[2]
    rope = rope_ref.shape[1]
    holds_own = lax.axis_index("kv") == 0
    lat, key = own_ref[:, :latent], own_ref[:, latent : latent + rope]
    for r in range(own):
        q_lat = q_ref[r, :, :latent]
        q_rope = q_ref[r, :, latent : latent + rope]
        keys = cache_ref[r]
        scores = (
            lax.dot_general(q_lat, keys, NT, preferred_element_type=F32)
            + jnp.dot(q_rope, rope_ref[r], preferred_element_type=F32)
        ) * score_scale
        own_score = (
            jnp.sum(q_lat.astype(F32) * lat[r : r + 1], axis=1, keepdims=True)
            + jnp.sum(q_rope.astype(F32) * key[r : r + 1], axis=1, keepdims=True)
        ) * score_scale
        peak = jnp.maximum(jnp.max(scores, axis=1, keepdims=True), own_score)
        probs = jnp.exp(scores - peak)
        own_prob = jnp.where(holds_own, jnp.exp(own_score - peak), 0.0)
        total = jnp.sum(probs, axis=1, keepdims=True) + own_prob
        value = jnp.dot(probs.astype(BF), keys, preferred_element_type=F32)
        msg_ref[r, :, :latent] = (value + own_prob * lat[r : r + 1]).astype(BF)
        columns = list(enumerate(terms(peak, 3) + terms(total, 3)))
        msg_ref[r, :, latent:] = placed(columns, (all_heads, 128)).astype(BF)


def value_kernel(heads, got_ref, vu_ref, a0, a1, a2, a3, m3, m2, m1, m0):
    nk, pairs, _ = got_ref.shape
    latent, value_dev = vu_ref.shape
    size = value_dev // heads
    nt = pairs // heads
    stats = [got_ref[j, :, latent:].astype(F32) for j in range(nk)]
    peaks = [picked(s, 0, 3) for s in stats]
    peak = functools.reduce(jnp.maximum, peaks)
    factors = [jnp.exp(p - peak) for p in peaks]
    total = sum(picked(s, 3, 3) * f for s, f in zip(stats, factors))
    value = sum(got_ref[j, :, :latent].astype(F32) * f for j, f in enumerate(factors))
    o_lat = (value / total).astype(BF)
    full = jnp.dot(o_lat, vu_ref[...], preferred_element_type=F32)
    shape = (nt, heads, value_dev)
    head = lax.broadcasted_iota(jnp.int32, shape, 1)
    lane = lax.broadcasted_iota(jnp.int32, shape, 2)
    keep = (lane >= head * size) & (lane < (head + 1) * size)
    o_heads = jnp.sum(jnp.where(keep, full.reshape(shape), 0.0), axis=1).astype(BF)
    for a, m in ((a3, m3), (a2, m2), (a1, m1), (a0, m0)):
        m[:nt] = o_heads
        m[nt:, : a.shape[1]] = a[...]


def out_kernel(b0, b1, b2, b3, w_ref, keep_ref, give_ref, base_ref, held_ref):
    half = keep_ref.shape[1]
    nt, wide = held_ref.shape[1], base_ref.shape[1]
    for k, ref in enumerate((b0, b1, b2, b3)):
        held_ref[other("kv", k)] = ref[:nt].astype(F32)
    a, b, c, d = (ref[nt:, :wide].astype(F32) for ref in (b0, b1, b2, b3))
    base_ref[...] = (a + b) + (c + d)
    first = lax.rem(lax.axis_index("tp"), 2) == 0
    o_heads = held_ref[...].reshape(keep_ref.shape[0], w_ref.shape[0]).astype(BF)
    out = jnp.dot(o_heads, w_ref[...], preferred_element_type=F32)
    keep_ref[...] = jnp.where(first, out[:, :half], out[:, half:])
    give_ref[...] = jnp.where(first, out[:, half:], out[:, :half]).astype(BF)


def pair_kernel(keep_ref, got_ref, out_ref):
    out_ref[...] = (keep_ref[...] + got_ref[...].astype(F32)).astype(BF)


def column_kernel(b0, b1, b2, b3, out_ref):
    out_ref[...] = four((b0, b1, b2, b3)).astype(BF)


def added(a, b):
    return jnp.sum(a * b, axis=1, keepdims=True)


def send_parts(left, wg_ref, wu_ref, sums, refs, msg_ref):
    nk, rows, wide = msg_ref.shape
    ff_dev, chunk = wg_ref.shape[0], (wide - 128) // 2
    columns = list(enumerate(t for value in sums for t in terms(value, 2)))
    stat = placed(columns, (rows, 128)).astype(BF)
    for k, w_ref in enumerate((wg_ref, wu_ref)):
        part = lax.dot_general(left, w_ref[...], NT, preferred_element_type=F32)
        for j in range(nk):
            lo, hi = j * chunk, min((j + 1) * chunk, ff_dev)
            size = max(hi - lo, 0)
            if size < chunk:
                msg_ref[j, :, k * chunk : (k + 1) * chunk] = jnp.zeros((rows, chunk), BF)
            if size > 0:
                msg_ref[j, :, k * chunk : k * chunk + size] = part[:, lo:hi].astype(BF)
    for j in range(nk):
        msg_ref[j, :, 2 * chunk :] = stat
    for k, ref in enumerate(refs):
        ref[...] = msg_ref[other("kv", k)]


def base_kernel(rows_ref, gains_ref, wg_ref, wu_ref, m3, m2, m1, m0, msg_ref):
    x = rows_ref[...].astype(F32)
    left = (x * gains_ref[2:3, :]).astype(BF)
    send_parts(left, wg_ref, wu_ref, [added(x, x)], (m0, m1, m2, m3), msg_ref)


def gate_kernel(
    half_ref, other_ref, rows_ref, gains_ref, wg_ref, wu_ref, m3, m2, m1, m0, post_ref, msg_ref
):
    first = lax.rem(lax.axis_index("tp"), 2) == 0
    mine, theirs = half_ref[...].astype(F32), other_ref[...].astype(F32)
    att = jnp.concatenate(
        [jnp.where(first, mine, theirs), jnp.where(first, theirs, mine)], axis=1
    )
    x = rows_ref[...].astype(F32)
    post = att * gains_ref[1:2, :]
    post_ref[...] = post
    left = (post * gains_ref[2:3, :]).astype(BF)
    sums = [added(att, att), added(x, post), added(post, post)]
    send_parts(left, wg_ref, wu_ref, sums, (m0, m1, m2, m3), msg_ref)


def hidden_kernel(model_width, b0, b1, b2, b3, base_ref, out_ref, s_ref):
    _, chunk = out_ref.shape
    total, base = four((b0, b1, b2, b3)), base_ref[...]
    stat = total[:, 2 * chunk :]
    x_square = picked(base[:, 2 * chunk :], 0, 2)
    att_square, cross, post_square = (picked(stat, 2 * i, 2) for i in range(3))
    s = lax.rsqrt(att_square / model_width + EPS)
    mid = jnp.maximum(x_square + 2.0 * s * cross + s * s * post_square, 0.0)
    scale = lax.rsqrt(mid / model_width + EPS)
    s_ref[...] = jnp.broadcast_to(s, s_ref.shape)
    mixed = (base[:, : 2 * chunk] + s * total[:, : 2 * chunk]) * scale
    gate, up = mixed[:, :chunk], mixed[:, chunk:]
    out_ref[...] = (gate / (1.0 + jnp.exp(-gate)) * up).astype(BF)


def down_kernel(b0, b1, b2, b3, w_ref, keep_ref, give_ref, held_ref, total_ref):
    nk, _, chunk = held_ref.shape
    for k, ref in enumerate((b0, b1, b2, b3)):
        held_ref[other("kv", k)] = ref[...]
    ff_dev = w_ref.shape[0]
    total = None
    for j in range(nk):
        lo, hi = j * chunk, min((j + 1) * chunk, ff_dev)
        if hi > lo:
            part = jnp.dot(
                held_ref[j, :, : hi - lo], w_ref[lo:hi, :], preferred_element_type=F32
            )
            total = part if total is None else total + part
    total_ref[...] = total.reshape(total_ref.shape)
    core = lax.rem(lax.axis_index("tp"), 2)
    for k in range(keep_ref.shape[0]):
        at = 2 * other("tp", k, 2)
        keep_ref[k] = total_ref[:, at + core, :]
        give_ref[k] = total_ref[:, at + 1 - core, :].astype(BF)


def chips_kernel(keep_ref, got_ref, m3, m2, m1, m0):
    for k, ref in enumerate((m0, m1, m2, m3)):
        ref[...] = (keep_ref[k] + got_ref[k].astype(F32)).astype(BF)


def last_kernel(b0, b1, b2, b3, resid_ref, post_ref, s_ref, out_ref):
    own, width = resid_ref.shape
    nt = post_ref.shape[0] // own
    total = four((b0, b1, b2, b3))
    added = (post_ref[...] * s_ref[:, 0:1]).reshape(own, nt, width)
    here = lax.broadcasted_iota(jnp.int32, added.shape, 1) == lax.axis_index("tp")
    mine = jnp.sum(jnp.where(here, added, 0.0), axis=1)
    mid = (resid_ref[...].astype(F32) + mine).astype(BF).astype(F32)
    out_ref[...] = (mid + total).astype(BF)


def exchange(message, axis):
    return lax.all_to_all(message, axis, 0, 0, tiled=True)


def deal(blocks, axis, step=1):
    size = lax.axis_size(axis)
    out = list(blocks)
    for k in reversed(range(1, len(blocks))):
        out[k] = lax.ppermute(blocks[k], axis, [(i, i ^ (k * step)) for i in range(size)])
    return out


def kernel_body(
    resid,
    attn_gain,
    w_query_nope,
    w_query_rope,
    w_latent,
    w_key_rope,
    latent_gain,
    key_up,
    value_up,
    w_out,
    post_gain,
    mlp_gain,
    w_gate,
    w_up,
    w_down,
    cache_latent,
    cache_rope_key,
):
    nk = lax.axis_size("kv")
    nt = lax.axis_size("tp")
    own, width = resid.shape
    rows = own * nt
    model_width = width * nk
    latent, heads, nope = key_up.shape
    rope = cache_rope_key.shape[2]
    nope_dev, rope_dev = heads * nope, heads * rope
    ff_dev = w_gate.shape[1]
    context = cache_latent.shape[1] * nk
    half_rope = rope // 2
    angles = context * THETA ** (-np.arange(half_rope) / half_rope)
    cos, sin = np.cos(angles), np.sin(angles)
    table = np.zeros((8, rope_dev), np.float32)
    table[0] = np.tile(np.concatenate([cos, cos]), heads)
    table[1] = np.tile(np.concatenate([-sin, sin]), heads)

    swap = [(i, i ^ 1) for i in range(nt)]
    chips = nt // 2
    unit = call(unit_kernel, like((rope_dev, 2 * rope)), flops=WAIT)
    value_dev = heads * value_up.shape[2]
    key_flat = call(flat_kernel, like((latent, nope_dev)), key_up, flops=WAIT)
    value_flat = call(flat_kernel, like((latent, value_dev)), value_up, flops=WAIT)
    column = call(
        start_kernel,
        like((own * chips, width)),
        *deal([resid] * chips, "tp", 2),
        unit,
        scratch=[pltpu.VMEM((chips, own, width), F32)],
        flops=WAIT,
    )
    sent_width = nope_dev + rope_dev + latent // 2 + 128
    *msg, x_rows, gains = call(
        query_kernel,
        [like((nt, sent_width))] * nk + [like((rows, width)), like((8, width), F32)],
        column,
        lax.ppermute(column, "tp", swap),
        resid,
        *[g.reshape(-1, 128) for g in (attn_gain, post_gain, mlp_gain)],
        w_query_nope,
        w_query_rope,
        w_latent,
        w_key_rope.T,
        scratch=[pltpu.VMEM((nk, nt, sent_width), BF)],
        flops=WAIT,
    )
    pairs = nt * heads
    chunk = -(-ff_dev // (nk * 128)) * 128
    wide = 2 * chunk + 128
    base_parts = call(
        base_kernel,
        [like((rows, wide))] * nk,
        x_rows,
        gains,
        w_gate.T,
        w_up.T,
        scratch=[pltpu.VMEM((nk, rows, wide), BF)],
        flops=WAIT,
    )[::-1]
    msg, new_latent, new_rope_key, own_block = call(
        functools.partial(latent_kernel, model_width),
        [
            like((nk, pairs, latent + 128)),
            like((own, latent)),
            like((own, rope)),
            like((nt, latent + 128), F32),
        ],
        *deal(msg[::-1], "kv"),
        key_flat,
        latent_gain.reshape(1, latent),
        jnp.asarray(table),
        unit,
        flops=WAIT,
    )
    got = exchange(msg.reshape(nk * nt, heads, latent + 128), ("kv", "tp"))
    msg = call(
        functools.partial(attend_kernel, (nope + rope) ** (-0.5)),
        like((own, pairs, latent + 128)),
        got.reshape(own, pairs, latent + 128),
        cache_latent,
        cache_rope_key.swapaxes(1, 2),
        own_block,
        flops=WAIT,
    )
    got = exchange(msg.reshape(nk * nt, heads, latent + 128), ("kv", "tp"))
    msg = call(
        functools.partial(value_kernel, heads),
        [like((nt + rows, value_dev))] * nk,
        got.reshape(nk, pairs, latent + 128),
        value_flat,
        *base_parts,
        flops=WAIT,
    )
    half = width // 2
    keep, give, base = call(
        out_kernel,
        [like((rows, half), F32), like((rows, half)), like((rows, wide), F32)],
        *deal(msg[::-1], "kv"),
        w_out,
        scratch=[pltpu.VMEM((nk, nt, value_dev), F32)],
        flops=WAIT,
    )
    pair = call(
        pair_kernel, like((rows, half)), keep, lax.ppermute(give, "tp", swap), flops=WAIT
    )
    att_half = call(column_kernel, like((rows, half)), *deal([pair] * chips, "tp", 2), flops=WAIT)
    att_other = lax.ppermute(att_half, "tp", swap)
    *msg, post = call(
        gate_kernel,
        [like((rows, wide))] * nk + [like((rows, width), F32)],
        att_half,
        att_other,
        x_rows,
        gains,
        w_gate.T,
        w_up.T,
        scratch=[pltpu.VMEM((nk, rows, wide), BF)],
        flops=WAIT,
    )
    hidden, s = call(
        functools.partial(hidden_kernel, model_width),
        [like((rows, chunk)), like((rows, 128), F32)],
        *deal(msg[::-1], "kv"),
        base,
        flops=WAIT,
    )
    keep, give = call(
        down_kernel,
        [like((chips, own, width), F32), like((chips, own, width))],
        *deal([hidden] * nk, "kv"),
        w_down,
        scratch=[pltpu.VMEM((nk, rows, chunk), BF), pltpu.VMEM((own, nt, width), F32)],
        flops=WAIT,
    )
    msg = call(
        chips_kernel,
        [like((own, width))] * chips,
        keep,
        lax.ppermute(give, "tp", swap),
        flops=WAIT,
    )
    next_resid = call(
        last_kernel, like((own, width)), *deal(msg[::-1], "tp", 2), resid, post, s, flops=WAIT
    )
    return (next_resid, new_latent, new_rope_key)


def body(*args):
    resid, key_up, cache = args[0], args[7], args[15]
    nk, nt = lax.axis_size("kv"), lax.axis_size("tp")
    own, width = resid.shape
    latent, heads, nope = key_up.shape
    fits = (
        own == nk == 4
        and nt == 8
        and heads == 8
        and 2 * own == nt
        and width % 1024 == 0
        and latent % 256 == 0
        and heads * args[8].shape[2] >= 2 * (-(-args[12].shape[1] // (nk * 128)) * 128) + 128
        and nope % 128 == 0
        and cache.shape[1] % 128 == 0
        and args[16].shape[2] == 64
    )
    if not fits:
        return plain_body(*args)
    return kernel_body(*args)


def solution(mesh):
    return jax.shard_map(
        body,
        mesh=mesh,
        in_specs=(
            P("tp", "kv"),
            P(),
            P("kv", "tp"),
            P("kv", "tp"),
            P("kv", None),
            P(),
            P(),
            P(None, "tp", None),
            P(None, "tp", None),
            P("tp", "kv"),
            P(),
            P(),
            P("kv", "tp"),
            P("kv", "tp"),
            P("tp", "kv"),
            P("tp", "kv", None),
            P("tp", "kv", None),
        ),
        out_specs=(P("tp", "kv"), P("tp", None), P("tp", None)),
        check_vma=False,
    )
```

```python
import functools

import jax
import jax.numpy as jnp
import numpy as np
from jax import lax
from jax.experimental import pallas as pl
from jax.experimental.pallas import tpu as pltpu
from jax.sharding import PartitionSpec as P


EPS = 1e-06
THETA = 10000.0
BF = jnp.bfloat16
F32 = jnp.float32


def rotate(vector, position):
    half_width = vector.shape[-1] // 2
    frequency = THETA ** (-jnp.arange(half_width, dtype=F32) / half_width)
    angles = jnp.asarray(position, F32) * frequency
    cos_table, sin_table = (jnp.cos(angles), jnp.sin(angles))
    lower_half, upper_half = (vector[..., :half_width], vector[..., half_width:])
    return jnp.concatenate(
        [
            lower_half * cos_table - upper_half * sin_table,
            lower_half * sin_table + upper_half * cos_table,
        ],
        axis=-1,
    )


def dot(a, b):
    return jnp.dot(a, b, preferred_element_type=F32)


def pieces(value, count):
    out, rest = [], value
    for _ in range(count):
        term = lax.reduce_precision(rest, 8, 7)
        out.append(term.astype(BF))
        rest = rest - term
    return out


def spread(block, axis, groups=None):
    count = len(groups[0]) if groups else lax.axis_size(axis)
    copies = jnp.broadcast_to(block[None], (count,) + block.shape)
    return lax.all_to_all(copies, axis, 0, 0, tiled=True, axis_index_groups=groups)


def plain_body(
    resid,
    attn_gain,
    w_query_nope,
    w_query_rope,
    w_latent,
    w_key_rope,
    latent_gain,
    key_up,
    value_up,
    w_out,
    post_gain,
    mlp_gain,
    w_gate,
    w_up,
    w_down,
    cache_latent,
    cache_rope_key,
):
    nk = lax.axis_size("kv")
    nt = lax.axis_size("tp")
    kv_index = lax.axis_index("kv")
    tp_index = lax.axis_index("tp")
    own, width = resid.shape
    rows = own * nt
    model_width = width * nk
    latent, heads, nope = key_up.shape
    value_width = value_up.shape[2]
    rope = cache_rope_key.shape[2]
    pos_dev = cache_latent.shape[1]
    context = pos_dev * nk
    score_scale = (nope + rope) ** (-0.5)
    col_start = kv_index * width
    split_rows = own % nk == 0

    def block_of(vector):
        return lax.dynamic_slice_in_dim(vector, col_start, width, 0).astype(F32)[None, :]

    gathered = spread(resid, "tp").swapaxes(0, 1).reshape(rows, width)
    gathered_float = gathered.astype(F32)
    gain_a = block_of(attn_gain)
    normed_a = (gathered_float * gain_a).astype(BF)
    own_normed = (resid.astype(F32) * gain_a).astype(BF)
    key_rows = lax.dynamic_slice_in_dim(w_key_rope, col_start, width, 0)
    squares = jnp.sum(gathered_float * gathered_float, axis=1, keepdims=True)
    own_squares = jnp.sum(resid.astype(F32) ** 2, axis=1, keepdims=True)
    q_part = jnp.concatenate(
        [
            dot(normed_a, w_query_nope).astype(BF),
            dot(normed_a, w_query_rope).astype(BF),
            *pieces(squares, 2),
            jnp.zeros((rows, 126), BF),
        ],
        axis=1,
    )
    own_part = jnp.concatenate(
        [
            dot(own_normed, w_latent).astype(BF),
            dot(own_normed, key_rows).astype(BF),
            *pieces(own_squares, 2),
        ],
        axis=1,
    )
    nope_dev, rope_dev = heads * nope, heads * rope
    q_width, own_width = q_part.shape[1], own_part.shape[1]
    sent_width = max(q_width, own_width)
    q_part = jnp.pad(q_part, ((0, 0), (0, sent_width - q_width)))
    own_part = jnp.pad(own_part, ((0, 0), (0, sent_width - own_width)))
    summed = jnp.sum(
        spread(jnp.concatenate([q_part, own_part], axis=0), "kv").astype(F32), axis=0
    )
    q_sum, own_sum = summed[:rows], summed[rows:, :own_width]
    square_sum = jnp.sum(q_sum[:, nope_dev + rope_dev :], axis=1, keepdims=True)
    scale_in = lax.rsqrt(square_sum / model_width + EPS)
    q_nope = (q_sum[:, :nope_dev] * scale_in).astype(BF).reshape(rows, heads, nope)
    q_rope = rotate(
        (q_sum[:, nope_dev : nope_dev + rope_dev] * scale_in).reshape(rows, heads, rope), context
    ).astype(BF)
    latent_sum = own_sum[:, :latent]
    own_scale = lax.rsqrt(
        jnp.sum(own_sum[:, latent + rope :], axis=1, keepdims=True) / model_width + EPS
    )
    new_latent = (
        latent_sum
        * lax.rsqrt(jnp.mean(latent_sum * latent_sum, axis=1, keepdims=True) + EPS)
        * latent_gain.astype(F32)[None, :]
    ).astype(BF)
    new_rope_key = rotate(own_sum[:, latent : latent + rope] * own_scale, context).astype(BF)
    q_lat = jnp.einsum("bhd,chd->bhc", q_nope, key_up, preferred_element_type=F32).astype(BF)

    query = jnp.concatenate([q_lat, q_rope], axis=-1).reshape(own, nt, heads, latent + rope)
    query = lax.all_to_all(query.swapaxes(0, 1), "tp", 0, 0, tiled=True)
    query = query.transpose(1, 0, 2, 3).reshape(own, nt * heads, latent + rope)
    all_heads = nt * heads
    seq_lat, seq_rope = query[..., :latent], query[..., latent:]
    scores = (
        jnp.einsum("bhc,bpc->bhp", seq_lat, cache_latent, preferred_element_type=F32)
        + jnp.einsum("bhr,bpr->bhp", seq_rope, cache_rope_key, preferred_element_type=F32)
    ) * score_scale
    own_score = (
        jnp.einsum("bhc,bc->bh", seq_lat, new_latent, preferred_element_type=F32)
        + jnp.einsum("bhr,br->bh", seq_rope, new_rope_key, preferred_element_type=F32)
    ) * score_scale
    peak = jnp.maximum(jnp.max(scores, axis=2), own_score)
    probs = jnp.exp(scores - peak[:, :, None])
    own_prob = jnp.where(kv_index == 0, jnp.exp(own_score - peak), 0.0)
    totals = jnp.sum(probs, axis=2) + own_prob
    partial_value = (
        jnp.einsum("bhp,bpc->bhc", probs.astype(BF), cache_latent, preferred_element_type=F32)
        + own_prob[:, :, None] * new_latent.astype(F32)[:, None, :]
    )
    packed = jnp.concatenate(
        [partial_value.astype(BF)]
        + [p[:, :, None] for p in pieces(peak, 3) + pieces(totals, 3)]
        + [jnp.zeros((own, all_heads, 122), BF)],
        axis=2,
    )

    def combine(blocks):
        stats = blocks[..., latent:].astype(F32)
        peaks = jnp.sum(stats[..., :3], axis=-1, keepdims=True)
        sums = jnp.sum(stats[..., 3:6], axis=-1, keepdims=True)
        factor = jnp.exp(peaks - jnp.max(peaks, axis=0, keepdims=True))
        value = jnp.sum(blocks[..., :latent].astype(F32) * factor, axis=0)
        return (value / jnp.sum(sums * factor, axis=0)).astype(BF)

    if split_rows:
        per = own // nk
        sent = packed.reshape(nk, per, nt, heads, latent + 128).swapaxes(1, 2)
        sent = sent.reshape(nk * nt, per, heads, latent + 128)
        got = lax.all_to_all(sent, ("kv", "tp"), 0, 0, tiled=True)
        got = got.reshape(nk, nt, per, heads, latent + 128)
        o_lat = combine(got).swapaxes(0, 1).reshape(per * nt, heads, latent)
    else:
        flat = own * all_heads // nk
        got = lax.all_to_all(packed.reshape(nk, flat, latent + 128), "kv", 0, 0, tiled=True)
        o_own = spread(combine(got), "kv").reshape(own, nt, heads, latent)
        o_lat = lax.all_to_all(o_own.swapaxes(0, 1), "tp", 0, 0, tiled=True)
        o_lat = o_lat.swapaxes(0, 1).reshape(rows, heads, latent)
    o_heads = jnp.einsum("bhc,che->bhe", o_lat, value_up, preferred_element_type=F32).astype(BF)
    o_flat = o_heads.reshape(-1, heads * value_width)
    if split_rows:
        o_flat = spread(o_flat, "kv").reshape(rows, heads * value_width)

    core = lax.rem(tp_index, 2)
    swap = [(i, i ^ 1) for i in range(nt)]
    column = [list(range(c, nt, 2)) for c in range(2)]
    half = width // 2
    out_part = dot(o_flat, w_out).reshape(rows, 2, half)
    keep = jnp.where(core == 0, out_part[:, 0], out_part[:, 1])
    give = jnp.where(core == 0, out_part[:, 1], out_part[:, 0]).astype(BF)
    pair_sum = (keep + lax.ppermute(give, "tp", swap).astype(F32)).astype(BF)
    att_half = jnp.sum(spread(pair_sum, "tp", column).astype(F32), axis=0).astype(BF)
    att_other = lax.ppermute(att_half, "tp", swap)
    attended = jnp.where(
        core == 0,
        jnp.concatenate([att_half, att_other], axis=1),
        jnp.concatenate([att_other, att_half], axis=1),
    ).astype(F32)

    gain_m = block_of(mlp_gain)
    post = attended * block_of(post_gain)
    stacked = jnp.concatenate(
        [(gathered_float * gain_m).astype(BF), (post * gain_m).astype(BF)], axis=0
    )
    ff_dev = w_gate.shape[1]
    stats = [
        jnp.sum(a * b, axis=1, keepdims=True)
        for a, b in (
            (attended, attended),
            (gathered_float, gathered_float),
            (gathered_float, post),
            (post, post),
        )
    ]
    stat_block = jnp.concatenate(
        [jnp.concatenate(pieces(jnp.concatenate(stats[2 * i : 2 * i + 2], axis=0), 2), axis=1)
         for i in range(2)],
        axis=1,
    )
    ff_part = jnp.concatenate(
        [
            dot(stacked, w_gate).astype(BF),
            dot(stacked, w_up).astype(BF),
            stat_block,
        ],
        axis=1,
    )
    ff_sum = jnp.sum(spread(ff_part, "kv").astype(F32), axis=0)
    first = jnp.sum(ff_sum[:, 2 * ff_dev : 2 * ff_dev + 2], axis=1, keepdims=True)
    second = jnp.sum(ff_sum[:, 2 * ff_dev + 2 :], axis=1, keepdims=True)
    att_square, resid_square, cross, post_square = (
        first[:rows],
        first[rows:],
        second[:rows],
        second[rows:],
    )
    s = lax.rsqrt(att_square / model_width + EPS)
    mid_square = resid_square + 2.0 * s * cross + s * s * post_square
    scale_mid = lax.rsqrt(jnp.maximum(mid_square, 0.0) / model_width + EPS)
    mixed = (ff_sum[:rows] + s * ff_sum[rows:]) * scale_mid
    hidden = (jax.nn.silu(mixed[:, :ff_dev]) * mixed[:, ff_dev : 2 * ff_dev]).astype(BF)
    down = dot(hidden, w_down).astype(BF).reshape(own, nt, width).swapaxes(0, 1)
    lowered = jnp.sum(lax.all_to_all(down, "tp", 0, 0, tiled=True).astype(F32), axis=0)

    own_post = lax.dynamic_slice_in_dim(post.reshape(own, nt, width), tp_index, 1, 1)[:, 0]
    own_s = lax.dynamic_slice_in_dim(s.reshape(own, nt, 1), tp_index, 1, 1)[:, 0]
    resid_mid = (resid.astype(F32) + own_s * own_post).astype(BF).astype(F32)
    next_resid = (resid_mid + lowered).astype(BF)
    return (next_resid, new_latent, new_rope_key)


VMEM = pl.BlockSpec(memory_space=pltpu.VMEM)
WAIT = 4_000_000_000
NT = (((1,), (1,)), ((), ()))


def call(kernel, outs, *args, flops=0, scratch=()):
    many = isinstance(outs, (list, tuple))
    sizes = list(args) + (list(outs) if many else [outs])
    moved = sum(int(np.prod(a.shape)) * a.dtype.itemsize for a in sizes)
    return pl.pallas_call(
        kernel,
        out_shape=outs,
        in_specs=[VMEM] * len(args),
        out_specs=[VMEM] * len(outs) if many else VMEM,
        scratch_shapes=list(scratch),
        compiler_params=pltpu.CompilerParams(vmem_limit_bytes=16 << 20),
        cost_estimate=pl.CostEstimate(
            flops=max(flops, moved), bytes_accessed=moved, transcendentals=0
        ),
    )(*args)


def like(shape, dtype=BF):
    return jax.ShapeDtypeStruct(shape, dtype)


def lane_of(shape):
    return lax.broadcasted_iota(jnp.int32, shape, len(shape) - 1)


def terms(value, count):
    out, rest = [], value
    for _ in range(count):
        term = rest.astype(BF).astype(F32)
        out.append(term)
        rest = rest - term
    return out


def placed(columns, shape):
    lane = lane_of(shape)
    block = jnp.zeros(shape, F32)
    for at, column in columns:
        block = jnp.where(lane == at, column, block)
    return block


def picked(block, first, count):
    lane = lane_of(block.shape)
    inside = (lane >= first) & (lane < first + count)
    return jnp.sum(jnp.where(inside, block, 0.0), axis=-1, keepdims=True)


def turned(vector, table, half):
    width = vector.shape[1]
    low = lax.rem(lane_of(vector.shape), 2 * half) < half
    other = jnp.where(
        low, pltpu.roll(vector, width - half, 1), pltpu.roll(vector, half, 1)
    )
    return vector * table[0:1, :width] + other * table[1:2, :width]


def other(axis, k, step=1):
    return jnp.bitwise_xor(lax.div(lax.axis_index(axis), step), k)


def unit_kernel(out_ref):
    row = lax.rem(lax.broadcasted_iota(jnp.int32, out_ref.shape, 0), out_ref.shape[1] // 2)
    out_ref[...] = jnp.where(row == lane_of(out_ref.shape), 1.0, 0.0).astype(BF)


def flat_kernel(in_ref, out_ref):
    out_ref[...] = in_ref[...].reshape(out_ref.shape)


def start_kernel(b0, b1, b2, b3, unit_ref, out_ref, held_ref):
    chips, own, _ = held_ref.shape
    for k, ref in enumerate((b0, b1, b2, b3)):
        held_ref[other("tp", k, 2)] = ref[...].astype(F32)
    out_ref[...] = jnp.concatenate(
        [held_ref[z, r : r + 1, :] for r in range(own) for z in range(chips)], axis=0
    ).astype(BF)


def query_kernel(
    half_ref, other_ref, resid_ref, ga_ref, gp_ref, gm_ref, wn_ref, wr_ref, wl_ref, wk_ref,
    m3, m2, m1, m0, rows_ref, gains_ref, sent_ref,
):
    own, width = resid_ref.shape
    nt = rows_ref.shape[0] // own
    latent = wl_ref.shape[1]
    rope = wk_ref.shape[0]
    nope_dev, rope_dev = wn_ref.shape[1], wr_ref.shape[1]
    first = lax.rem(lax.axis_index("tp"), 2) == 0
    mine, theirs = half_ref[...].astype(F32), other_ref[...].astype(F32)
    cores = (jnp.where(first, mine, theirs), jnp.where(first, theirs, mine))
    x = jnp.concatenate(
        [core[i : i + 1] for i in range(mine.shape[0]) for core in cores], axis=0
    )
    rows_ref[...] = x.astype(BF)
    tiles = width // 128
    at = pl.multiple_of(lax.axis_index("kv") * tiles, tiles)
    gains = []
    for ref in (ga_ref, gp_ref, gm_ref):
        block = ref[pl.ds(at, tiles), :].astype(F32)
        gains.append(jnp.concatenate([block[i : i + 1] for i in range(tiles)], axis=1))
    gain = gains[0]
    gains_ref[...] = jnp.concatenate(gains + [jnp.zeros((8 - len(gains), width), F32)], axis=0)
    normed = (x * gain).astype(BF)
    qn = jnp.dot(normed, wn_ref[...], preferred_element_type=F32)
    qr = jnp.dot(normed, wr_ref[...], preferred_element_type=F32)
    square = jnp.sum(x * x, axis=1, keepdims=True)
    mine = jnp.concatenate([resid_ref[...].astype(F32), jnp.zeros((nt - own, width), F32)], axis=0)
    own_square = jnp.sum(mine * mine, axis=1, keepdims=True)
    own_normed = (mine * gain).astype(BF)
    lat = jnp.dot(own_normed, wl_ref[...], preferred_element_type=F32)
    at = pl.multiple_of(lax.axis_index("kv") * width, width)
    key = lax.dot_general(own_normed, wk_ref[:, pl.ds(at, width)], NT, preferred_element_type=F32)
    half = latent // 2
    lat = lat[:, :half] + pltpu.roll(lat[:, half:], own, 0)
    key = jnp.concatenate([key, jnp.zeros((nt, 128 - rope), F32)], axis=1)
    own_terms = terms(own_square, 2)
    for r in range(sent_ref.shape[0]):
        part = slice(r * nt, (r + 1) * nt)
        sent_ref[r, :, :nope_dev] = qn[part].astype(BF)
        sent_ref[r, :, nope_dev : nope_dev + rope_dev] = qr[part].astype(BF)
        base = nope_dev + rope_dev
        sent_ref[r, :, base : base + half] = lat.astype(BF)
        columns = [(rope + i, c) for i, c in enumerate(own_terms + terms(square[part], 2))]
        stat = placed(columns, key.shape)
        sent_ref[r, :, base + half :] = jnp.where(lane_of(key.shape) < rope, key, stat).astype(BF)
    for k, ref in enumerate((m0, m1, m2, m3)):
        ref[...] = sent_ref[other("kv", k)]


def four(refs):
    a, b, c, d = (ref[...].astype(F32) for ref in refs)
    return (a + b) + (c + d)


def latent_kernel(
    model_width, b0, b1, b2, b3, ku_ref, gain_ref, table_ref, unit_ref,
    msg_ref, lat_ref, key_ref, own_ref,
):
    nk, pairs, _ = msg_ref.shape
    nt = b0.shape[0]
    heads = pairs // nt
    latent, nope_dev = ku_ref.shape
    nope = nope_dev // heads
    own, rope = key_ref.shape
    rope_dev = heads * rope
    total = four((b0, b1, b2, b3))
    base, half = nope_dev + rope_dev, latent // 2
    stat = total[:, base + half :]
    scale = lax.rsqrt(picked(stat, rope + 2, 2) / model_width + EPS)
    own_scale = lax.rsqrt(picked(stat, rope, 2) / model_width + EPS)
    lat = total[:, base : base + half]
    lat = jnp.concatenate([lat, pltpu.roll(lat, own, 0)], axis=1)
    lat = lat * lax.rsqrt(jnp.mean(lat * lat, axis=1, keepdims=True) + EPS)
    lat = (lat * gain_ref[...].astype(F32)).astype(BF)
    table = table_ref[...]
    key = turned(stat * own_scale, table, rope // 2).astype(BF)
    lat_ref[...] = lat[:own]
    key_ref[...] = key[:own, :rope]
    own_ref[:, :latent] = lat.astype(F32)
    own_ref[:, latent:] = key.astype(F32)
    qn = (total[:, :nope_dev] * scale).astype(BF).astype(F32)
    qr = turned(total[:, nope_dev:base] * scale, table, rope // 2).astype(BF).astype(F32)

    def diagonal(q, size):
        shape = (nt, heads, heads * size)
        head = lax.broadcasted_iota(jnp.int32, shape, 1)
        lane = lax.broadcasted_iota(jnp.int32, shape, 2)
        keep = (lane >= head * size) & (lane < (head + 1) * size)
        spread_q = jnp.broadcast_to(q[:, None, :], shape)
        return jnp.where(keep, spread_q, 0.0).reshape(nt * heads, heads * size).astype(BF)

    q_lat = lax.dot_general(
        diagonal(qn, nope), ku_ref[...], NT, preferred_element_type=F32
    ).astype(BF)
    q_rope = jnp.dot(diagonal(qr, rope), unit_ref[...], preferred_element_type=F32).astype(BF)
    for j in range(nk):
        msg_ref[j, :, :latent] = q_lat
        msg_ref[j, :, latent:] = q_rope


def attend_kernel(score_scale, q_ref, cache_ref, rope_ref, own_ref, msg_ref):
    own, all_heads, _ = q_ref.shape
    latent = cache_ref.shape[2]
    rope = rope_ref.shape[1]
    holds_own = lax.axis_index("kv") == 0
    lat, key = own_ref[:, :latent], own_ref[:, latent : latent + rope]
    seqs = range(own)
    q_lat = [q_ref[r, :, :latent] for r in seqs]
    q_rope = [q_ref[r, :, latent : latent + rope] for r in seqs]
    scores = [
        (
            lax.dot_general(q_lat[r], cache_ref[r], NT, preferred_element_type=F32)
            + jnp.dot(q_rope[r], rope_ref[r], preferred_element_type=F32)
        )
        * score_scale
        for r in seqs
    ]
    own_scores = [
        (
            jnp.sum(q_lat[r].astype(F32) * lat[r : r + 1], axis=1, keepdims=True)
            + jnp.sum(q_rope[r].astype(F32) * key[r : r + 1], axis=1, keepdims=True)
        )
        * score_scale
        for r in seqs
    ]
    peaks = [
        jnp.maximum(jnp.max(scores[r], axis=1, keepdims=True), own_scores[r]) for r in seqs
    ]
    probs = [jnp.exp(scores[r] - peaks[r]) for r in seqs]
    values = [
        jnp.dot(probs[r].astype(BF), cache_ref[r], preferred_element_type=F32) for r in seqs
    ]
    for r in seqs:
        own_prob = jnp.where(holds_own, jnp.exp(own_scores[r] - peaks[r]), 0.0)
        total = jnp.sum(probs[r], axis=1, keepdims=True) + own_prob
        msg_ref[r, :, :latent] = (values[r] + own_prob * lat[r : r + 1]).astype(BF)
        columns = list(enumerate(terms(peaks[r], 3) + terms(total, 3)))
        msg_ref[r, :, latent:] = placed(columns, (all_heads, 128)).astype(BF)


def value_kernel(heads, got_ref, vu_ref, a0, a1, a2, a3, m3, m2, m1, m0):
    nk, pairs, _ = got_ref.shape
    latent, value_dev = vu_ref.shape
    size = value_dev // heads
    nt = pairs // heads
    stats = [got_ref[j, :, latent:].astype(F32) for j in range(nk)]
    peaks = [picked(s, 0, 3) for s in stats]
    peak = functools.reduce(jnp.maximum, peaks)
    factors = [jnp.exp(p - peak) for p in peaks]
    total = sum(picked(s, 3, 3) * f for s, f in zip(stats, factors))
    value = sum(got_ref[j, :, :latent].astype(F32) * f for j, f in enumerate(factors))
    o_lat = (value / total).astype(BF)
    full = jnp.dot(o_lat, vu_ref[...], preferred_element_type=F32)
    shape = (nt, heads, value_dev)
    head = lax.broadcasted_iota(jnp.int32, shape, 1)
    lane = lax.broadcasted_iota(jnp.int32, shape, 2)
    keep = (lane >= head * size) & (lane < (head + 1) * size)
    o_heads = jnp.sum(jnp.where(keep, full.reshape(shape), 0.0), axis=1).astype(BF)
    rows, wide = a0.shape
    for a, m in ((a3, m3), (a2, m2), (a1, m1), (a0, m0)):
        m[:, :value_dev] = o_heads
        for g in range(rows // nt):
            m[:, value_dev + g * wide : value_dev + (g + 1) * wide] = a[g * nt : (g + 1) * nt]


def out_kernel(b0, b1, b2, b3, w_ref, keep_ref, give_ref, base_ref, held_ref):
    half = keep_ref.shape[1]
    _, nt, value_dev = held_ref.shape
    rows, wide = base_ref.shape
    for k, ref in enumerate((b0, b1, b2, b3)):
        held_ref[other("kv", k)] = ref[:, :value_dev].astype(F32)
    for g in range(rows // nt):
        lo = value_dev + g * wide
        a, b, c, d = (ref[:, lo : lo + wide].astype(F32) for ref in (b0, b1, b2, b3))
        base_ref[g * nt : (g + 1) * nt] = (a + b) + (c + d)
    first = lax.rem(lax.axis_index("tp"), 2) == 0
    o_heads = held_ref[...].reshape(keep_ref.shape[0], w_ref.shape[0]).astype(BF)
    out = jnp.dot(o_heads, w_ref[...], preferred_element_type=F32)
    keep_ref[...] = jnp.where(first, out[:, :half], out[:, half:])
    give_ref[...] = jnp.where(first, out[:, half:], out[:, :half]).astype(BF)


def pair_kernel(keep_ref, got_ref, out_ref):
    out_ref[...] = (keep_ref[...] + got_ref[...].astype(F32)).astype(BF)


def column_kernel(b0, b1, b2, b3, out_ref):
    out_ref[...] = four((b0, b1, b2, b3)).astype(BF)


def added(a, b):
    return jnp.sum(a * b, axis=1, keepdims=True)


def send_parts(parts, sums, refs, msg_ref):
    nk, rows, wide = msg_ref.shape
    chunk = (wide - 128) // 2
    columns = list(enumerate(t for value in sums for t in terms(value, 2)))
    stat = placed(columns, (rows, 128)).astype(BF)
    for k, part in enumerate(parts):
        ff_dev = part.shape[1]
        for j in range(nk):
            lo, hi = j * chunk, min((j + 1) * chunk, ff_dev)
            size = max(hi - lo, 0)
            if size < chunk:
                msg_ref[j, :, k * chunk : (k + 1) * chunk] = jnp.zeros((rows, chunk), BF)
            if size > 0:
                msg_ref[j, :, k * chunk : k * chunk + size] = part[:, lo:hi].astype(BF)
    for j in range(nk):
        msg_ref[j, :, 2 * chunk :] = stat
    for k, ref in enumerate(refs):
        ref[...] = msg_ref[other("kv", k)]


def base_kernel(rows_ref, gains_ref, wg_ref, wu_ref, m3, m2, m1, m0, msg_ref):
    x = rows_ref[...].astype(F32)
    left = (x * gains_ref[2:3, :]).astype(BF)
    parts = [
        lax.dot_general(left, w[...], NT, preferred_element_type=F32) for w in (wg_ref, wu_ref)
    ]
    send_parts(parts, [added(x, x)], (m0, m1, m2, m3), msg_ref)


def half_products(half_ref, core, gains_ref, wg_ref, wu_ref):
    half = half_ref.shape[1]
    at = pl.ds(pl.multiple_of(core * half, half), half)
    gain = gains_ref[1:3, at]
    left = (half_ref[...].astype(F32) * gain[0:1] * gain[1:2]).astype(BF)
    return [
        lax.dot_general(left, w[:, at], NT, preferred_element_type=F32) for w in (wg_ref, wu_ref)
    ]


def early_kernel(half_ref, gains_ref, wg_ref, wu_ref, gate_ref, up_ref):
    core = lax.rem(lax.axis_index("tp"), 2)
    gate_ref[...], up_ref[...] = half_products(half_ref, core, gains_ref, wg_ref, wu_ref)


def gate_kernel(
    half_ref, other_ref, gate_ref, up_ref, rows_ref, gains_ref, wg_ref, wu_ref,
    m3, m2, m1, m0, post_ref, msg_ref,
):
    core = lax.rem(lax.axis_index("tp"), 2)
    late = half_products(other_ref, 1 - core, gains_ref, wg_ref, wu_ref)
    parts = [gate_ref[...] + late[0], up_ref[...] + late[1]]
    mine, theirs = half_ref[...].astype(F32), other_ref[...].astype(F32)
    first = core == 0
    att = jnp.concatenate(
        [jnp.where(first, mine, theirs), jnp.where(first, theirs, mine)], axis=1
    )
    x = rows_ref[...].astype(F32)
    post = att * gains_ref[1:2, :]
    post_ref[...] = post
    sums = [added(att, att), added(x, post), added(post, post)]
    send_parts(parts, sums, (m0, m1, m2, m3), msg_ref)


def hidden_kernel(model_width, b0, b1, b2, b3, base_ref, out_ref, s_ref):
    _, chunk = out_ref.shape
    total, base = four((b0, b1, b2, b3)), base_ref[...]
    stat = total[:, 2 * chunk :]
    x_square = picked(base[:, 2 * chunk :], 0, 2)
    att_square, cross, post_square = (picked(stat, 2 * i, 2) for i in range(3))
    s = lax.rsqrt(att_square / model_width + EPS)
    mid = jnp.maximum(x_square + 2.0 * s * cross + s * s * post_square, 0.0)
    scale = lax.rsqrt(mid / model_width + EPS)
    s_ref[...] = jnp.broadcast_to(s, s_ref.shape)
    mixed = (base[:, : 2 * chunk] + s * total[:, : 2 * chunk]) * scale
    gate, up = mixed[:, :chunk], mixed[:, chunk:]
    out_ref[...] = (gate / (1.0 + jnp.exp(-gate)) * up).astype(BF)


def down_kernel(b0, b1, b2, b3, w_ref, keep_ref, give_ref, held_ref, total_ref):
    nk, _, chunk = held_ref.shape
    for k, ref in enumerate((b0, b1, b2, b3)):
        held_ref[other("kv", k)] = ref[...]
    ff_dev = w_ref.shape[0]
    total = None
    for j in range(nk):
        lo, hi = j * chunk, min((j + 1) * chunk, ff_dev)
        if hi > lo:
            part = jnp.dot(
                held_ref[j, :, : hi - lo], w_ref[lo:hi, :], preferred_element_type=F32
            )
            total = part if total is None else total + part
    total_ref[...] = total.reshape(total_ref.shape)
    core = lax.rem(lax.axis_index("tp"), 2)
    for k in range(keep_ref.shape[0]):
        at = 2 * other("tp", k, 2)
        keep_ref[k] = total_ref[:, at + core, :]
        give_ref[k] = total_ref[:, at + 1 - core, :].astype(BF)


def chips_kernel(keep_ref, got_ref, m3, m2, m1, m0):
    for k, ref in enumerate((m0, m1, m2, m3)):
        ref[...] = (keep_ref[k] + got_ref[k].astype(F32)).astype(BF)


def last_kernel(b0, b1, b2, b3, resid_ref, post_ref, s_ref, out_ref):
    own, width = resid_ref.shape
    nt = post_ref.shape[0] // own
    total = four((b0, b1, b2, b3))
    added = (post_ref[...] * s_ref[:, 0:1]).reshape(own, nt, width)
    here = lax.broadcasted_iota(jnp.int32, added.shape, 1) == lax.axis_index("tp")
    mine = jnp.sum(jnp.where(here, added, 0.0), axis=1)
    mid = (resid_ref[...].astype(F32) + mine).astype(BF).astype(F32)
    out_ref[...] = (mid + total).astype(BF)


def exchange(message, axis):
    return lax.all_to_all(message, axis, 0, 0, tiled=True)


def deal(blocks, axis, step=1):
    size = lax.axis_size(axis)
    out = list(blocks)
    for k in reversed(range(1, len(blocks))):
        out[k] = lax.ppermute(blocks[k], axis, [(i, i ^ (k * step)) for i in range(size)])
    return out


def kernel_body(
    resid,
    attn_gain,
    w_query_nope,
    w_query_rope,
    w_latent,
    w_key_rope,
    latent_gain,
    key_up,
    value_up,
    w_out,
    post_gain,
    mlp_gain,
    w_gate,
    w_up,
    w_down,
    cache_latent,
    cache_rope_key,
):
    nk = lax.axis_size("kv")
    nt = lax.axis_size("tp")
    own, width = resid.shape
    rows = own * nt
    model_width = width * nk
    latent, heads, nope = key_up.shape
    rope = cache_rope_key.shape[2]
    nope_dev, rope_dev = heads * nope, heads * rope
    ff_dev = w_gate.shape[1]
    context = cache_latent.shape[1] * nk
    half_rope = rope // 2
    angles = context * THETA ** (-np.arange(half_rope) / half_rope)
    cos, sin = np.cos(angles), np.sin(angles)
    table = np.zeros((8, rope_dev), np.float32)
    table[0] = np.tile(np.concatenate([cos, cos]), heads)
    table[1] = np.tile(np.concatenate([-sin, sin]), heads)

    swap = [(i, i ^ 1) for i in range(nt)]
    chips = nt // 2
    unit = call(unit_kernel, like((rope_dev, 2 * rope)), flops=WAIT)
    value_dev = heads * value_up.shape[2]
    key_flat = call(flat_kernel, like((latent, nope_dev)), key_up, flops=WAIT)
    value_flat = call(flat_kernel, like((latent, value_dev)), value_up, flops=WAIT)
    column = call(
        start_kernel,
        like((own * chips, width)),
        *deal([resid] * chips, "tp", 2),
        unit,
        scratch=[pltpu.VMEM((chips, own, width), F32)],
        flops=WAIT,
    )
    sent_width = nope_dev + rope_dev + latent // 2 + 128
    *msg, x_rows, gains = call(
        query_kernel,
        [like((nt, sent_width))] * nk + [like((rows, width)), like((8, width), F32)],
        column,
        lax.ppermute(column, "tp", swap),
        resid,
        *[g.reshape(-1, 128) for g in (attn_gain, post_gain, mlp_gain)],
        w_query_nope,
        w_query_rope,
        w_latent,
        w_key_rope.T,
        scratch=[pltpu.VMEM((nk, nt, sent_width), BF)],
        flops=WAIT,
    )
    pairs = nt * heads
    chunk = -(-ff_dev // (nk * 128)) * 128
    wide = 2 * chunk + 128
    base_parts = call(
        base_kernel,
        [like((rows, wide))] * nk,
        x_rows,
        gains,
        w_gate.T,
        w_up.T,
        scratch=[pltpu.VMEM((nk, rows, wide), BF)],
        flops=WAIT,
    )[::-1]
    msg, new_latent, new_rope_key, own_block = call(
        functools.partial(latent_kernel, model_width),
        [
            like((nk, pairs, latent + 128)),
            like((own, latent)),
            like((own, rope)),
            like((nt, latent + 128), F32),
        ],
        *deal(msg[::-1], "kv"),
        key_flat,
        latent_gain.reshape(1, latent),
        jnp.asarray(table),
        unit,
        flops=WAIT,
    )
    got = exchange(msg.reshape(nk * nt, heads, latent + 128), ("kv", "tp"))
    msg = call(
        functools.partial(attend_kernel, (nope + rope) ** (-0.5)),
        like((own, pairs, latent + 128)),
        got.reshape(own, pairs, latent + 128),
        cache_latent,
        cache_rope_key.swapaxes(1, 2),
        own_block,
        flops=WAIT,
    )
    got = exchange(msg.reshape(nk * nt, heads, latent + 128), ("kv", "tp"))
    msg = call(
        functools.partial(value_kernel, heads),
        [like((nt, value_dev + own * wide))] * nk,
        got.reshape(nk, pairs, latent + 128),
        value_flat,
        *base_parts,
        flops=WAIT,
    )
    half = width // 2
    keep, give, base = call(
        out_kernel,
        [like((rows, half), F32), like((rows, half)), like((rows, wide), F32)],
        *deal(msg[::-1], "kv"),
        w_out,
        scratch=[pltpu.VMEM((nk, nt, value_dev), F32)],
        flops=WAIT,
    )
    pair = call(
        pair_kernel, like((rows, half)), keep, lax.ppermute(give, "tp", swap), flops=WAIT
    )
    att_half = call(column_kernel, like((rows, half)), *deal([pair] * chips, "tp", 2), flops=WAIT)
    att_other = lax.ppermute(att_half, "tp", swap)
    early = call(
        early_kernel,
        [like((rows, ff_dev), F32)] * 2,
        att_half,
        gains,
        w_gate.T,
        w_up.T,
        flops=WAIT,
    )
    *msg, post = call(
        gate_kernel,
        [like((rows, wide))] * nk + [like((rows, width), F32)],
        att_half,
        att_other,
        *early,
        x_rows,
        gains,
        w_gate.T,
        w_up.T,
        scratch=[pltpu.VMEM((nk, rows, wide), BF)],
        flops=WAIT,
    )
    hidden, s = call(
        functools.partial(hidden_kernel, model_width),
        [like((rows, chunk)), like((rows, 128), F32)],
        *deal(msg[::-1], "kv"),
        base,
        flops=WAIT,
    )
    keep, give = call(
        down_kernel,
        [like((chips, own, width), F32), like((chips, own, width))],
        *deal([hidden] * nk, "kv"),
        w_down,
        scratch=[pltpu.VMEM((nk, rows, chunk), BF), pltpu.VMEM((own, nt, width), F32)],
        flops=WAIT,
    )
    msg = call(
        chips_kernel,
        [like((own, width))] * chips,
        keep,
        lax.ppermute(give, "tp", swap),
        flops=WAIT,
    )
    next_resid = call(
        last_kernel, like((own, width)), *deal(msg[::-1], "tp", 2), resid, post, s, flops=WAIT
    )
    return (next_resid, new_latent, new_rope_key)


def body(*args):
    resid, key_up, cache = args[0], args[7], args[15]
    nk, nt = lax.axis_size("kv"), lax.axis_size("tp")
    own, width = resid.shape
    latent, heads, nope = key_up.shape
    fits = (
        own == nk == 4
        and nt == 8
        and heads == 8
        and 2 * own == nt
        and width % 1024 == 0
        and latent % 256 == 0
        and nope % 128 == 0
        and cache.shape[1] % 128 == 0
        and args[16].shape[2] == 64
    )
    if not fits:
        return plain_body(*args)
    return kernel_body(*args)


def solution(mesh):
    return jax.shard_map(
        body,
        mesh=mesh,
        in_specs=(
            P("tp", "kv"),
            P(),
            P("kv", "tp"),
            P("kv", "tp"),
            P("kv", None),
            P(),
            P(),
            P(None, "tp", None),
            P(None, "tp", None),
            P("tp", "kv"),
            P(),
            P(),
            P("kv", "tp"),
            P("kv", "tp"),
            P("tp", "kv"),
            P("tp", "kv", None),
            P("tp", "kv", None),
        ),
        out_specs=(P("tp", "kv"), P("tp", None), P("tp", None)),
        check_vma=False,
    )
```

```python
import functools

import jax
import jax.numpy as jnp
import numpy as np
from jax import lax
from jax.experimental import pallas as pl
from jax.experimental.pallas import tpu as pltpu
from jax.sharding import PartitionSpec as P


EPS = 1e-06
THETA = 10000.0
BF = jnp.bfloat16
F32 = jnp.float32


def rotate(vector, position):
    half_width = vector.shape[-1] // 2
    frequency = THETA ** (-jnp.arange(half_width, dtype=F32) / half_width)
    angles = jnp.asarray(position, F32) * frequency
    cos_table, sin_table = (jnp.cos(angles), jnp.sin(angles))
    lower_half, upper_half = (vector[..., :half_width], vector[..., half_width:])
    return jnp.concatenate(
        [
            lower_half * cos_table - upper_half * sin_table,
            lower_half * sin_table + upper_half * cos_table,
        ],
        axis=-1,
    )


def dot(a, b):
    return jnp.dot(a, b, preferred_element_type=F32)


def pieces(value, count):
    out, rest = [], value
    for _ in range(count):
        term = lax.reduce_precision(rest, 8, 7)
        out.append(term.astype(BF))
        rest = rest - term
    return out


def spread(block, axis, groups=None):
    count = len(groups[0]) if groups else lax.axis_size(axis)
    copies = jnp.broadcast_to(block[None], (count,) + block.shape)
    return lax.all_to_all(copies, axis, 0, 0, tiled=True, axis_index_groups=groups)


def plain_body(
    resid,
    attn_gain,
    w_query_nope,
    w_query_rope,
    w_latent,
    w_key_rope,
    latent_gain,
    key_up,
    value_up,
    w_out,
    post_gain,
    mlp_gain,
    w_gate,
    w_up,
    w_down,
    cache_latent,
    cache_rope_key,
):
    nk = lax.axis_size("kv")
    nt = lax.axis_size("tp")
    kv_index = lax.axis_index("kv")
    tp_index = lax.axis_index("tp")
    own, width = resid.shape
    rows = own * nt
    model_width = width * nk
    latent, heads, nope = key_up.shape
    value_width = value_up.shape[2]
    rope = cache_rope_key.shape[2]
    pos_dev = cache_latent.shape[1]
    context = pos_dev * nk
    score_scale = (nope + rope) ** (-0.5)
    col_start = kv_index * width
    split_rows = own % nk == 0

    def block_of(vector):
        return lax.dynamic_slice_in_dim(vector, col_start, width, 0).astype(F32)[None, :]

    gathered = spread(resid, "tp").swapaxes(0, 1).reshape(rows, width)
    gathered_float = gathered.astype(F32)
    gain_a = block_of(attn_gain)
    normed_a = (gathered_float * gain_a).astype(BF)
    own_normed = (resid.astype(F32) * gain_a).astype(BF)
    key_rows = lax.dynamic_slice_in_dim(w_key_rope, col_start, width, 0)
    squares = jnp.sum(gathered_float * gathered_float, axis=1, keepdims=True)
    own_squares = jnp.sum(resid.astype(F32) ** 2, axis=1, keepdims=True)
    q_part = jnp.concatenate(
        [
            dot(normed_a, w_query_nope).astype(BF),
            dot(normed_a, w_query_rope).astype(BF),
            *pieces(squares, 2),
            jnp.zeros((rows, 126), BF),
        ],
        axis=1,
    )
    own_part = jnp.concatenate(
        [
            dot(own_normed, w_latent).astype(BF),
            dot(own_normed, key_rows).astype(BF),
            *pieces(own_squares, 2),
        ],
        axis=1,
    )
    nope_dev, rope_dev = heads * nope, heads * rope
    q_width, own_width = q_part.shape[1], own_part.shape[1]
    sent_width = max(q_width, own_width)
    q_part = jnp.pad(q_part, ((0, 0), (0, sent_width - q_width)))
    own_part = jnp.pad(own_part, ((0, 0), (0, sent_width - own_width)))
    summed = jnp.sum(
        spread(jnp.concatenate([q_part, own_part], axis=0), "kv").astype(F32), axis=0
    )
    q_sum, own_sum = summed[:rows], summed[rows:, :own_width]
    square_sum = jnp.sum(q_sum[:, nope_dev + rope_dev :], axis=1, keepdims=True)
    scale_in = lax.rsqrt(square_sum / model_width + EPS)
    q_nope = (q_sum[:, :nope_dev] * scale_in).astype(BF).reshape(rows, heads, nope)
    q_rope = rotate(
        (q_sum[:, nope_dev : nope_dev + rope_dev] * scale_in).reshape(rows, heads, rope), context
    ).astype(BF)
    latent_sum = own_sum[:, :latent]
    own_scale = lax.rsqrt(
        jnp.sum(own_sum[:, latent + rope :], axis=1, keepdims=True) / model_width + EPS
    )
    new_latent = (
        latent_sum
        * lax.rsqrt(jnp.mean(latent_sum * latent_sum, axis=1, keepdims=True) + EPS)
        * latent_gain.astype(F32)[None, :]
    ).astype(BF)
    new_rope_key = rotate(own_sum[:, latent : latent + rope] * own_scale, context).astype(BF)
    q_lat = jnp.einsum("bhd,chd->bhc", q_nope, key_up, preferred_element_type=F32).astype(BF)

    query = jnp.concatenate([q_lat, q_rope], axis=-1).reshape(own, nt, heads, latent + rope)
    query = lax.all_to_all(query.swapaxes(0, 1), "tp", 0, 0, tiled=True)
    query = query.transpose(1, 0, 2, 3).reshape(own, nt * heads, latent + rope)
    all_heads = nt * heads
    seq_lat, seq_rope = query[..., :latent], query[..., latent:]
    scores = (
        jnp.einsum("bhc,bpc->bhp", seq_lat, cache_latent, preferred_element_type=F32)
        + jnp.einsum("bhr,bpr->bhp", seq_rope, cache_rope_key, preferred_element_type=F32)
    ) * score_scale
    own_score = (
        jnp.einsum("bhc,bc->bh", seq_lat, new_latent, preferred_element_type=F32)
        + jnp.einsum("bhr,br->bh", seq_rope, new_rope_key, preferred_element_type=F32)
    ) * score_scale
    peak = jnp.maximum(jnp.max(scores, axis=2), own_score)
    probs = jnp.exp(scores - peak[:, :, None])
    own_prob = jnp.where(kv_index == 0, jnp.exp(own_score - peak), 0.0)
    totals = jnp.sum(probs, axis=2) + own_prob
    partial_value = (
        jnp.einsum("bhp,bpc->bhc", probs.astype(BF), cache_latent, preferred_element_type=F32)
        + own_prob[:, :, None] * new_latent.astype(F32)[:, None, :]
    )
    packed = jnp.concatenate(
        [partial_value.astype(BF)]
        + [p[:, :, None] for p in pieces(peak, 3) + pieces(totals, 3)]
        + [jnp.zeros((own, all_heads, 122), BF)],
        axis=2,
    )

    def combine(blocks):
        stats = blocks[..., latent:].astype(F32)
        peaks = jnp.sum(stats[..., :3], axis=-1, keepdims=True)
        sums = jnp.sum(stats[..., 3:6], axis=-1, keepdims=True)
        factor = jnp.exp(peaks - jnp.max(peaks, axis=0, keepdims=True))
        value = jnp.sum(blocks[..., :latent].astype(F32) * factor, axis=0)
        return (value / jnp.sum(sums * factor, axis=0)).astype(BF)

    if split_rows:
        per = own // nk
        sent = packed.reshape(nk, per, nt, heads, latent + 128).swapaxes(1, 2)
        sent = sent.reshape(nk * nt, per, heads, latent + 128)
        got = lax.all_to_all(sent, ("kv", "tp"), 0, 0, tiled=True)
        got = got.reshape(nk, nt, per, heads, latent + 128)
        o_lat = combine(got).swapaxes(0, 1).reshape(per * nt, heads, latent)
    else:
        flat = own * all_heads // nk
        got = lax.all_to_all(packed.reshape(nk, flat, latent + 128), "kv", 0, 0, tiled=True)
        o_own = spread(combine(got), "kv").reshape(own, nt, heads, latent)
        o_lat = lax.all_to_all(o_own.swapaxes(0, 1), "tp", 0, 0, tiled=True)
        o_lat = o_lat.swapaxes(0, 1).reshape(rows, heads, latent)
    o_heads = jnp.einsum("bhc,che->bhe", o_lat, value_up, preferred_element_type=F32).astype(BF)
    o_flat = o_heads.reshape(-1, heads * value_width)
    if split_rows:
        o_flat = spread(o_flat, "kv").reshape(rows, heads * value_width)

    core = lax.rem(tp_index, 2)
    swap = [(i, i ^ 1) for i in range(nt)]
    column = [list(range(c, nt, 2)) for c in range(2)]
    half = width // 2
    out_part = dot(o_flat, w_out).reshape(rows, 2, half)
    keep = jnp.where(core == 0, out_part[:, 0], out_part[:, 1])
    give = jnp.where(core == 0, out_part[:, 1], out_part[:, 0]).astype(BF)
    pair_sum = (keep + lax.ppermute(give, "tp", swap).astype(F32)).astype(BF)
    att_half = jnp.sum(spread(pair_sum, "tp", column).astype(F32), axis=0).astype(BF)
    att_other = lax.ppermute(att_half, "tp", swap)
    attended = jnp.where(
        core == 0,
        jnp.concatenate([att_half, att_other], axis=1),
        jnp.concatenate([att_other, att_half], axis=1),
    ).astype(F32)

    gain_m = block_of(mlp_gain)
    post = attended * block_of(post_gain)
    stacked = jnp.concatenate(
        [(gathered_float * gain_m).astype(BF), (post * gain_m).astype(BF)], axis=0
    )
    ff_dev = w_gate.shape[1]
    stats = [
        jnp.sum(a * b, axis=1, keepdims=True)
        for a, b in (
            (attended, attended),
            (gathered_float, gathered_float),
            (gathered_float, post),
            (post, post),
        )
    ]
    stat_block = jnp.concatenate(
        [jnp.concatenate(pieces(jnp.concatenate(stats[2 * i : 2 * i + 2], axis=0), 2), axis=1)
         for i in range(2)],
        axis=1,
    )
    ff_part = jnp.concatenate(
        [
            dot(stacked, w_gate).astype(BF),
            dot(stacked, w_up).astype(BF),
            stat_block,
        ],
        axis=1,
    )
    ff_sum = jnp.sum(spread(ff_part, "kv").astype(F32), axis=0)
    first = jnp.sum(ff_sum[:, 2 * ff_dev : 2 * ff_dev + 2], axis=1, keepdims=True)
    second = jnp.sum(ff_sum[:, 2 * ff_dev + 2 :], axis=1, keepdims=True)
    att_square, resid_square, cross, post_square = (
        first[:rows],
        first[rows:],
        second[:rows],
        second[rows:],
    )
    s = lax.rsqrt(att_square / model_width + EPS)
    mid_square = resid_square + 2.0 * s * cross + s * s * post_square
    scale_mid = lax.rsqrt(jnp.maximum(mid_square, 0.0) / model_width + EPS)
    mixed = (ff_sum[:rows] + s * ff_sum[rows:]) * scale_mid
    hidden = (jax.nn.silu(mixed[:, :ff_dev]) * mixed[:, ff_dev : 2 * ff_dev]).astype(BF)
    down = dot(hidden, w_down).astype(BF).reshape(own, nt, width).swapaxes(0, 1)
    lowered = jnp.sum(lax.all_to_all(down, "tp", 0, 0, tiled=True).astype(F32), axis=0)

    own_post = lax.dynamic_slice_in_dim(post.reshape(own, nt, width), tp_index, 1, 1)[:, 0]
    own_s = lax.dynamic_slice_in_dim(s.reshape(own, nt, 1), tp_index, 1, 1)[:, 0]
    resid_mid = (resid.astype(F32) + own_s * own_post).astype(BF).astype(F32)
    next_resid = (resid_mid + lowered).astype(BF)
    return (next_resid, new_latent, new_rope_key)


VMEM = pl.BlockSpec(memory_space=pltpu.VMEM)
WAIT = 4_000_000_000
NT = (((1,), (1,)), ((), ()))


def call(kernel, outs, *args, flops=0, scratch=()):
    many = isinstance(outs, (list, tuple))
    sizes = list(args) + (list(outs) if many else [outs])
    moved = sum(int(np.prod(a.shape)) * a.dtype.itemsize for a in sizes)
    return pl.pallas_call(
        kernel,
        out_shape=outs,
        in_specs=[VMEM] * len(args),
        out_specs=[VMEM] * len(outs) if many else VMEM,
        scratch_shapes=list(scratch),
        compiler_params=pltpu.CompilerParams(vmem_limit_bytes=16 << 20),
        cost_estimate=pl.CostEstimate(
            flops=max(flops, moved), bytes_accessed=moved, transcendentals=0
        ),
    )(*args)


def like(shape, dtype=BF):
    return jax.ShapeDtypeStruct(shape, dtype)


def lane_of(shape):
    return lax.broadcasted_iota(jnp.int32, shape, len(shape) - 1)


def terms(value, count):
    out, rest = [], value
    for _ in range(count):
        term = rest.astype(BF).astype(F32)
        out.append(term)
        rest = rest - term
    return out


def placed(columns, shape):
    lane = lane_of(shape)
    block = jnp.zeros(shape, F32)
    for at, column in columns:
        block = jnp.where(lane == at, column, block)
    return block


def picked(block, first, count):
    lane = lane_of(block.shape)
    inside = (lane >= first) & (lane < first + count)
    return jnp.sum(jnp.where(inside, block, 0.0), axis=-1, keepdims=True)


def turned(vector, table, half):
    width = vector.shape[1]
    low = lax.rem(lane_of(vector.shape), 2 * half) < half
    other = jnp.where(
        low, pltpu.roll(vector, width - half, 1), pltpu.roll(vector, half, 1)
    )
    return vector * table[0:1, :width] + other * table[1:2, :width]


def other(axis, k, step=1):
    return jnp.bitwise_xor(lax.div(lax.axis_index(axis), step), k)


def unit_kernel(out_ref):
    row = lax.rem(lax.broadcasted_iota(jnp.int32, out_ref.shape, 0), out_ref.shape[1] // 2)
    out_ref[...] = jnp.where(row == lane_of(out_ref.shape), 1.0, 0.0).astype(BF)


def start_kernel(b0, b1, b2, b3, unit_ref, out_ref, held_ref):
    chips, own, _ = held_ref.shape
    for k, ref in enumerate((b0, b1, b2, b3)):
        held_ref[other("tp", k, 2)] = ref[...].astype(F32)
    out_ref[...] = jnp.concatenate(
        [held_ref[z, r : r + 1, :] for r in range(own) for z in range(chips)], axis=0
    ).astype(BF)


def own_kernel(resid_ref, ga_ref, gp_ref, gm_ref, wl_ref, wk_ref, gains_ref, own_ref):
    own, width = resid_ref.shape
    nt = own_ref.shape[0]
    latent, rope = wl_ref.shape[1], wk_ref.shape[0]
    tiles = width // 128
    at = pl.multiple_of(lax.axis_index("kv") * tiles, tiles)
    gains = []
    for ref in (ga_ref, gp_ref, gm_ref):
        block = ref[pl.ds(at, tiles), :].astype(F32)
        gains.append(jnp.concatenate([block[i : i + 1] for i in range(tiles)], axis=1))
    gains_ref[...] = jnp.concatenate(gains + [jnp.zeros((8 - len(gains), width), F32)], axis=0)
    mine = jnp.concatenate([resid_ref[...].astype(F32), jnp.zeros((nt - own, width), F32)], axis=0)
    own_normed = (mine * gains[0]).astype(BF)
    lat = jnp.dot(own_normed, wl_ref[...], preferred_element_type=F32)
    at = pl.multiple_of(lax.axis_index("kv") * width, width)
    key = lax.dot_general(own_normed, wk_ref[:, pl.ds(at, width)], NT, preferred_element_type=F32)
    half = latent // 2
    own_ref[:, :half] = lat[:, :half] + pltpu.roll(lat[:, half:], own, 0)
    key = jnp.concatenate([key, jnp.zeros((nt, 128 - rope), F32)], axis=1)
    squares = terms(jnp.sum(mine * mine, axis=1, keepdims=True), 2)
    stat = placed([(rope + i, c) for i, c in enumerate(squares)], key.shape)
    own_ref[:, half:] = jnp.where(lane_of(key.shape) < rope, key, stat)


def query_kernel(
    rope, half_ref, other_ref, gains_ref, own_ref, wn_ref, wr_ref, m3, m2, m1, m0, rows_ref, sent_ref
):
    nt = own_ref.shape[0]
    nope_dev, rope_dev = wn_ref.shape[1], wr_ref.shape[1]
    first = lax.rem(lax.axis_index("tp"), 2) == 0
    mine, theirs = half_ref[...].astype(F32), other_ref[...].astype(F32)
    cores = (jnp.where(first, mine, theirs), jnp.where(first, theirs, mine))
    x = jnp.concatenate(
        [core[i : i + 1] for i in range(mine.shape[0]) for core in cores], axis=0
    )
    rows_ref[...] = x.astype(BF)
    gain = gains_ref[0:1, :]
    normed = (x * gain).astype(BF)
    qn = jnp.dot(normed, wn_ref[...], preferred_element_type=F32)
    qr = jnp.dot(normed, wr_ref[...], preferred_element_type=F32)
    square = jnp.sum(x * x, axis=1, keepdims=True)
    half = own_ref.shape[1] - 128
    lat, key = own_ref[:, :half], own_ref[:, half:]
    lane = lane_of(key.shape)
    for r in range(sent_ref.shape[0]):
        part = slice(r * nt, (r + 1) * nt)
        sent_ref[r, :, :nope_dev] = qn[part].astype(BF)
        sent_ref[r, :, nope_dev : nope_dev + rope_dev] = qr[part].astype(BF)
        base = nope_dev + rope_dev
        sent_ref[r, :, base : base + half] = lat.astype(BF)
        block = key
        for i, column in enumerate(terms(square[part], 2)):
            block = jnp.where(lane == rope + 2 + i, column, block)
        sent_ref[r, :, base + half :] = block.astype(BF)
    for k, ref in enumerate((m0, m1, m2, m3)):
        ref[...] = sent_ref[other("kv", k)]


def four(refs):
    a, b, c, d = (ref[...].astype(F32) for ref in refs)
    return (a + b) + (c + d)


def latent_kernel(
    model_width, b0, b1, b2, b3, ku_ref, gain_ref, table_ref, unit_ref,
    msg_ref, lat_ref, key_ref, own_ref,
):
    nk, pairs, _ = msg_ref.shape
    nt = b0.shape[0]
    heads = pairs // nt
    latent, _, nope = ku_ref.shape
    nope_dev = heads * nope
    own, rope = key_ref.shape
    rope_dev = heads * rope
    total = four((b0, b1, b2, b3))
    base, half = nope_dev + rope_dev, latent // 2
    stat = total[:, base + half :]
    scale = lax.rsqrt(picked(stat, rope + 2, 2) / model_width + EPS)
    own_scale = lax.rsqrt(picked(stat, rope, 2) / model_width + EPS)
    lat = total[:, base : base + half]
    lat = jnp.concatenate([lat, pltpu.roll(lat, own, 0)], axis=1)
    lat = lat * lax.rsqrt(jnp.mean(lat * lat, axis=1, keepdims=True) + EPS)
    lat = (lat * gain_ref[...].astype(F32)).astype(BF)
    table = table_ref[...]
    key = turned(stat * own_scale, table, rope // 2).astype(BF)
    lat_ref[...] = lat[:own]
    key_ref[...] = key[:own, :rope]
    own_ref[:, :latent] = lat.astype(F32)
    own_ref[:, latent:] = key.astype(F32)
    qn = total[:, :nope_dev].astype(BF).astype(F32)
    qr = turned(total[:, nope_dev:base] * scale, table, rope // 2).astype(BF).astype(F32)

    def diagonal(q, size):
        shape = (nt, heads, heads * size)
        head = lax.broadcasted_iota(jnp.int32, shape, 1)
        lane = lax.broadcasted_iota(jnp.int32, shape, 2)
        keep = (lane >= head * size) & (lane < (head + 1) * size)
        spread_q = jnp.broadcast_to(q[:, None, :], shape)
        return jnp.where(keep, spread_q, 0.0).reshape(nt * heads, heads * size).astype(BF)

    raw = lax.dot_general(
        diagonal(qn, nope), ku_ref[...].reshape(latent, nope_dev), NT, preferred_element_type=F32
    )
    scales = jnp.broadcast_to(scale[:, None, :], (nt, heads, latent)).reshape(pairs, latent)
    q_lat = (raw * scales).astype(BF)
    q_rope = jnp.dot(diagonal(qr, rope), unit_ref[...], preferred_element_type=F32).astype(BF)
    for j in range(nk):
        msg_ref[j, :, :latent] = q_lat
        msg_ref[j, :, latent:] = q_rope


def attend_kernel(score_scale, q_ref, cache_ref, rope_ref, own_ref, msg_ref):
    own, all_heads, _ = q_ref.shape
    latent = cache_ref.shape[2]
    rope = rope_ref.shape[1]
    holds_own = lax.axis_index("kv") == 0
    lat, key = own_ref[:, :latent], own_ref[:, latent : latent + rope]
    seqs = range(own)
    q_lat = [q_ref[r, :, :latent] for r in seqs]
    q_rope = [q_ref[r, :, latent : latent + rope] for r in seqs]
    scores = [
        (
            lax.dot_general(q_lat[r], cache_ref[r], NT, preferred_element_type=F32)
            + jnp.dot(q_rope[r], rope_ref[r], preferred_element_type=F32)
        )
        * score_scale
        for r in seqs
    ]
    own_scores = [
        (
            jnp.sum(q_lat[r].astype(F32) * lat[r : r + 1], axis=1, keepdims=True)
            + jnp.sum(q_rope[r].astype(F32) * key[r : r + 1], axis=1, keepdims=True)
        )
        * score_scale
        for r in seqs
    ]
    peaks = [
        jnp.maximum(jnp.max(scores[r], axis=1, keepdims=True), own_scores[r]) for r in seqs
    ]
    probs = [jnp.exp(scores[r] - peaks[r]) for r in seqs]
    values = [
        jnp.dot(probs[r].astype(BF), cache_ref[r], preferred_element_type=F32) for r in seqs
    ]
    for r in seqs:
        own_prob = jnp.where(holds_own, jnp.exp(own_scores[r] - peaks[r]), 0.0)
        total = jnp.sum(probs[r], axis=1, keepdims=True) + own_prob
        msg_ref[r, :, :latent] = (values[r] + own_prob * lat[r : r + 1]).astype(BF)
        columns = list(enumerate(terms(peaks[r], 3) + terms(total, 3)))
        msg_ref[r, :, latent:] = placed(columns, (all_heads, 128)).astype(BF)


def value_kernel(heads, got_ref, vu_ref, a0, a1, a2, a3, m3, m2, m1, m0):
    nk, pairs, _ = got_ref.shape
    latent, _, size = vu_ref.shape
    value_dev = heads * size
    nt = pairs // heads
    stats = [got_ref[j, :, latent:].astype(F32) for j in range(nk)]
    peaks = [picked(s, 0, 3) for s in stats]
    peak = functools.reduce(jnp.maximum, peaks)
    factors = [jnp.exp(p - peak) for p in peaks]
    total = sum(picked(s, 3, 3) * f for s, f in zip(stats, factors))
    value = sum(got_ref[j, :, :latent].astype(F32) * f for j, f in enumerate(factors))
    o_lat = (value / total).astype(BF)
    full = jnp.dot(o_lat, vu_ref[...].reshape(latent, value_dev), preferred_element_type=F32)
    shape = (nt, heads, value_dev)
    head = lax.broadcasted_iota(jnp.int32, shape, 1)
    lane = lax.broadcasted_iota(jnp.int32, shape, 2)
    keep = (lane >= head * size) & (lane < (head + 1) * size)
    o_heads = jnp.sum(jnp.where(keep, full.reshape(shape), 0.0), axis=1).astype(BF)
    rows, wide = a0.shape
    for a, m in ((a3, m3), (a2, m2), (a1, m1), (a0, m0)):
        m[:, :value_dev] = o_heads
        for g in range(rows // nt):
            m[:, value_dev + g * wide : value_dev + (g + 1) * wide] = a[g * nt : (g + 1) * nt]


def out_kernel(b0, b1, b2, b3, w_ref, keep_ref, give_ref, base_ref, held_ref):
    half = keep_ref.shape[1]
    _, nt, value_dev = held_ref.shape
    rows, wide = base_ref.shape
    for k, ref in enumerate((b0, b1, b2, b3)):
        held_ref[other("kv", k)] = ref[:, :value_dev].astype(F32)
    for g in range(rows // nt):
        lo = value_dev + g * wide
        a, b, c, d = (ref[:, lo : lo + wide].astype(F32) for ref in (b0, b1, b2, b3))
        base_ref[g * nt : (g + 1) * nt] = (a + b) + (c + d)
    first = lax.rem(lax.axis_index("tp"), 2) == 0
    o_heads = held_ref[...].reshape(keep_ref.shape[0], w_ref.shape[0]).astype(BF)
    out = jnp.dot(o_heads, w_ref[...], preferred_element_type=F32)
    keep_ref[...] = jnp.where(first, out[:, :half], out[:, half:])
    give_ref[...] = jnp.where(first, out[:, half:], out[:, :half]).astype(BF)


def pair_kernel(keep_ref, got_ref, out_ref):
    out_ref[...] = (keep_ref[...] + got_ref[...].astype(F32)).astype(BF)


def column_kernel(b0, b1, b2, b3, out_ref):
    out_ref[...] = four((b0, b1, b2, b3)).astype(BF)


def added(a, b):
    return jnp.sum(a * b, axis=1, keepdims=True)


def send_parts(parts, sums, refs, msg_ref):
    nk, rows, wide = msg_ref.shape
    chunk = parts[0].shape[1] // nk
    columns = list(enumerate(t for value in sums for t in terms(value, 3)))
    stat = placed(columns, (rows, 128))[:, : wide - 2 * chunk]
    for j in range(nk):
        block = slice(j * chunk, (j + 1) * chunk)
        msg_ref[j] = jnp.concatenate([part[:, block] for part in parts] + [stat], axis=1).astype(BF)
    for k, ref in enumerate(refs):
        ref[...] = msg_ref[other("kv", k)]


def base_kernel(rows_ref, gains_ref, wg_ref, wu_ref, m3, m2, m1, m0, msg_ref):
    x = rows_ref[...].astype(F32)
    left = (x * gains_ref[2:3, :]).astype(BF)
    parts = [
        lax.dot_general(left, w[...], NT, preferred_element_type=F32) for w in (wg_ref, wu_ref)
    ]
    send_parts(parts, [added(x, x)], (m0, m1, m2, m3), msg_ref)


def half_products(half_ref, core, gains_ref, wg_ref, wu_ref):
    half = half_ref.shape[1]
    at = pl.ds(pl.multiple_of(core * half, half), half)
    gain = gains_ref[1:3, at]
    left = (half_ref[...].astype(F32) * gain[0:1] * gain[1:2]).astype(BF)
    return [
        lax.dot_general(left, w[:, at], NT, preferred_element_type=F32) for w in (wg_ref, wu_ref)
    ]


def early_kernel(half_ref, gains_ref, wg_ref, wu_ref, gate_ref, up_ref):
    core = lax.rem(lax.axis_index("tp"), 2)
    gate_ref[...], up_ref[...] = half_products(half_ref, core, gains_ref, wg_ref, wu_ref)


def gate_kernel(
    half_ref, other_ref, gate_ref, up_ref, rows_ref, gains_ref, wg_ref, wu_ref,
    m3, m2, m1, m0, post_ref, msg_ref,
):
    core = lax.rem(lax.axis_index("tp"), 2)
    late = half_products(other_ref, 1 - core, gains_ref, wg_ref, wu_ref)
    parts = [gate_ref[...] + late[0], up_ref[...] + late[1]]
    mine, theirs = half_ref[...].astype(F32), other_ref[...].astype(F32)
    first = core == 0
    att = jnp.concatenate(
        [jnp.where(first, mine, theirs), jnp.where(first, theirs, mine)], axis=1
    )
    x = rows_ref[...].astype(F32)
    post = att * gains_ref[1:2, :]
    post_ref[...] = post
    sums = [added(att, att), added(x, post), added(post, post)]
    send_parts(parts, sums, (m0, m1, m2, m3), msg_ref)


def hidden_kernel(model_width, b0, b1, b2, b3, base_ref, out_ref, s_ref):
    _, chunk = out_ref.shape
    total, base = four((b0, b1, b2, b3)), base_ref[...]
    tail = total.shape[1] - 128
    at = 2 * chunk - tail
    x_square = picked(base[:, tail:], at, 3)
    att_square, cross, post_square = (picked(total[:, tail:], at + 3 * i, 3) for i in range(3))
    s = lax.rsqrt(att_square / model_width + EPS)
    mid = jnp.maximum(x_square + 2.0 * s * cross + s * s * post_square, 0.0)
    scale = lax.rsqrt(mid / model_width + EPS)
    s_ref[...] = jnp.broadcast_to(s, s_ref.shape)
    mixed = (base[:, : 2 * chunk] + s * total[:, : 2 * chunk]) * scale
    gate, up = mixed[:, :chunk], mixed[:, chunk : 2 * chunk]
    out_ref[...] = (gate / (1.0 + jnp.exp(-gate)) * up).astype(BF)


def down_part(hidden_ref, w_ref, k):
    chunk = hidden_ref.shape[1]
    at = pl.multiple_of(other("kv", k) * chunk, 8)
    return jnp.dot(hidden_ref[...], w_ref[pl.ds(at, chunk), :], preferred_element_type=F32)


def first_kernel(hidden_ref, w_ref, out_ref):
    out_ref[...] = down_part(hidden_ref, w_ref, 0)


def down_kernel(first_ref, b1, b2, b3, w_ref, keep_ref, give_ref, total_ref):
    total = first_ref[...]
    for k, ref in ((1, b1), (2, b2), (3, b3)):
        total = total + down_part(ref, w_ref, k)
    total_ref[...] = total.reshape(total_ref.shape)
    core = lax.rem(lax.axis_index("tp"), 2)
    for k in range(keep_ref.shape[0]):
        at = 2 * other("tp", k, 2)
        keep_ref[k] = total_ref[:, at + core, :]
        give_ref[k] = total_ref[:, at + 1 - core, :].astype(BF)


def chips_kernel(keep_ref, got_ref, m3, m2, m1, m0):
    for k, ref in enumerate((m0, m1, m2, m3)):
        ref[...] = (keep_ref[k] + got_ref[k].astype(F32)).astype(BF)


def last_kernel(b0, b1, b2, b3, resid_ref, post_ref, s_ref, out_ref):
    own, width = resid_ref.shape
    nt = post_ref.shape[0] // own
    total = four((b0, b1, b2, b3))
    added = (post_ref[...] * s_ref[:, 0:1]).reshape(own, nt, width)
    here = lax.broadcasted_iota(jnp.int32, added.shape, 1) == lax.axis_index("tp")
    mine = jnp.sum(jnp.where(here, added, 0.0), axis=1)
    mid = (resid_ref[...].astype(F32) + mine).astype(BF).astype(F32)
    out_ref[...] = (mid + total).astype(BF)


def exchange(message, axis):
    return lax.all_to_all(message, axis, 0, 0, tiled=True)


def deal(blocks, axis, step=1):
    size = lax.axis_size(axis)
    out = list(blocks)
    for k in reversed(range(1, len(blocks))):
        out[k] = lax.ppermute(blocks[k], axis, [(i, i ^ (k * step)) for i in range(size)])
    return out


def kernel_body(
    resid,
    attn_gain,
    w_query_nope,
    w_query_rope,
    w_latent,
    w_key_rope,
    latent_gain,
    key_up,
    value_up,
    w_out,
    post_gain,
    mlp_gain,
    w_gate,
    w_up,
    w_down,
    cache_latent,
    cache_rope_key,
):
    nk = lax.axis_size("kv")
    nt = lax.axis_size("tp")
    own, width = resid.shape
    rows = own * nt
    model_width = width * nk
    latent, heads, nope = key_up.shape
    rope = cache_rope_key.shape[2]
    nope_dev, rope_dev = heads * nope, heads * rope
    ff_dev = w_gate.shape[1]
    context = cache_latent.shape[1] * nk
    half_rope = rope // 2
    angles = context * THETA ** (-np.arange(half_rope) / half_rope)
    cos, sin = np.cos(angles), np.sin(angles)
    table = np.zeros((8, rope_dev), np.float32)
    table[0] = np.tile(np.concatenate([cos, cos]), heads)
    table[1] = np.tile(np.concatenate([-sin, sin]), heads)

    swap = [(i, i ^ 1) for i in range(nt)]
    chips = nt // 2
    unit = call(unit_kernel, like((rope_dev, 2 * rope)), flops=WAIT)
    value_dev = heads * value_up.shape[2]
    gains, own_rows = call(
        own_kernel,
        [like((8, width), F32), like((nt, latent // 2 + 128), F32)],
        resid,
        *[g.reshape(-1, 128) for g in (attn_gain, post_gain, mlp_gain)],
        w_latent,
        w_key_rope.T,
        flops=WAIT,
    )
    column = call(
        start_kernel,
        like((own * chips, width)),
        *deal([resid] * chips, "tp", 2),
        unit,
        scratch=[pltpu.VMEM((chips, own, width), F32)],
        flops=WAIT,
    )
    sent_width = nope_dev + rope_dev + latent // 2 + 128
    *msg, x_rows = call(
        functools.partial(query_kernel, rope),
        [like((nt, sent_width))] * nk + [like((rows, width))],
        column,
        lax.ppermute(column, "tp", swap),
        gains,
        own_rows,
        w_query_nope,
        w_query_rope,
        scratch=[pltpu.VMEM((nk, nt, sent_width), BF)],
        flops=WAIT,
    )
    pairs = nt * heads
    chunk = ff_dev // nk
    wide = -(-(2 * chunk + 9) // 128) * 128
    base_parts = call(
        base_kernel,
        [like((rows, wide))] * nk,
        x_rows,
        gains,
        w_gate.T,
        w_up.T,
        scratch=[pltpu.VMEM((nk, rows, wide), BF)],
        flops=WAIT,
    )[::-1]
    msg, new_latent, new_rope_key, own_block = call(
        functools.partial(latent_kernel, model_width),
        [
            like((nk, pairs, latent + 128)),
            like((own, latent)),
            like((own, rope)),
            like((nt, latent + 128), F32),
        ],
        *deal(msg[::-1], "kv"),
        key_up,
        latent_gain.reshape(1, latent),
        jnp.asarray(table),
        unit,
        flops=WAIT,
    )
    got = exchange(msg.reshape(nk * nt, heads, latent + 128), ("kv", "tp"))
    msg = call(
        functools.partial(attend_kernel, (nope + rope) ** (-0.5)),
        like((own, pairs, latent + 128)),
        got.reshape(own, pairs, latent + 128),
        cache_latent,
        cache_rope_key.swapaxes(1, 2),
        own_block,
        flops=WAIT,
    )
    got = exchange(msg.reshape(nk * nt, heads, latent + 128), ("kv", "tp"))
    msg = call(
        functools.partial(value_kernel, heads),
        [like((nt, value_dev + own * wide))] * nk,
        got.reshape(nk, pairs, latent + 128),
        value_up,
        *base_parts,
        flops=WAIT,
    )
    half = width // 2
    keep, give, base = call(
        out_kernel,
        [like((rows, half), F32), like((rows, half)), like((rows, wide), F32)],
        *deal(msg[::-1], "kv"),
        w_out,
        scratch=[pltpu.VMEM((nk, nt, value_dev), F32)],
        flops=WAIT,
    )
    pair = call(
        pair_kernel, like((rows, half)), keep, lax.ppermute(give, "tp", swap), flops=WAIT
    )
    att_half = call(column_kernel, like((rows, half)), *deal([pair] * chips, "tp", 2), flops=WAIT)
    att_other = lax.ppermute(att_half, "tp", swap)
    early = call(
        early_kernel,
        [like((rows, ff_dev), F32)] * 2,
        att_half,
        gains,
        w_gate.T,
        w_up.T,
        flops=WAIT,
    )
    *msg, post = call(
        gate_kernel,
        [like((rows, wide))] * nk + [like((rows, width), F32)],
        att_half,
        att_other,
        *early,
        x_rows,
        gains,
        w_gate.T,
        w_up.T,
        scratch=[pltpu.VMEM((nk, rows, wide), BF)],
        flops=WAIT,
    )
    hidden, s = call(
        functools.partial(hidden_kernel, model_width),
        [like((rows, chunk)), like((rows, 128), F32)],
        *deal(msg[::-1], "kv"),
        base,
        flops=WAIT,
    )
    first = call(first_kernel, like((rows, width), F32), hidden, w_down, flops=WAIT)
    keep, give = call(
        down_kernel,
        [like((chips, own, width), F32), like((chips, own, width))],
        first,
        *deal([hidden] * nk, "kv")[1:],
        w_down,
        scratch=[pltpu.VMEM((own, nt, width), F32)],
        flops=WAIT,
    )
    msg = call(
        chips_kernel,
        [like((own, width))] * chips,
        keep,
        lax.ppermute(give, "tp", swap),
        flops=WAIT,
    )
    next_resid = call(
        last_kernel, like((own, width)), *deal(msg[::-1], "tp", 2), resid, post, s, flops=WAIT
    )
    return (next_resid, new_latent, new_rope_key)


def body(*args):
    resid, key_up, cache = args[0], args[7], args[15]
    nk, nt = lax.axis_size("kv"), lax.axis_size("tp")
    own, width = resid.shape
    latent, heads, nope = key_up.shape
    fits = (
        own == nk == 4
        and nt == 8
        and heads == 8
        and 2 * own == nt
        and width % 1024 == 0
        and latent % 256 == 0
        and args[12].shape[1] % (8 * nk) == 0
        and args[12].shape[1] // nk >= 64
        and nope % 128 == 0
        and cache.shape[1] % 128 == 0
        and args[16].shape[2] == 64
    )
    if not fits:
        return plain_body(*args)
    return kernel_body(*args)


def solution(mesh):
    return jax.shard_map(
        body,
        mesh=mesh,
        in_specs=(
            P("tp", "kv"),
            P(),
            P("kv", "tp"),
            P("kv", "tp"),
            P("kv", None),
            P(),
            P(),
            P(None, "tp", None),
            P(None, "tp", None),
            P("tp", "kv"),
            P(),
            P(),
            P("kv", "tp"),
            P("kv", "tp"),
            P("tp", "kv"),
            P("tp", "kv", None),
            P("tp", "kv", None),
        ),
        out_specs=(P("tp", "kv"), P("tp", None), P("tp", None)),
        check_vma=False,
    )
```

```python
import functools

import jax
import jax.numpy as jnp
import numpy as np
from jax import lax
from jax.experimental import pallas as pl
from jax.experimental.pallas import tpu as pltpu
from jax.sharding import PartitionSpec as P


EPS = 1e-06
THETA = 10000.0
BF = jnp.bfloat16
F32 = jnp.float32


def rotate(vector, position):
    half_width = vector.shape[-1] // 2
    frequency = THETA ** (-jnp.arange(half_width, dtype=F32) / half_width)
    angles = jnp.asarray(position, F32) * frequency
    cos_table, sin_table = (jnp.cos(angles), jnp.sin(angles))
    lower_half, upper_half = (vector[..., :half_width], vector[..., half_width:])
    return jnp.concatenate(
        [
            lower_half * cos_table - upper_half * sin_table,
            lower_half * sin_table + upper_half * cos_table,
        ],
        axis=-1,
    )


def dot(a, b):
    return jnp.dot(a, b, preferred_element_type=F32)


def pieces(value, count):
    out, rest = [], value
    for _ in range(count):
        term = lax.reduce_precision(rest, 8, 7)
        out.append(term.astype(BF))
        rest = rest - term
    return out


def spread(block, axis, groups=None):
    count = len(groups[0]) if groups else lax.axis_size(axis)
    copies = jnp.broadcast_to(block[None], (count,) + block.shape)
    return lax.all_to_all(copies, axis, 0, 0, tiled=True, axis_index_groups=groups)


def plain_body(
    resid,
    attn_gain,
    w_query_nope,
    w_query_rope,
    w_latent,
    w_key_rope,
    latent_gain,
    key_up,
    value_up,
    w_out,
    post_gain,
    mlp_gain,
    w_gate,
    w_up,
    w_down,
    cache_latent,
    cache_rope_key,
):
    nk = lax.axis_size("kv")
    nt = lax.axis_size("tp")
    kv_index = lax.axis_index("kv")
    tp_index = lax.axis_index("tp")
    own, width = resid.shape
    rows = own * nt
    model_width = width * nk
    latent, heads, nope = key_up.shape
    value_width = value_up.shape[2]
    rope = cache_rope_key.shape[2]
    pos_dev = cache_latent.shape[1]
    context = pos_dev * nk
    score_scale = (nope + rope) ** (-0.5)
    col_start = kv_index * width
    split_rows = own % nk == 0

    def block_of(vector):
        return lax.dynamic_slice_in_dim(vector, col_start, width, 0).astype(F32)[None, :]

    gathered = spread(resid, "tp").swapaxes(0, 1).reshape(rows, width)
    gathered_float = gathered.astype(F32)
    gain_a = block_of(attn_gain)
    normed_a = (gathered_float * gain_a).astype(BF)
    own_normed = (resid.astype(F32) * gain_a).astype(BF)
    key_rows = lax.dynamic_slice_in_dim(w_key_rope, col_start, width, 0)
    squares = jnp.sum(gathered_float * gathered_float, axis=1, keepdims=True)
    own_squares = jnp.sum(resid.astype(F32) ** 2, axis=1, keepdims=True)
    q_part = jnp.concatenate(
        [
            dot(normed_a, w_query_nope).astype(BF),
            dot(normed_a, w_query_rope).astype(BF),
            *pieces(squares, 2),
            jnp.zeros((rows, 126), BF),
        ],
        axis=1,
    )
    own_part = jnp.concatenate(
        [
            dot(own_normed, w_latent).astype(BF),
            dot(own_normed, key_rows).astype(BF),
            *pieces(own_squares, 2),
        ],
        axis=1,
    )
    nope_dev, rope_dev = heads * nope, heads * rope
    q_width, own_width = q_part.shape[1], own_part.shape[1]
    sent_width = max(q_width, own_width)
    q_part = jnp.pad(q_part, ((0, 0), (0, sent_width - q_width)))
    own_part = jnp.pad(own_part, ((0, 0), (0, sent_width - own_width)))
    summed = jnp.sum(
        spread(jnp.concatenate([q_part, own_part], axis=0), "kv").astype(F32), axis=0
    )
    q_sum, own_sum = summed[:rows], summed[rows:, :own_width]
    square_sum = jnp.sum(q_sum[:, nope_dev + rope_dev :], axis=1, keepdims=True)
    scale_in = lax.rsqrt(square_sum / model_width + EPS)
    q_nope = (q_sum[:, :nope_dev] * scale_in).astype(BF).reshape(rows, heads, nope)
    q_rope = rotate(
        (q_sum[:, nope_dev : nope_dev + rope_dev] * scale_in).reshape(rows, heads, rope), context
    ).astype(BF)
    latent_sum = own_sum[:, :latent]
    own_scale = lax.rsqrt(
        jnp.sum(own_sum[:, latent + rope :], axis=1, keepdims=True) / model_width + EPS
    )
    new_latent = (
        latent_sum
        * lax.rsqrt(jnp.mean(latent_sum * latent_sum, axis=1, keepdims=True) + EPS)
        * latent_gain.astype(F32)[None, :]
    ).astype(BF)
    new_rope_key = rotate(own_sum[:, latent : latent + rope] * own_scale, context).astype(BF)
    q_lat = jnp.einsum("bhd,chd->bhc", q_nope, key_up, preferred_element_type=F32).astype(BF)

    query = jnp.concatenate([q_lat, q_rope], axis=-1).reshape(own, nt, heads, latent + rope)
    query = lax.all_to_all(query.swapaxes(0, 1), "tp", 0, 0, tiled=True)
    query = query.transpose(1, 0, 2, 3).reshape(own, nt * heads, latent + rope)
    all_heads = nt * heads
    seq_lat, seq_rope = query[..., :latent], query[..., latent:]
    scores = (
        jnp.einsum("bhc,bpc->bhp", seq_lat, cache_latent, preferred_element_type=F32)
        + jnp.einsum("bhr,bpr->bhp", seq_rope, cache_rope_key, preferred_element_type=F32)
    ) * score_scale
    own_score = (
        jnp.einsum("bhc,bc->bh", seq_lat, new_latent, preferred_element_type=F32)
        + jnp.einsum("bhr,br->bh", seq_rope, new_rope_key, preferred_element_type=F32)
    ) * score_scale
    peak = jnp.maximum(jnp.max(scores, axis=2), own_score)
    probs = jnp.exp(scores - peak[:, :, None])
    own_prob = jnp.where(kv_index == 0, jnp.exp(own_score - peak), 0.0)
    totals = jnp.sum(probs, axis=2) + own_prob
    partial_value = (
        jnp.einsum("bhp,bpc->bhc", probs.astype(BF), cache_latent, preferred_element_type=F32)
        + own_prob[:, :, None] * new_latent.astype(F32)[:, None, :]
    )
    packed = jnp.concatenate(
        [partial_value.astype(BF)]
        + [p[:, :, None] for p in pieces(peak, 3) + pieces(totals, 3)]
        + [jnp.zeros((own, all_heads, 122), BF)],
        axis=2,
    )

    def combine(blocks):
        stats = blocks[..., latent:].astype(F32)
        peaks = jnp.sum(stats[..., :3], axis=-1, keepdims=True)
        sums = jnp.sum(stats[..., 3:6], axis=-1, keepdims=True)
        factor = jnp.exp(peaks - jnp.max(peaks, axis=0, keepdims=True))
        value = jnp.sum(blocks[..., :latent].astype(F32) * factor, axis=0)
        return (value / jnp.sum(sums * factor, axis=0)).astype(BF)

    if split_rows:
        per = own // nk
        sent = packed.reshape(nk, per, nt, heads, latent + 128).swapaxes(1, 2)
        sent = sent.reshape(nk * nt, per, heads, latent + 128)
        got = lax.all_to_all(sent, ("kv", "tp"), 0, 0, tiled=True)
        got = got.reshape(nk, nt, per, heads, latent + 128)
        o_lat = combine(got).swapaxes(0, 1).reshape(per * nt, heads, latent)
    else:
        flat = own * all_heads // nk
        got = lax.all_to_all(packed.reshape(nk, flat, latent + 128), "kv", 0, 0, tiled=True)
        o_own = spread(combine(got), "kv").reshape(own, nt, heads, latent)
        o_lat = lax.all_to_all(o_own.swapaxes(0, 1), "tp", 0, 0, tiled=True)
        o_lat = o_lat.swapaxes(0, 1).reshape(rows, heads, latent)
    o_heads = jnp.einsum("bhc,che->bhe", o_lat, value_up, preferred_element_type=F32).astype(BF)
    o_flat = o_heads.reshape(-1, heads * value_width)
    if split_rows:
        o_flat = spread(o_flat, "kv").reshape(rows, heads * value_width)

    core = lax.rem(tp_index, 2)
    swap = [(i, i ^ 1) for i in range(nt)]
    column = [list(range(c, nt, 2)) for c in range(2)]
    half = width // 2
    out_part = dot(o_flat, w_out).reshape(rows, 2, half)
    keep = jnp.where(core == 0, out_part[:, 0], out_part[:, 1])
    give = jnp.where(core == 0, out_part[:, 1], out_part[:, 0]).astype(BF)
    pair_sum = (keep + lax.ppermute(give, "tp", swap).astype(F32)).astype(BF)
    att_half = jnp.sum(spread(pair_sum, "tp", column).astype(F32), axis=0).astype(BF)
    att_other = lax.ppermute(att_half, "tp", swap)
    attended = jnp.where(
        core == 0,
        jnp.concatenate([att_half, att_other], axis=1),
        jnp.concatenate([att_other, att_half], axis=1),
    ).astype(F32)

    gain_m = block_of(mlp_gain)
    post = attended * block_of(post_gain)
    stacked = jnp.concatenate(
        [(gathered_float * gain_m).astype(BF), (post * gain_m).astype(BF)], axis=0
    )
    ff_dev = w_gate.shape[1]
    stats = [
        jnp.sum(a * b, axis=1, keepdims=True)
        for a, b in (
            (attended, attended),
            (gathered_float, gathered_float),
            (gathered_float, post),
            (post, post),
        )
    ]
    stat_block = jnp.concatenate(
        [jnp.concatenate(pieces(jnp.concatenate(stats[2 * i : 2 * i + 2], axis=0), 2), axis=1)
         for i in range(2)],
        axis=1,
    )
    ff_part = jnp.concatenate(
        [
            dot(stacked, w_gate).astype(BF),
            dot(stacked, w_up).astype(BF),
            stat_block,
        ],
        axis=1,
    )
    ff_sum = jnp.sum(spread(ff_part, "kv").astype(F32), axis=0)
    first = jnp.sum(ff_sum[:, 2 * ff_dev : 2 * ff_dev + 2], axis=1, keepdims=True)
    second = jnp.sum(ff_sum[:, 2 * ff_dev + 2 :], axis=1, keepdims=True)
    att_square, resid_square, cross, post_square = (
        first[:rows],
        first[rows:],
        second[:rows],
        second[rows:],
    )
    s = lax.rsqrt(att_square / model_width + EPS)
    mid_square = resid_square + 2.0 * s * cross + s * s * post_square
    scale_mid = lax.rsqrt(jnp.maximum(mid_square, 0.0) / model_width + EPS)
    mixed = (ff_sum[:rows] + s * ff_sum[rows:]) * scale_mid
    hidden = (jax.nn.silu(mixed[:, :ff_dev]) * mixed[:, ff_dev : 2 * ff_dev]).astype(BF)
    down = dot(hidden, w_down).astype(BF).reshape(own, nt, width).swapaxes(0, 1)
    lowered = jnp.sum(lax.all_to_all(down, "tp", 0, 0, tiled=True).astype(F32), axis=0)

    own_post = lax.dynamic_slice_in_dim(post.reshape(own, nt, width), tp_index, 1, 1)[:, 0]
    own_s = lax.dynamic_slice_in_dim(s.reshape(own, nt, 1), tp_index, 1, 1)[:, 0]
    resid_mid = (resid.astype(F32) + own_s * own_post).astype(BF).astype(F32)
    next_resid = (resid_mid + lowered).astype(BF)
    return (next_resid, new_latent, new_rope_key)


VMEM = pl.BlockSpec(memory_space=pltpu.VMEM)
WAIT = 4_000_000_000
NT = (((1,), (1,)), ((), ()))


def call(kernel, outs, *args, flops=0, scratch=()):
    many = isinstance(outs, (list, tuple))
    sizes = list(args) + (list(outs) if many else [outs])
    moved = sum(int(np.prod(a.shape)) * a.dtype.itemsize for a in sizes)
    return pl.pallas_call(
        kernel,
        out_shape=outs,
        in_specs=[VMEM] * len(args),
        out_specs=[VMEM] * len(outs) if many else VMEM,
        scratch_shapes=list(scratch),
        compiler_params=pltpu.CompilerParams(vmem_limit_bytes=16 << 20),
        cost_estimate=pl.CostEstimate(
            flops=max(flops, moved), bytes_accessed=moved, transcendentals=0
        ),
    )(*args)


def like(shape, dtype=BF):
    return jax.ShapeDtypeStruct(shape, dtype)


def lane_of(shape):
    return lax.broadcasted_iota(jnp.int32, shape, len(shape) - 1)


def terms(value, count):
    out, rest = [], value
    for _ in range(count):
        term = rest.astype(BF).astype(F32)
        out.append(term)
        rest = rest - term
    return out


def placed(columns, shape):
    lane = lane_of(shape)
    block = jnp.zeros(shape, F32)
    for at, column in columns:
        block = jnp.where(lane == at, column, block)
    return block


def picked(block, first, count):
    lane = lane_of(block.shape)
    inside = (lane >= first) & (lane < first + count)
    return jnp.sum(jnp.where(inside, block, 0.0), axis=-1, keepdims=True)


def turned(vector, table, half):
    width = vector.shape[1]
    low = lax.rem(lane_of(vector.shape), 2 * half) < half
    other = jnp.where(
        low, pltpu.roll(vector, width - half, 1), pltpu.roll(vector, half, 1)
    )
    return vector * table[0:1, :width] + other * table[1:2, :width]


def other(axis, k, step=1):
    return jnp.bitwise_xor(lax.div(lax.axis_index(axis), step), k)


def unit_kernel(out_ref):
    row = lax.rem(lax.broadcasted_iota(jnp.int32, out_ref.shape, 0), out_ref.shape[1] // 2)
    out_ref[...] = jnp.where(row == lane_of(out_ref.shape), 1.0, 0.0).astype(BF)


def start_kernel(b0, b1, b2, b3, unit_ref, out_ref, held_ref):
    chips, own, _ = held_ref.shape
    for k, ref in enumerate((b0, b1, b2, b3)):
        held_ref[other("tp", k, 2)] = ref[...].astype(F32)
    out_ref[...] = jnp.concatenate(
        [held_ref[z, r : r + 1, :] for r in range(own) for z in range(chips)], axis=0
    ).astype(BF)


def own_kernel(resid_ref, ga_ref, gp_ref, gm_ref, wl_ref, wk_ref, gains_ref, own_ref):
    own, width = resid_ref.shape
    nt = own_ref.shape[0]
    latent, rope = wl_ref.shape[1], wk_ref.shape[0]
    tiles = width // 128
    at = pl.multiple_of(lax.axis_index("kv") * tiles, tiles)
    gains = []
    for ref in (ga_ref, gp_ref, gm_ref):
        block = ref[pl.ds(at, tiles), :].astype(F32)
        gains.append(jnp.concatenate([block[i : i + 1] for i in range(tiles)], axis=1))
    gains_ref[...] = jnp.concatenate(gains + [jnp.zeros((8 - len(gains), width), F32)], axis=0)
    mine = jnp.concatenate([resid_ref[...].astype(F32), jnp.zeros((nt - own, width), F32)], axis=0)
    own_normed = (mine * gains[0]).astype(BF)
    lat = jnp.dot(own_normed, wl_ref[...], preferred_element_type=F32)
    at = pl.multiple_of(lax.axis_index("kv") * width, width)
    key = lax.dot_general(own_normed, wk_ref[:, pl.ds(at, width)], NT, preferred_element_type=F32)
    half = latent // 2
    own_ref[:, :half] = lat[:, :half] + pltpu.roll(lat[:, half:], own, 0)
    key = jnp.concatenate([key, jnp.zeros((nt, 128 - rope), F32)], axis=1)
    squares = terms(jnp.sum(mine * mine, axis=1, keepdims=True), 2)
    stat = placed([(rope + i, c) for i, c in enumerate(squares)], key.shape)
    own_ref[:, half:] = jnp.where(lane_of(key.shape) < rope, key, stat)


def query_kernel(
    rope, half_ref, other_ref, gains_ref, own_ref, wn_ref, wr_ref, m3, m2, m1, m0, rows_ref, sent_ref
):
    nt = own_ref.shape[0]
    nope_dev, rope_dev = wn_ref.shape[1], wr_ref.shape[1]
    first = lax.rem(lax.axis_index("tp"), 2) == 0
    mine, theirs = half_ref[...].astype(F32), other_ref[...].astype(F32)
    cores = (jnp.where(first, mine, theirs), jnp.where(first, theirs, mine))
    x = jnp.concatenate(
        [core[i : i + 1] for i in range(mine.shape[0]) for core in cores], axis=0
    )
    rows_ref[...] = x.astype(BF)
    gain = gains_ref[0:1, :]
    normed = (x * gain).astype(BF)
    qn = jnp.dot(normed, wn_ref[...], preferred_element_type=F32)
    qr = jnp.dot(normed, wr_ref[...], preferred_element_type=F32)
    square = jnp.sum(x * x, axis=1, keepdims=True)
    half = own_ref.shape[1] - 128
    lat, key = own_ref[:, :half], own_ref[:, half:]
    lane = lane_of(key.shape)
    for r in range(sent_ref.shape[0]):
        part = slice(r * nt, (r + 1) * nt)
        sent_ref[r, :, :nope_dev] = qn[part].astype(BF)
        sent_ref[r, :, nope_dev : nope_dev + rope_dev] = qr[part].astype(BF)
        base = nope_dev + rope_dev
        sent_ref[r, :, base : base + half] = lat.astype(BF)
        block = key
        for i, column in enumerate(terms(square[part], 2)):
            block = jnp.where(lane == rope + 2 + i, column, block)
        sent_ref[r, :, base + half :] = block.astype(BF)
    for k, ref in enumerate((m0, m1, m2, m3)):
        ref[...] = sent_ref[other("kv", k)]


def four(refs):
    a, b, c, d = (ref[...].astype(F32) for ref in refs)
    return (a + b) + (c + d)


def latent_kernel(
    model_width, own, b0, b1, b2, b3, ku_ref, gain_ref, table_ref, unit_ref,
    msg_ref, own_ref,
):
    nk, pairs, _ = msg_ref.shape
    nt = b0.shape[0]
    heads = pairs // nt
    latent, _, nope = ku_ref.shape
    nope_dev = heads * nope
    rope = unit_ref.shape[1] // 2
    rope_dev = heads * rope
    total = four((b0, b1, b2, b3))
    base, half = nope_dev + rope_dev, latent // 2
    stat = total[:, base + half :]
    scale = lax.rsqrt(picked(stat, rope + 2, 2) / model_width + EPS)
    own_scale = lax.rsqrt(picked(stat, rope, 2) / model_width + EPS)
    lat = total[:, base : base + half]
    lat = jnp.concatenate([lat, pltpu.roll(lat, own, 0)], axis=1)
    lat = lat * lax.rsqrt(jnp.mean(lat * lat, axis=1, keepdims=True) + EPS)
    lat = (lat * gain_ref[...].astype(F32)).astype(BF)
    table = table_ref[...]
    key = turned(stat * own_scale, table, rope // 2).astype(BF)
    own_ref[:, :latent] = lat.astype(F32)
    own_ref[:, latent:] = key.astype(F32)
    qn = total[:, :nope_dev].astype(BF).astype(F32)
    qr = turned(total[:, nope_dev:base] * scale, table, rope // 2).astype(BF).astype(F32)

    def diagonal(q, size):
        shape = (nt, heads, heads * size)
        head = lax.broadcasted_iota(jnp.int32, shape, 1)
        lane = lax.broadcasted_iota(jnp.int32, shape, 2)
        keep = (lane >= head * size) & (lane < (head + 1) * size)
        spread_q = jnp.broadcast_to(q[:, None, :], shape)
        return jnp.where(keep, spread_q, 0.0).reshape(nt * heads, heads * size).astype(BF)

    raw = lax.dot_general(
        diagonal(qn, nope), ku_ref[...].reshape(latent, nope_dev), NT, preferred_element_type=F32
    )
    scales = jnp.broadcast_to(scale[:, None, :], (nt, heads, latent)).reshape(pairs, latent)
    q_lat = (raw * scales).astype(BF)
    q_rope = jnp.dot(diagonal(qr, rope), unit_ref[...], preferred_element_type=F32).astype(BF)
    for j in range(nk):
        msg_ref[j, :, :latent] = q_lat
        msg_ref[j, :, latent:] = q_rope


def attend_kernel(score_scale, q_ref, cache_ref, rope_ref, own_ref, msg_ref):
    own, all_heads, _ = q_ref.shape
    latent = cache_ref.shape[2]
    rope = rope_ref.shape[1]
    holds_own = lax.axis_index("kv") == 0
    lat, key = own_ref[:, :latent], own_ref[:, latent : latent + rope]
    seqs = range(own)
    q_lat = [q_ref[r, :, :latent] for r in seqs]
    q_rope = [q_ref[r, :, latent : latent + rope] for r in seqs]
    scores = [
        (
            lax.dot_general(q_lat[r], cache_ref[r], NT, preferred_element_type=F32)
            + jnp.dot(q_rope[r], rope_ref[r], preferred_element_type=F32)
        )
        * score_scale
        for r in seqs
    ]
    own_scores = [
        (
            jnp.sum(q_lat[r].astype(F32) * lat[r : r + 1], axis=1, keepdims=True)
            + jnp.sum(q_rope[r].astype(F32) * key[r : r + 1], axis=1, keepdims=True)
        )
        * score_scale
        for r in seqs
    ]
    peaks = [
        jnp.maximum(jnp.max(scores[r], axis=1, keepdims=True), own_scores[r]) for r in seqs
    ]
    probs = [jnp.exp(scores[r] - peaks[r]) for r in seqs]
    values = [
        jnp.dot(probs[r].astype(BF), cache_ref[r], preferred_element_type=F32) for r in seqs
    ]
    for r in seqs:
        own_prob = jnp.where(holds_own, jnp.exp(own_scores[r] - peaks[r]), 0.0)
        total = jnp.sum(probs[r], axis=1, keepdims=True) + own_prob
        msg_ref[r, :, :latent] = (values[r] + own_prob * lat[r : r + 1]).astype(BF)
        columns = list(enumerate(terms(peaks[r], 3) + terms(total, 3)))
        msg_ref[r, :, latent:] = placed(columns, (all_heads, 128)).astype(BF)


def value_kernel(heads, got_ref, vu_ref, a0, a1, a2, a3, m3, m2, m1, m0):
    nk, pairs, _ = got_ref.shape
    latent, _, size = vu_ref.shape
    value_dev = heads * size
    nt = pairs // heads
    stats = [got_ref[j, :, latent:].astype(F32) for j in range(nk)]
    peaks = [picked(s, 0, 3) for s in stats]
    peak = functools.reduce(jnp.maximum, peaks)
    factors = [jnp.exp(p - peak) for p in peaks]
    total = sum(picked(s, 3, 3) * f for s, f in zip(stats, factors))
    value = sum(got_ref[j, :, :latent].astype(F32) * f for j, f in enumerate(factors))
    o_lat = (value / total).astype(BF)
    full = jnp.dot(o_lat, vu_ref[...].reshape(latent, value_dev), preferred_element_type=F32)
    shape = (nt, heads, value_dev)
    head = lax.broadcasted_iota(jnp.int32, shape, 1)
    lane = lax.broadcasted_iota(jnp.int32, shape, 2)
    keep = (lane >= head * size) & (lane < (head + 1) * size)
    o_heads = jnp.sum(jnp.where(keep, full.reshape(shape), 0.0), axis=1).astype(BF)
    rows, wide = a0.shape
    for a, m in ((a3, m3), (a2, m2), (a1, m1), (a0, m0)):
        m[:, :value_dev] = o_heads
        for g in range(rows // nt):
            m[:, value_dev + g * wide : value_dev + (g + 1) * wide] = a[g * nt : (g + 1) * nt]


def out_kernel(b0, b1, b2, b3, w_ref, keep_ref, give_ref, base_ref, held_ref):
    half = keep_ref.shape[1]
    _, nt, value_dev = held_ref.shape
    rows, wide = base_ref.shape
    for k, ref in enumerate((b0, b1, b2, b3)):
        held_ref[other("kv", k)] = ref[:, :value_dev].astype(F32)
    for g in range(rows // nt):
        lo = value_dev + g * wide
        a, b, c, d = (ref[:, lo : lo + wide].astype(F32) for ref in (b0, b1, b2, b3))
        base_ref[g * nt : (g + 1) * nt] = (a + b) + (c + d)
    first = lax.rem(lax.axis_index("tp"), 2) == 0
    o_heads = held_ref[...].reshape(keep_ref.shape[0], w_ref.shape[0]).astype(BF)
    out = jnp.dot(o_heads, w_ref[...], preferred_element_type=F32)
    keep_ref[...] = jnp.where(first, out[:, :half], out[:, half:])
    give_ref[...] = jnp.where(first, out[:, half:], out[:, :half]).astype(BF)


def pair_kernel(keep_ref, got_ref, out_ref):
    out_ref[...] = (keep_ref[...] + got_ref[...].astype(F32)).astype(BF)


def column_kernel(b0, b1, b2, b3, out_ref):
    out_ref[...] = four((b0, b1, b2, b3)).astype(BF)


def added(a, b):
    return jnp.sum(a * b, axis=1, keepdims=True)


def send_parts(parts, sums, refs, msg_ref):
    nk, rows, wide = msg_ref.shape
    chunk = parts[0].shape[1] // nk
    columns = list(enumerate(t for value in sums for t in terms(value, 3)))
    stat = placed(columns, (rows, 128))[:, : wide - 2 * chunk]
    for j in range(nk):
        block = slice(j * chunk, (j + 1) * chunk)
        msg_ref[j] = jnp.concatenate([part[:, block] for part in parts] + [stat], axis=1).astype(BF)
    for k, ref in enumerate(refs):
        ref[...] = msg_ref[other("kv", k)]


def base_kernel(rows_ref, gains_ref, wg_ref, wu_ref, m3, m2, m1, m0, msg_ref):
    x = rows_ref[...].astype(F32)
    left = (x * gains_ref[2:3, :]).astype(BF)
    parts = [
        lax.dot_general(left, w[...], NT, preferred_element_type=F32) for w in (wg_ref, wu_ref)
    ]
    send_parts(parts, [added(x, x)], (m0, m1, m2, m3), msg_ref)


def half_products(half_ref, core, gains_ref, wg_ref, wu_ref):
    half = half_ref.shape[1]
    at = pl.ds(pl.multiple_of(core * half, half), half)
    gain = gains_ref[1:3, at]
    left = (half_ref[...].astype(F32) * gain[0:1] * gain[1:2]).astype(BF)
    return [
        lax.dot_general(left, w[:, at], NT, preferred_element_type=F32) for w in (wg_ref, wu_ref)
    ]


def early_kernel(half_ref, gains_ref, wg_ref, wu_ref, gate_ref, up_ref):
    core = lax.rem(lax.axis_index("tp"), 2)
    gate_ref[...], up_ref[...] = half_products(half_ref, core, gains_ref, wg_ref, wu_ref)


def gate_kernel(
    half_ref, other_ref, gate_ref, up_ref, rows_ref, gains_ref, wg_ref, wu_ref,
    m3, m2, m1, m0, post_ref, msg_ref,
):
    core = lax.rem(lax.axis_index("tp"), 2)
    late = half_products(other_ref, 1 - core, gains_ref, wg_ref, wu_ref)
    parts = [gate_ref[...] + late[0], up_ref[...] + late[1]]
    mine, theirs = half_ref[...].astype(F32), other_ref[...].astype(F32)
    first = core == 0
    att = jnp.concatenate(
        [jnp.where(first, mine, theirs), jnp.where(first, theirs, mine)], axis=1
    )
    x = rows_ref[...].astype(F32)
    post = att * gains_ref[1:2, :]
    post_ref[...] = post
    sums = [added(att, att), added(x, post), added(post, post)]
    send_parts(parts, sums, (m0, m1, m2, m3), msg_ref)


def hidden_kernel(model_width, b0, b1, b2, b3, base_ref, out_ref, s_ref):
    _, chunk = out_ref.shape
    total, base = four((b0, b1, b2, b3)), base_ref[...]
    tail = total.shape[1] - 128
    at = 2 * chunk - tail
    x_square = picked(base[:, tail:], at, 3)
    att_square, cross, post_square = (picked(total[:, tail:], at + 3 * i, 3) for i in range(3))
    s = lax.rsqrt(att_square / model_width + EPS)
    mid = jnp.maximum(x_square + 2.0 * s * cross + s * s * post_square, 0.0)
    scale = lax.rsqrt(mid / model_width + EPS)
    s_ref[...] = jnp.broadcast_to(s, s_ref.shape)
    mixed = (base[:, : 2 * chunk] + s * total[:, : 2 * chunk]) * scale
    gate, up = mixed[:, :chunk], mixed[:, chunk : 2 * chunk]
    out_ref[...] = (gate / (1.0 + jnp.exp(-gate)) * up).astype(BF)


def down_part(hidden_ref, w_ref, k):
    chunk = hidden_ref.shape[1]
    at = pl.multiple_of(other("kv", k) * chunk, 8)
    return jnp.dot(hidden_ref[...], w_ref[pl.ds(at, chunk), :], preferred_element_type=F32)


def first_kernel(hidden_ref, w_ref, out_ref):
    out_ref[...] = down_part(hidden_ref, w_ref, 0)


def down_kernel(first_ref, b1, b2, b3, w_ref, keep_ref, give_ref, total_ref):
    total = first_ref[...]
    for k, ref in ((1, b1), (2, b2), (3, b3)):
        total = total + down_part(ref, w_ref, k)
    total_ref[...] = total.reshape(total_ref.shape)
    core = lax.rem(lax.axis_index("tp"), 2)
    for k in range(keep_ref.shape[0]):
        at = 2 * other("tp", k, 2)
        keep_ref[k] = total_ref[:, at + core, :]
        give_ref[k] = total_ref[:, at + 1 - core, :].astype(BF)


def chips_kernel(keep_ref, got_ref, m3, m2, m1, m0):
    for k, ref in enumerate((m0, m1, m2, m3)):
        ref[...] = (keep_ref[k] + got_ref[k].astype(F32)).astype(BF)


def last_kernel(
    b0, b1, b2, b3, resid_ref, post_ref, s_ref, own_ref, out_ref, lat_ref, key_ref
):
    own, width = resid_ref.shape
    nt = post_ref.shape[0] // own
    total = four((b0, b1, b2, b3))
    added = (post_ref[...] * s_ref[:, 0:1]).reshape(own, nt, width)
    here = lax.broadcasted_iota(jnp.int32, added.shape, 1) == lax.axis_index("tp")
    mine = jnp.sum(jnp.where(here, added, 0.0), axis=1)
    mid = (resid_ref[...].astype(F32) + mine).astype(BF).astype(F32)
    out_ref[...] = (mid + total).astype(BF)
    latent, rope = lat_ref.shape[1], key_ref.shape[1]
    lat_ref[...] = own_ref[:own, :latent].astype(BF)
    key_ref[...] = own_ref[:own, latent : latent + rope].astype(BF)


def exchange(message, axis):
    return lax.all_to_all(message, axis, 0, 0, tiled=True)


def deal(blocks, axis, step=1):
    size = lax.axis_size(axis)
    out = list(blocks)
    for k in reversed(range(1, len(blocks))):
        out[k] = lax.ppermute(blocks[k], axis, [(i, i ^ (k * step)) for i in range(size)])
    return out


def kernel_body(
    resid,
    attn_gain,
    w_query_nope,
    w_query_rope,
    w_latent,
    w_key_rope,
    latent_gain,
    key_up,
    value_up,
    w_out,
    post_gain,
    mlp_gain,
    w_gate,
    w_up,
    w_down,
    cache_latent,
    cache_rope_key,
):
    nk = lax.axis_size("kv")
    nt = lax.axis_size("tp")
    own, width = resid.shape
    rows = own * nt
    model_width = width * nk
    latent, heads, nope = key_up.shape
    rope = cache_rope_key.shape[2]
    nope_dev, rope_dev = heads * nope, heads * rope
    ff_dev = w_gate.shape[1]
    context = cache_latent.shape[1] * nk
    half_rope = rope // 2
    angles = context * THETA ** (-np.arange(half_rope) / half_rope)
    cos, sin = np.cos(angles), np.sin(angles)
    table = np.zeros((8, rope_dev), np.float32)
    table[0] = np.tile(np.concatenate([cos, cos]), heads)
    table[1] = np.tile(np.concatenate([-sin, sin]), heads)

    swap = [(i, i ^ 1) for i in range(nt)]
    chips = nt // 2
    unit = call(unit_kernel, like((rope_dev, 2 * rope)), flops=WAIT)
    value_dev = heads * value_up.shape[2]
    gains, own_rows = call(
        own_kernel,
        [like((8, width), F32), like((nt, latent // 2 + 128), F32)],
        resid,
        *[g.reshape(-1, 128) for g in (attn_gain, post_gain, mlp_gain)],
        w_latent,
        w_key_rope.T,
        flops=WAIT,
    )
    column = call(
        start_kernel,
        like((own * chips, width)),
        *deal([resid] * chips, "tp", 2),
        unit,
        scratch=[pltpu.VMEM((chips, own, width), F32)],
        flops=WAIT,
    )
    sent_width = nope_dev + rope_dev + latent // 2 + 128
    *msg, x_rows = call(
        functools.partial(query_kernel, rope),
        [like((nt, sent_width))] * nk + [like((rows, width))],
        column,
        lax.ppermute(column, "tp", swap),
        gains,
        own_rows,
        w_query_nope,
        w_query_rope,
        scratch=[pltpu.VMEM((nk, nt, sent_width), BF)],
        flops=WAIT,
    )
    pairs = nt * heads
    chunk = ff_dev // nk
    wide = -(-(2 * chunk + 9) // 128) * 128
    base_parts = call(
        base_kernel,
        [like((rows, wide))] * nk,
        x_rows,
        gains,
        w_gate.T,
        w_up.T,
        scratch=[pltpu.VMEM((nk, rows, wide), BF)],
        flops=WAIT,
    )[::-1]
    msg, own_block = call(
        functools.partial(latent_kernel, model_width, own),
        [like((nk, pairs, latent + 128)), like((nt, latent + 128), F32)],
        *deal(msg[::-1], "kv"),
        key_up,
        latent_gain.reshape(1, latent),
        jnp.asarray(table),
        unit,
        flops=WAIT,
    )
    got = exchange(msg.reshape(nk * nt, heads, latent + 128), ("kv", "tp"))
    msg = call(
        functools.partial(attend_kernel, (nope + rope) ** (-0.5)),
        like((own, pairs, latent + 128)),
        got.reshape(own, pairs, latent + 128),
        cache_latent,
        cache_rope_key.swapaxes(1, 2),
        own_block,
        flops=WAIT,
    )
    got = exchange(msg.reshape(nk * nt, heads, latent + 128), ("kv", "tp"))
    msg = call(
        functools.partial(value_kernel, heads),
        [like((nt, value_dev + own * wide))] * nk,
        got.reshape(nk, pairs, latent + 128),
        value_up,
        *base_parts,
        flops=WAIT,
    )
    half = width // 2
    keep, give, base = call(
        out_kernel,
        [like((rows, half), F32), like((rows, half)), like((rows, wide), F32)],
        *deal(msg[::-1], "kv"),
        w_out,
        scratch=[pltpu.VMEM((nk, nt, value_dev), F32)],
        flops=WAIT,
    )
    pair = call(
        pair_kernel, like((rows, half)), keep, lax.ppermute(give, "tp", swap), flops=WAIT
    )
    att_half = call(column_kernel, like((rows, half)), *deal([pair] * chips, "tp", 2), flops=WAIT)
    att_other = lax.ppermute(att_half, "tp", swap)
    early = call(
        early_kernel,
        [like((rows, ff_dev), F32)] * 2,
        att_half,
        gains,
        w_gate.T,
        w_up.T,
        flops=WAIT,
    )
    *msg, post = call(
        gate_kernel,
        [like((rows, wide))] * nk + [like((rows, width), F32)],
        att_half,
        att_other,
        *early,
        x_rows,
        gains,
        w_gate.T,
        w_up.T,
        scratch=[pltpu.VMEM((nk, rows, wide), BF)],
        flops=WAIT,
    )
    hidden, s = call(
        functools.partial(hidden_kernel, model_width),
        [like((rows, chunk)), like((rows, 128), F32)],
        *deal(msg[::-1], "kv"),
        base,
        flops=WAIT,
    )
    first = call(first_kernel, like((rows, width), F32), hidden, w_down, flops=WAIT)
    keep, give = call(
        down_kernel,
        [like((chips, own, width), F32), like((chips, own, width))],
        first,
        *deal([hidden] * nk, "kv")[1:],
        w_down,
        scratch=[pltpu.VMEM((own, nt, width), F32)],
        flops=WAIT,
    )
    msg = call(
        chips_kernel,
        [like((own, width))] * chips,
        keep,
        lax.ppermute(give, "tp", swap),
        flops=WAIT,
    )
    next_resid, new_latent, new_rope_key = call(
        last_kernel,
        [like((own, width)), like((own, latent)), like((own, rope))],
        *deal(msg[::-1], "tp", 2),
        resid,
        post,
        s,
        own_block,
        flops=WAIT,
    )
    return (next_resid, new_latent, new_rope_key)


def body(*args):
    resid, key_up, cache = args[0], args[7], args[15]
    nk, nt = lax.axis_size("kv"), lax.axis_size("tp")
    own, width = resid.shape
    latent, heads, nope = key_up.shape
    fits = (
        own == nk == 4
        and nt == 8
        and heads == 8
        and 2 * own == nt
        and width % 1024 == 0
        and latent % 256 == 0
        and args[12].shape[1] % (8 * nk) == 0
        and args[12].shape[1] // nk >= 64
        and nope % 128 == 0
        and cache.shape[1] % 128 == 0
        and args[16].shape[2] == 64
    )
    if not fits:
        return plain_body(*args)
    return kernel_body(*args)


def solution(mesh):
    return jax.shard_map(
        body,
        mesh=mesh,
        in_specs=(
            P("tp", "kv"),
            P(),
            P("kv", "tp"),
            P("kv", "tp"),
            P("kv", None),
            P(),
            P(),
            P(None, "tp", None),
            P(None, "tp", None),
            P("tp", "kv"),
            P(),
            P(),
            P("kv", "tp"),
            P("kv", "tp"),
            P("tp", "kv"),
            P("tp", "kv", None),
            P("tp", "kv", None),
        ),
        out_specs=(P("tp", "kv"), P("tp", None), P("tp", None)),
        check_vma=False,
    )
```
